512 devices in a mesh: sp: 32 (over z, core), tp: 16 (over y, x).
Axes of the slice: x: 4, y: 4, z: 16, core: 2. Of those that a mesh axis runs over, the one named last changes fastest.
Arguments:
- cotangent: bfloat16 [4096, 2048], P('sp'), may hold values from -6 to 6
- moe_input: bfloat16 [4096, 2048], P('sp'), may hold values from -6 to 6
- expert_ids: int32 [4096, 2], P('sp'), may hold values from 0 to 31, all different within a row; in each aligned block of 128 rows (0 to 127, 128 to 255, ...) at most 12 rows name the same one
- group_weight: float32 [4096], P('sp'), may hold values from 0.3 to 1
- expert_weight: float32 [4096, 2], P('sp'), may hold values from 0.1 to 0.9
- mixer_out: bfloat16 [4096, 2048], P('sp', 'tp'), may hold values from -6 to 6
- queries: bfloat16 [1024, 4096], P('tp', 'sp'), may hold values from -6 to 6
- key_vectors: bfloat16 [1024, 4096], P('tp', 'sp'), may hold values from -6 to 6
- value_vectors: bfloat16 [2048, 4096], P('tp', 'sp'), may hold values from -6 to 6
- decay_rates: float32 [16, 4096], P('tp', 'sp'), may hold values from 0 to 1, as said below
- proj_weight: bfloat16 [2048, 2048], P(None, 'tp'), may hold values from -0.125 to 0.125
- gate_weight: bfloat16 [32, 2048, 2048], P('sp', None, 'tp'), may hold values from -0.125 to 0.125
- up_weight: bfloat16 [32, 2048, 2048], P('sp', None, 'tp'), may hold values from -0.125 to 0.125
- down_weight: bfloat16 [32, 2048, 2048], P('sp', 'tp'), may hold values from -0.125 to 0.125
Outputs:
- grad_gate: bfloat16 [32, 2048, 2048], P('sp', None, 'tp')
- grad_up: bfloat16 [32, 2048, 2048], P('sp', None, 'tp')
- grad_down: bfloat16 [32, 2048, 2048], P('sp', 'tp')
- grad_proj: float32 [2048, 2048], P('sp', 'tp')
- grad_queries: float32 [1024, 4096], P('tp', 'sp')
- grad_keys: float32 [1024, 4096], P('tp', 'sp')
- grad_values: float32 [2048, 4096], P('tp', 'sp')
The draws below stay inside these ranges and needn't reach their ends.
Inputs may be any that keep to these rules, and one draw needn't show every extreme that they name: `expert_ids`: in the rows of one device no expert is named by more than 12 entries, a bound that some block reaches; the 2 experts of a row differ. `decay_rates`: Positive.
All inputs are finite; a program needn't handle non-finite values.
Results may differ from the reference program's by a relative error of at most 0.0058.
Values may be sent and summed in bfloat16 or wider, within the bound.
No kernel may reach another device: no remote copies, remote signals or barrier semaphores. Data moves between devices by JAX's collectives and lax.ppermute only.
A program may use at most 64 MiB of HBM per device.

```python
import math
from functools import partial
import jax
import jax.numpy as jnp
import numpy as np
from jax import lax

D = 2048
KD = 64
VD = 128
RETENTION_HEADS = 16
FF = 2048
EXPERTS = 32
TOP = 2
TOK_DEV = 128
SEQUENCE_TOKENS = 4096
CAP = 12
N_SP = 32


def draw_decay_rates(key, part):
    random_subkeys = jax.random.split(key, 6)
    fast_share = 0.5
    fast_heads = jax.random.uniform(random_subkeys[0], (RETENTION_HEADS, 1)) < fast_share
    block_count = SEQUENCE_TOKENS // TOK_DEV
    block_multiplier = jax.random.uniform(random_subkeys[1], (RETENTION_HEADS, block_count, 1), minval=0.5, maxval=1.5)
    block_multiplier = jnp.broadcast_to(block_multiplier, (RETENTION_HEADS, block_count, TOK_DEV)).reshape(RETENTION_HEADS, SEQUENCE_TOKENS)
    jaggedness = jnp.exp(jax.random.uniform(random_subkeys[2], (RETENTION_HEADS, SEQUENCE_TOKENS), minval=math.log(0.7), maxval=math.log(1.4)))
    fast_rate = jnp.exp(jax.random.uniform(random_subkeys[3], (RETENTION_HEADS, 1), minval=math.log(1.0 / 40.0), maxval=math.log(1.0 / 15.0)))
    baseline_rate = jnp.where(fast_heads, fast_rate, 0.8 / SEQUENCE_TOKENS)
    spike_position = jax.random.randint(random_subkeys[4], (RETENTION_HEADS, 2, 1), 0, SEQUENCE_TOKENS)
    spike_penalty = jax.random.uniform(random_subkeys[5], (RETENTION_HEADS, 2, 1), minval=0.2, maxval=0.4)
    token_positions = jnp.arange(SEQUENCE_TOKENS, dtype=jnp.int32)[None, None, :]
    spike_events = jnp.sum(jnp.where(token_positions == spike_position, -jnp.log(1.0 - spike_penalty), 0.0), axis=1)
    return (baseline_rate * block_multiplier * jaggedness + spike_events).astype(jnp.float32)


def with_spikes(array, rng, source, target, blocks, factor):
    owner, partner = [(jnp.arange(array.shape[dim]) // (array.shape[dim] // blocks)).reshape([-1 if axis == dim else 1 for axis in range(array.ndim)]) for dim in (source, target)]
    chosen = jax.random.permutation(rng, blocks)[partner]
    strong = (owner == chosen) | (owner == (partner + blocks // 2) % blocks)
    return jnp.where(strong, factor * array, array)


def level_of(rng, shape, pieces, low, high):
    def one(dim, blocks):
        heights = jax.random.uniform(jax.random.fold_in(jax.random.fold_in(rng, 6), dim), (blocks,), jnp.float32, low / len(pieces), high / len(pieces))
        return jnp.repeat(jnp.exp(heights), shape[dim] // blocks).reshape((-1,) + (1,) * (len(shape) - dim - 1))

    loudness = one(*pieces[0])
    for cut in pieces[1:]:
        loudness = loudness * one(*cut)
    return loudness


def shared_out(key, own, number, rows, count, top, most, skew):
    order = jax.random.permutation(key, count)
    packed, common = shares(count, rows * top, most, skew, True), shares(count, rows * top, most, skew, False)
    places = jnp.arange(count)

    def named(tallies, rotation):
        used = int((tallies > 0).sum())
        fixed = max(1, used // 4)
        moved = fixed + (places - fixed + rotation * (used - fixed)) % max(1, count - fixed)
        return jnp.zeros((count,), jnp.int32).at[order[jnp.where(places < fixed, places, moved)]].set(jnp.asarray(tallies, jnp.int32))

    tallies = jnp.where(number % 4 == 0, named(packed, number // 4), named(common, number - number // 4 - 1))
    mixed = jax.random.permutation(jax.random.fold_in(own, 3), count)
    source_of, taker = mixed[0:count // 2 * 2:2], mixed[1:count // 2 * 2:2]
    room = jnp.minimum(tallies[source_of] - 1, most - tallies[taker]) // 2
    room = jnp.where((source_of == order[0]) | (taker == order[0]) | (tallies[taker] == 0), 0, jnp.maximum(room, 0))
    moved = jax.random.randint(jax.random.fold_in(own, 4), (count // 2,), 0, 1 << 20) % (room + 1)
    tallies = tallies.at[source_of].add(-moved).at[taker].add(moved)
    members = jnp.searchsorted(jnp.cumsum(tallies), jnp.arange(rows * top), side="right").astype(jnp.int32)
    table = members.reshape(top, rows).T
    table = table[jax.random.permutation(jax.random.fold_in(own, 1), rows)]
    rotation = jax.random.randint(jax.random.fold_in(own, 2), (rows, 1), 0, top)
    return jnp.take_along_axis(table, (jnp.arange(top)[None, :] + rotation) % top, axis=1)


def shares(count, total, bound, slope, full):
    loads = [(1 << 20) // math.isqrt(grade ** slope) + 1 for grade in range(1, count + 1)]
    largest = bound if full else min(bound, max(-(-total // count), total * loads[0] // sum(loads)))
    least = 1 if total - largest >= count - 1 else 0
    holding, spare = [largest] + [least] * (count - 1), total - largest - least * (count - 1)
    while spare > 0:
        free = [i for i in range(1, count) if holding[i] < largest] or [i for i in range(1, count) if holding[i] < bound]
        pool, remaining = sum([loads[i] for i in free]), spare
        for i in free:
            addition = min(bound - holding[i], max(1, remaining * loads[i] // pool), spare)
            holding[i] = holding[i] + addition
            spare = spare - addition
    return np.array(holding)


def bell_draw(key, shape, width, limit, cuts=(), held_as=jnp.bfloat16):
    loudness = level_of(key, shape, cuts, -0.22, 0.18) if cuts else 1.0
    values = jax.random.normal(key, shape, jnp.float32) * width * loudness
    return jnp.minimum(jnp.maximum(values, -limit), limit).astype(held_as)


def noise_with(key, dims, deviation, reach, pieces, heavy, kind=jnp.bfloat16):
    array = deviation * jax.random.normal(key, dims, jnp.float32)
    if pieces:
        array = array * level_of(key, dims, pieces, -0.22, 0.18)
    return jnp.clip(with_spikes(array, jax.random.fold_in(key, 3), *heavy), -reach, reach).astype(kind)


def setup_inputs(seed: int = 0) -> dict:
    splits = jax.random.split(jax.random.key(seed), 15)
    cotangent = noise_with(splits[0], (SEQUENCE_TOKENS, D), 1.0, 6.0, ((0, 32),), (0, 1, 32, 2.75))
    moe_input = bell_draw(splits[1], (SEQUENCE_TOKENS, D), 1.0, 6.0, ((0, 32),))
    expert_ids_keys = jax.random.split(jax.random.fold_in(splits[2], 1), SEQUENCE_TOKENS // TOK_DEV)
    expert_ids_turns = jax.random.permutation(jax.random.fold_in(splits[2], 3), SEQUENCE_TOKENS // TOK_DEV)
    expert_ids = jax.vmap(lambda own, number: shared_out(jax.random.fold_in(splits[2], 2), own, number, TOK_DEV, EXPERTS, TOP, CAP, 1))(expert_ids_keys, expert_ids_turns).reshape((SEQUENCE_TOKENS, TOP))
    group_weight = jnp.clip(0.3 + 0.7 * jax.random.uniform(splits[3], (SEQUENCE_TOKENS,), jnp.float32) ** level_of(splits[3], (SEQUENCE_TOKENS,), ((0, 32),), -0.2, 0.2), 0.3, 1.0)
    expert_weight = jnp.clip(0.1 + 0.79999997 * jax.random.uniform(splits[4], (SEQUENCE_TOKENS, TOP), jnp.float32) ** level_of(splits[4], (SEQUENCE_TOKENS, TOP), ((0, 32),), -0.2, 0.2), 0.1, 0.9)
    mixer_out = bell_draw(splits[5], (SEQUENCE_TOKENS, RETENTION_HEADS * VD), 1.0, 6.0, ((0, 32), (1, 16)))
    queries = bell_draw(splits[6], (RETENTION_HEADS * KD, SEQUENCE_TOKENS), 1.0, 6.0, ((0, 16), (1, 32)))
    key_vectors = bell_draw(splits[7], (RETENTION_HEADS * KD, SEQUENCE_TOKENS), 1.0, 6.0, ((0, 16), (1, 32)))
    value_vectors = bell_draw(splits[8], (RETENTION_HEADS * VD, SEQUENCE_TOKENS), 1.0, 6.0, ((0, 16), (1, 32)))
    decay_rates = draw_decay_rates(jax.random.fold_in(splits[14], 71), 0)
    proj_weight = bell_draw(splits[10], (D, RETENTION_HEADS * VD), (RETENTION_HEADS * VD) ** -0.5, 0.125, ((1, 16),))
    gate_weight = bell_draw(splits[11], (EXPERTS, D, FF), D ** -0.5, 0.125, ((0, 32), (2, 16)))
    up_weight = bell_draw(splits[12], (EXPERTS, D, FF), D ** -0.5, 0.125, ((0, 32), (2, 16)))
    down_weight = bell_draw(splits[13], (EXPERTS, FF, D), FF ** -0.5, 0.125, ((0, 32), (1, 16)))
    return dict(cotangent=cotangent, moe_input=moe_input, expert_ids=expert_ids, group_weight=group_weight, expert_weight=expert_weight, mixer_out=mixer_out, queries=queries, key_vectors=key_vectors, value_vectors=value_vectors, decay_rates=decay_rates, proj_weight=proj_weight, gate_weight=gate_weight, up_weight=up_weight, down_weight=down_weight)


def slot_table(block_ids, experts_all, capacity):
    flat_ids = block_ids.reshape(-1).astype(jnp.int32)
    expert_range = jnp.arange(experts_all, dtype=jnp.int32)
    onehot = (flat_ids[:, None] == expert_range[None, :]).astype(jnp.int32)
    before = jnp.cumsum(onehot, axis=0) - onehot
    rank_in = jnp.sum(before * onehot, axis=1)
    slot_ids = flat_ids * capacity + rank_in
    slot_range = jnp.arange(experts_all * capacity, dtype=jnp.int32)
    entry_numbers = jnp.arange(1, flat_ids.shape[0] + 1, dtype=jnp.int32)
    owners = jnp.sum(jnp.where(slot_ids[None, :] == slot_range[:, None], entry_numbers[None, :], 0), axis=1) - 1
    return slot_ids, owners


def pack_rows(cotangent, moe_input, group_weight, expert_weight, expert_ids, experts_all, capacity):
    slot_ids, owners = slot_table(expert_ids, experts_all, capacity)
    present = owners >= 0
    entry_ids = jnp.maximum(owners, 0)
    token_ids = entry_ids // expert_ids.shape[1]
    route_weight = (group_weight[:, None] * expert_weight).reshape(-1)
    row_scale = jnp.where(present, route_weight[entry_ids], 0.0)
    cot_rows = (cotangent[token_ids].astype(jnp.float32) * row_scale[:, None]).astype(jnp.bfloat16)
    inp_rows = jnp.where(present[:, None], moe_input[token_ids], jnp.zeros((), moe_input.dtype))
    return cot_rows, inp_rows, slot_ids


def expert_grads(operands):
    rows_cot, rows_inp, w_gate, w_up, w_down = operands
    gate_pre = jnp.dot(rows_inp, w_gate, preferred_element_type=jnp.float32)
    up_pre = jnp.dot(rows_inp, w_up, preferred_element_type=jnp.float32)
    sigmoid_gate = jax.nn.sigmoid(gate_pre)
    hidden = (gate_pre * sigmoid_gate * up_pre).astype(jnp.bfloat16)
    grad_down = jnp.dot(hidden.T, rows_cot, preferred_element_type=jnp.float32).astype(jnp.bfloat16)
    hidden_grad = jnp.dot(rows_cot, w_down.T, preferred_element_type=jnp.float32)
    gate_grad = (hidden_grad * up_pre * sigmoid_gate * (1.0 + gate_pre * (1.0 - sigmoid_gate))).astype(jnp.bfloat16)
    up_grad = (hidden_grad * gate_pre * sigmoid_gate).astype(jnp.bfloat16)
    grad_gate = jnp.dot(rows_inp.T, gate_grad, preferred_element_type=jnp.float32).astype(jnp.bfloat16)
    grad_up = jnp.dot(rows_inp.T, up_grad, preferred_element_type=jnp.float32).astype(jnp.bfloat16)
    entry_sum = jnp.dot(gate_grad, w_gate.T, preferred_element_type=jnp.float32) + jnp.dot(up_grad, w_up.T, preferred_element_type=jnp.float32)
    entry_grad = entry_sum.astype(jnp.bfloat16)
    return grad_gate, grad_up, grad_down, entry_grad


def head_grads(operands):
    query_head, key_head, value_head, grad_head, rate_head = operands
    exact_result = lax.Precision.HIGHEST
    cumulative = jnp.cumsum(rate_head)
    mixing = jnp.exp(-jnp.abs(cumulative[:, None] - cumulative[None, :]))
    score_scale = KD ** -0.5
    scores = score_scale * jnp.dot(query_head.T, key_head, precision=exact_result) * mixing
    score_grad = score_scale * jnp.dot(grad_head.T, value_head, precision=exact_result) * mixing
    query_grad = jnp.dot(key_head, score_grad.T, precision=exact_result)
    key_grad = jnp.dot(query_head, score_grad, precision=exact_result)
    value_grad = jnp.dot(grad_head, scores, precision=exact_result)
    return query_grad, key_grad, value_grad


def reference(cotangent, moe_input, expert_ids, group_weight, expert_weight, mixer_out, queries, key_vectors, value_vectors, decay_rates, proj_weight, gate_weight, up_weight, down_weight):
    packer = jax.vmap(partial(pack_rows, experts_all=EXPERTS, capacity=CAP))
    cot_rows, inp_rows, slot_ids = packer(cotangent.reshape(N_SP, TOK_DEV, D), moe_input.reshape(N_SP, TOK_DEV, D), group_weight.reshape(N_SP, TOK_DEV), expert_weight.reshape(N_SP, TOK_DEV, TOP), expert_ids.reshape(N_SP, TOK_DEV, TOP))

    def by_expert(rows):
        return rows.reshape(N_SP, EXPERTS, CAP, D).transpose(1, 0, 2, 3).reshape(EXPERTS, N_SP * CAP, D)

    grad_gate, grad_up, grad_down, entry_grad = lax.map(expert_grads, (by_expert(cot_rows), by_expert(inp_rows), gate_weight, up_weight, down_weight))
    returned = entry_grad.reshape(EXPERTS, N_SP, CAP, D).transpose(1, 0, 2, 3).reshape(N_SP, EXPERTS * CAP, D)

    def pick_rows(rows, indices):
        return rows[indices]

    picked = jax.vmap(pick_rows)(returned, slot_ids)
    moe_grad = jnp.sum(picked.astype(jnp.float32).reshape(SEQUENCE_TOKENS, TOP, D), axis=1)
    resid_grad = (cotangent.astype(jnp.float32) + moe_grad).astype(jnp.bfloat16)
    grad_proj = jnp.dot(resid_grad.T, mixer_out, preferred_element_type=jnp.float32)
    out_grad = jnp.dot(proj_weight.T, resid_grad.T, preferred_element_type=jnp.float32)
    query_heads = queries.astype(jnp.float32).reshape(RETENTION_HEADS, KD, SEQUENCE_TOKENS)
    key_heads = key_vectors.astype(jnp.float32).reshape(RETENTION_HEADS, KD, SEQUENCE_TOKENS)
    value_heads = value_vectors.astype(jnp.float32).reshape(RETENTION_HEADS, VD, SEQUENCE_TOKENS)
    grad_heads = out_grad.reshape(RETENTION_HEADS, VD, SEQUENCE_TOKENS)
    query_grad, key_grad, value_grad = lax.map(head_grads, (query_heads, key_heads, value_heads, grad_heads, decay_rates))
    return (grad_gate, grad_up, grad_down, grad_proj, query_grad.reshape(RETENTION_HEADS * KD, SEQUENCE_TOKENS), key_grad.reshape(RETENTION_HEADS * KD, SEQUENCE_TOKENS), value_grad.reshape(RETENTION_HEADS * VD, SEQUENCE_TOKENS))
```

```python
import jax
import jax.numpy as jnp
from jax import lax
from jax.experimental import pallas as pl
from jax.experimental.pallas import tpu as pltpu
from jax.sharding import Mesh
from jax.sharding import PartitionSpec as P

BF = jnp.bfloat16
F32 = jnp.float32
NZ = 16
NT = 16
CAP = 12
TOK = 128
COL = 128
KD = 64
VD = 128
SP = ("z", "c")
HIGHEST = lax.Precision.HIGHEST
SWAP = [(0, 1), (1, 0)]

NN = (((1,), (0,)), ((), ()))
NTR = (((1,), (1,)), ((), ()))
TN = (((0,), (0,)), ((), ()))


def mm(a, b, dims=NN):
    return lax.dot_general(a, b, dims, preferred_element_type=F32)


def exact(a, b, dims=NN):
    return lax.dot_general(a, b, dims, precision=HIGHEST, preferred_element_type=F32)


def vmem():
    return pl.BlockSpec(memory_space=pltpu.VMEM)


def smem():
    return pl.BlockSpec(memory_space=pltpu.SMEM)


def call(kernel, outs, args, name, flops=1 << 27):
    return pl.pallas_call(
        kernel,
        out_shape=outs,
        in_specs=[smem()] + [vmem()] * (len(args) - 1),
        out_specs=jax.tree.map(lambda _: vmem(), outs),
        name=name,
        cost_estimate=pl.CostEstimate(flops=flops, bytes_accessed=1 << 20, transcendentals=0),
    )(*args)


def arr(shape, dtype):
    return jax.ShapeDtypeStruct(shape, dtype)


def placement(ids, wanted, rank):
    first = ids[0:1, :] == wanted
    match = first | (ids[1:2, :] == wanted)
    tok = TOK
    before = lax.broadcasted_iota(jnp.int32, (tok, tok), 0) < lax.broadcasted_iota(
        jnp.int32, (tok, tok), 1
    )
    ranks = mm(jnp.where(match, 1.0, 0.0).astype(BF), jnp.where(before, 1.0, 0.0).astype(BF))
    return match & (ranks == rank.astype(F32)), first


def rows_of(stride, shift, mul, core):
    n = lax.broadcasted_iota(jnp.int32, (NZ * stride, TOK), 0)
    z = lax.shift_right_logical(n * mul, shift)
    q = n - stride * z
    keep = jnp.where(q < CAP, 2 * z + core, -1)
    send = jnp.where((q >= CAP) & (q < 2 * CAP), 2 * z + 1 - core, -1)
    return keep, q, send, q - CAP


def pack_kernel(s_ref, ids_ref, gw_ref, ew_ref, cot_ref, inp_ref, keep_ref, send_ref):
    ids = ids_ref[...]
    weights = gw_ref[...] * ew_ref[...]
    cot, inp = cot_ref[...], inp_ref[...]
    ek, rk, es, rs = rows_of(2 * CAP, 16, 2731, s_ref[1])
    for wanted, rank, out in ((ek, rk, keep_ref), (es, rs, send_ref)):
        hit, first = placement(ids, wanted, rank)
        scale = jnp.sum(
            jnp.where(hit, jnp.where(first, weights[0:1, :], weights[1:2, :]), 0.0),
            axis=1,
            keepdims=True,
        )
        take = jnp.where(hit, 1.0, 0.0).astype(BF)
        out[:, 0 : 2 * CAP, :] = mm(take, inp).reshape(NZ, 2 * CAP, COL).astype(BF)
        out[:, 2 * CAP : 4 * CAP, :] = (
            (mm(take, cot) * scale).reshape(NZ, 2 * CAP, COL).astype(BF)
        )


def early_kernel(
    s_ref, ids_ref, rate_ref, q_ref, k_ref, v_ref,
    keep_ref, send_ref, piece_ref, weight_ref, mixed_ref, scores_ref, kv_ref,
):
    ek, rk, es, rs = rows_of(32, 5, 1, s_ref[1])
    ids = ids_ref[...]
    for wanted, rank, out in ((ek, rk, keep_ref), (es, rs, send_ref)):
        hit, _ = placement(ids, wanted, rank)
        out[...] = jnp.where(hit, 1.0, 0.0).astype(BF)
    rates = rate_ref[...]
    upto = lax.broadcasted_iota(jnp.int32, (TOK, TOK), 1) <= lax.broadcasted_iota(
        jnp.int32, (TOK, TOK), 0
    )
    col = jnp.broadcast_to(
        jnp.sum(jnp.where(upto, rates, 0.0), axis=1, keepdims=True), (TOK, TOK)
    )
    row = col.T
    total = jnp.sum(rates, axis=1, keepdims=True)
    prefix = row[0:1, :]
    start = jnp.exp(-prefix)
    end = jnp.exp(jnp.minimum(prefix - total, 0.0))
    mixed = KD ** (-0.5) * jnp.exp(-jnp.abs(col - row))
    mixed_ref[...] = mixed
    query, key, value = q_ref[...], k_ref[...], v_ref[...]
    scores_ref[...] = mm(query, key, TN) * mixed
    weight_ref[...] = jnp.concatenate(
        [start, end, jnp.broadcast_to(total, (1, TOK)), jnp.zeros((5, TOK), F32)], axis=0
    )
    keys = key.astype(F32)
    values = value.astype(F32)
    kv_ref[0] = exact(keys * end, values, NTR)
    kv_ref[1] = exact(keys * start, values, NTR)
    hi = jnp.broadcast_to(total, (8, TOK)).astype(BF).astype(F32)
    mid = (total - hi).astype(BF).astype(F32)
    low = total - hi - mid
    number = lax.broadcasted_iota(jnp.int32, (8, TOK), 0)
    piece_ref[...] = jnp.where(
        number == 0, hi, jnp.where(number == 1, mid, jnp.where(number == 2, low, 0.0))
    ).astype(BF)


def expert_kernel(s_ref, x_ref, gw_ref, uw_ref, dw_ref, part_ref, hid_ref, both_ref):
    inp = jnp.concatenate([x_ref[t, 0] for t in range(NT)], axis=1)
    cot = jnp.concatenate([x_ref[t, 1] for t in range(NT)], axis=1)
    both_w = jnp.concatenate([gw_ref[...], uw_ref[...]], axis=1)
    pre = mm(inp, both_w)
    gate, up = pre[:, :128], pre[:, 128:]
    hidden_grad = mm(cot, dw_ref[...], NTR)
    sig = jax.nn.sigmoid(gate)
    act = gate * sig
    hid_ref[...] = (act * up).astype(BF)
    gate_grad = (hidden_grad * up * sig * (1.0 + gate * (1.0 - sig))).astype(BF)
    up_grad = (hidden_grad * act).astype(BF)
    both = jnp.concatenate([gate_grad, up_grad], axis=1)
    both_ref[...] = both
    for t in range(0, NT, 2):
        out = mm(both, both_w[t * COL : (t + 2) * COL], NTR).astype(BF)
        part_ref[t] = out[:, :COL]
        part_ref[t + 1] = out[:, COL:]


def weight_kernel(s_ref, x_ref, hid_ref, both_ref, gg_ref, gu_ref, gd_ref):
    both = both_ref[...]
    hidden = hid_ref[...]
    for t in range(0, NT, 2):
        rows = slice(t * COL, (t + 2) * COL)
        inp = jnp.concatenate([x_ref[t, 0], x_ref[t + 1, 0]], axis=1)
        cot = jnp.concatenate([x_ref[t, 1], x_ref[t + 1, 1]], axis=1)
        out = mm(inp, both, TN).astype(BF)
        gg_ref[rows, :] = out[:, :128]
        gu_ref[rows, :] = out[:, 128:]
        gd_ref[:, rows] = mm(hidden, cot, TN).astype(BF)


def sum_kernel(s_ref, part_ref, piece_ref, out_ref):
    total = part_ref[0].astype(F32)
    for t in range(1, NT):
        total = total + part_ref[t].astype(F32)
    out_ref[:, 0 : 2 * CAP, :] = total.reshape(NZ, 2 * CAP, COL).astype(BF)
    out_ref[:, 2 * CAP : 32, :] = jnp.broadcast_to(piece_ref[...][None], (NZ, 8, COL))


def resid_kernel(s_ref, keep_ref, send_ref, own_ref, other_ref, cot_ref, out_ref):
    moe = mm(keep_ref[...], own_ref[...], TN) + mm(send_ref[...], other_ref[...], TN)
    resid = (cot_ref[...].astype(F32) + moe).astype(BF)
    for t in range(NT):
        out_ref[t] = resid


def proj_kernel(
    s_ref, r_ref, p_ref, mixer_ref, q_ref, weight_ref, kv_ref,
    og_ref, keep_ref, send_ref, state_ref,
):
    core = s_ref[1]
    resid = jnp.concatenate([r_ref[t] for t in range(NT)], axis=1)
    out_grad = mm(resid, p_ref[...])
    og_ref[...] = out_grad
    query = q_ref[...].astype(F32)
    early = exact(query * weight_ref[1:2, :], out_grad)
    late = exact(query * weight_ref[0:1, :], out_grad)
    state_ref[0] = early
    state_ref[1] = late
    send_ref[16] = early.astype(BF)
    send_ref[17] = late.astype(BF)
    send_ref[18] = kv_ref[0].astype(BF)
    send_ref[19] = kv_ref[1].astype(BF)
    mixer = mixer_ref[...]
    for t in range(NT):
        share = mm(r_ref[t], mixer, TN)
        low, high = share[:64], share[64:]
        keep_ref[t] = jnp.where(core == 0, low, high)
        send_ref[t] = jnp.where(core == 0, high, low).astype(BF)


def decays(own_ref, other_ref):
    def total(ref):
        rows = ref[:, 2 * CAP : 32, :].astype(F32)
        return rows[:, 0, :] + rows[:, 1, :] + rows[:, 2, :]

    return total(own_ref), total(other_ref)


def row_at(table, place):
    number = lax.broadcasted_iota(jnp.int32, table.shape, 0)
    return jnp.sum(jnp.where(number == place, table, 0.0), axis=0, keepdims=True)


def chip_kernel(s_ref, keep_ref, got_ref, state_ref, kv_ref, own_ref, other_ref, out_ref):
    place, core = s_ref[0], s_ref[1]
    own, other = decays(own_ref, other_ref)
    mine = jnp.exp(-row_at(own, place))
    theirs = jnp.exp(-row_at(other, place))
    is_first = core == 0
    early_own, early_other = jnp.where(is_first, theirs, 1.0), jnp.where(is_first, 1.0, mine)
    late_own, late_other = jnp.where(is_first, 1.0, theirs), jnp.where(is_first, mine, 1.0)

    def halves(mine_ref, at):
        early = mine_ref[0] * early_own + got_ref[at].astype(F32) * early_other
        late = mine_ref[1] * late_own + got_ref[at + 1].astype(F32) * late_other
        return [jnp.where(is_first, a[:32], a[32:]) for a in (early, late)]

    pairs = [jnp.concatenate(p, axis=0).astype(BF) for p in zip(halves(state_ref, 16), halves(kv_ref, 18))]
    for z in range(NZ):
        out_ref[z, 0:64, :] = (keep_ref[z] + got_ref[z].astype(F32)).astype(BF)
        out_ref[z, 64:128, :] = jnp.where(z > place, pairs[0], pairs[1])


def gather_kernel(s_ref, got_ref, own_ref, other_ref, proj_ref, state_ref):
    place = s_ref[0]
    own, other = decays(own_ref, other_ref)
    chip = own + other
    number = lax.broadcasted_iota(jnp.int32, (NZ, COL), 0)
    between = jnp.zeros((NZ, COL), F32)
    for u in range(NZ):
        inside = ((number < u) & (u < place)) | ((number > u) & (u > place))
        between = between + jnp.where(inside, chip[u : u + 1, :], 0.0)
    weight = jnp.exp(-between)
    early_w = jnp.where(number < place, weight, 0.0)
    late_w = jnp.where(number > place, weight, 0.0)
    share = got_ref[0, 0:64, :].astype(F32)
    state = got_ref[0, 64:128, :].astype(F32)
    early, late = state * early_w[0:1, :], state * late_w[0:1, :]
    for z in range(1, NZ):
        share = share + got_ref[z, 0:64, :].astype(F32)
        state = got_ref[z, 64:128, :].astype(F32)
        early = early + state * early_w[z : z + 1, :]
        late = late + state * late_w[z : z + 1, :]
    proj_ref[...] = share
    state_ref[0] = early
    state_ref[1] = late


def final_kernel(
    s_ref, far_ref, got_ref, og_ref, mixed_ref, scores_ref, weight_ref, q_ref, k_ref, v_ref,
    own_ref, other_ref, gq_ref, gk_ref, gv_ref,
):
    place, core = s_ref[0], s_ref[1]
    is_first = core == 0
    _, other = decays(own_ref, other_ref)
    theirs = jnp.exp(-row_at(other, place))
    early_w, late_w = jnp.where(is_first, 1.0, theirs), jnp.where(is_first, theirs, 1.0)
    early_add, late_add = jnp.where(is_first, 0.0, 1.0), jnp.where(is_first, 1.0, 0.0)

    def state(way, at, w, add):
        far = jnp.concatenate([far_ref[0, way, at : at + 32], far_ref[1, way, at : at + 32]], axis=0)
        near = got_ref[(16 if at == 0 else 18) + way].astype(F32)
        return far * w + near * add

    qd_early, kv_early = [state(0, at, early_w, early_add) for at in (0, 32)]
    qd_late, kv_late = [state(1, at, late_w, late_add) for at in (0, 32)]
    scale = KD ** (-0.5)
    low = scale * weight_ref[0:1, :]
    high = scale * weight_ref[1:2, :]
    out_grad = og_ref[...]
    query, key, value = [r[...].astype(F32) for r in (q_ref, k_ref, v_ref)]
    score_grad = exact(out_grad, value) * mixed_ref[...]
    gq_ref[...] = (
        exact(key, score_grad, NTR)
        + low * exact(kv_early, out_grad, NTR)
        + high * exact(kv_late, out_grad, NTR)
    )
    gk_ref[...] = (
        exact(query, score_grad) + low * exact(qd_early, value) + high * exact(qd_late, value)
    )
    gv_ref[...] = (
        exact(out_grad, scores_ref[...], TN)
        + low * exact(qd_early, key, TN)
        + high * exact(qd_late, key, TN)
    )


def to_all(shard, axis):
    copies = jnp.broadcast_to(shard, (lax.axis_size(axis), *shard.shape))
    return exchange(copies, axis)


def exchange(blocks, axis):
    return lax.all_to_all(blocks, axis, split_axis=0, concat_axis=0, tiled=True)


def on_device(
    cotangent, moe_input, expert_ids, group_weight, expert_weight, mixer_out,
    queries, key_vectors, value_vectors, decay_rates, proj_weight,
    gate_weight, up_weight, down_weight,
):
    place, core, part = [lax.axis_index(a).astype(jnp.int32) for a in ("z", "c", "tp")]
    where = jnp.stack([place, core, part])
    ids = expert_ids.T
    cot = lax.dynamic_slice_in_dim(cotangent, part * COL, COL, 1)
    inp = lax.dynamic_slice_in_dim(moe_input, part * COL, COL, 1)

    keep, send = call(
        pack_kernel,
        [arr((NZ, 4 * CAP, COL), BF)] * 2,
        (where, ids, group_weight.reshape(1, TOK), expert_weight.T, cot, inp),
        "pack",
    )
    rows = keep + lax.ppermute(send, "c", SWAP)
    rows = exchange(rows, "z")
    rows = rows.reshape(NZ, 2, 2 * CAP, COL).transpose(1, 0, 2, 3).reshape(2, NZ * 2 * CAP, COL)
    rows = to_all(rows, "tp")

    pick_keep, pick_send, piece, weight, mixed, scores, kv = call(
        early_kernel,
        [
            arr((NZ * 32, TOK), BF), arr((NZ * 32, TOK), BF), arr((8, TOK), BF), arr((8, TOK), F32),
            arr((TOK, TOK), F32), arr((TOK, TOK), F32), arr((2, KD, VD), F32),
        ],
        (where, ids, decay_rates, queries, key_vectors, value_vectors),
        "early",
    )

    shares, hidden, both = call(
        expert_kernel,
        [arr((NT, 384, COL), BF), arr((384, 128), BF), arr((384, 256), BF)],
        (where, rows, gate_weight[0], up_weight[0], down_weight[0]),
        "expert",
    )
    grad_gate, grad_up, grad_down = call(
        weight_kernel,
        [arr((2048, 128), BF), arr((2048, 128), BF), arr((128, 2048), BF)],
        (where, rows, hidden, both),
        "weights",
        1 << 29,
    )
    shares = exchange(shares, "tp")
    back = call(sum_kernel, arr((NZ, 32, COL), BF), (where, shares, piece), "sums")
    own = exchange(back, "z")
    other = lax.ppermute(own, "c", SWAP)
    resid = call(
        resid_kernel,
        arr((NT, TOK, COL), BF),
        (
            where, pick_keep, pick_send,
            own.reshape(NZ * 32, COL), other.reshape(NZ * 32, COL), cot,
        ),
        "resid",
    )
    resid = exchange(resid, "tp")
    out_grad, proj_keep, proj_send, state = call(
        proj_kernel,
        [
            arr((TOK, VD), F32), arr((NZ, 64, COL), F32), arr((20, 64, COL), BF),
            arr((2, KD, VD), F32),
        ],
        (where, resid, proj_weight, mixer_out, queries, weight, kv),
        "proj",
    )
    got = lax.ppermute(proj_send, "c", SWAP)
    chip = call(
        chip_kernel,
        arr((NZ, 128, COL), BF),
        (where, proj_keep, got, state, kv, own, other),
        "chip",
    )
    chip = exchange(chip, "z")
    grad_proj, far = call(
        gather_kernel,
        [arr((64, COL), F32), arr((2, 64, COL), F32)],
        (where, chip, own, other),
        "gather",
    )
    far = lax.all_gather(far, "c")
    grad_queries, grad_keys, grad_values = call(
        final_kernel,
        [arr((KD, TOK), F32), arr((KD, TOK), F32), arr((VD, TOK), F32)],
        (
            where, far, got, out_grad, mixed, scores, weight,
            queries, key_vectors, value_vectors, own, other,
        ),
        "final",
    )
    return (
        grad_gate[None], grad_up[None], grad_down[None],
        grad_proj, grad_queries, grad_keys, grad_values,
    )


def solution(mesh):
    finer = Mesh(mesh.devices.reshape(NZ, 2, NT), ("z", "c", "tp"))
    in_specs = (
        P(SP, None), P(SP, None), P(SP, None), P(SP), P(SP, None), P(SP, "tp"),
        P("tp", SP), P("tp", SP), P("tp", SP), P("tp", SP), P(None, "tp"),
        P(SP, None, "tp"), P(SP, None, "tp"), P(SP, "tp", None),
    )
    out_specs = (
        P(SP, None, "tp"), P(SP, None, "tp"), P(SP, "tp", None), P(SP, "tp"),
        P("tp", SP), P("tp", SP), P("tp", SP),
    )
    return jax.shard_map(
        on_device, mesh=finer, in_specs=in_specs, out_specs=out_specs, check_vma=False
    )
```

```python
import jax
import jax.numpy as jnp
from jax import lax
from jax.experimental import pallas as pl
from jax.experimental.pallas import tpu as pltpu
from jax.sharding import Mesh
from jax.sharding import PartitionSpec as P

BF = jnp.bfloat16
F32 = jnp.float32
NZ = 16
NT = 16
CAP = 12
TOK = 128
COL = 128
KD = 64
VD = 128
SP = ("z", "c")
HIGHEST = lax.Precision.HIGHEST
SWAP = [(0, 1), (1, 0)]

NN = (((1,), (0,)), ((), ()))
NTR = (((1,), (1,)), ((), ()))
TN = (((0,), (0,)), ((), ()))


def mm(a, b, dims=NN):
    return lax.dot_general(a, b, dims, preferred_element_type=F32)


def exact(a, b, dims=NN):
    return lax.dot_general(a, b, dims, precision=HIGHEST, preferred_element_type=F32)


def vmem():
    return pl.BlockSpec(memory_space=pltpu.VMEM)


def call(kernel, outs, args, name, mib=4, flops=1 << 27):
    return pl.pallas_call(
        kernel,
        out_shape=outs,
        in_specs=[vmem()] * len(args),
        out_specs=jax.tree.map(lambda _: vmem(), outs),
        name=name,
        compiler_params=pltpu.CompilerParams(vmem_limit_bytes=mib << 20),
        cost_estimate=pl.CostEstimate(flops=flops, bytes_accessed=1 << 20, transcendentals=0),
    )(*args)


def spot(axis):
    return lax.axis_index(axis).astype(jnp.int32)


def arr(shape, dtype):
    return jax.ShapeDtypeStruct(shape, dtype)


def placement(ids, wanted, rank):
    first = ids[0:1, :] == wanted
    match = first | (ids[1:2, :] == wanted)
    tok = TOK
    before = lax.broadcasted_iota(jnp.int32, (tok, tok), 0) < lax.broadcasted_iota(
        jnp.int32, (tok, tok), 1
    )
    ranks = mm(jnp.where(match, 1.0, 0.0).astype(BF), jnp.where(before, 1.0, 0.0).astype(BF))
    return match & (ranks == rank.astype(F32)), first


def rows_of(stride, shift, mul, core):
    n = lax.broadcasted_iota(jnp.int32, (NZ * stride, TOK), 0)
    z = lax.shift_right_logical(n * mul, shift)
    q = n - stride * z
    keep = jnp.where(q < CAP, 2 * z + core, -1)
    send = jnp.where((q >= CAP) & (q < 2 * CAP), 2 * z + 1 - core, -1)
    return keep, q, send, q - CAP


def pack_kernel(ids_ref, gw_ref, ew_ref, cot_ref, inp_ref, keep_ref, send_ref, cols_ref):
    ids = ids_ref[...]
    weights = gw_ref[...] * ew_ref[...]
    here = pl.ds(pl.multiple_of(spot("tp") * COL, COL), COL)
    cot, inp = cot_ref[:, here], inp_ref[:, here]
    cols_ref[...] = cot
    ek, rk, es, rs = rows_of(2 * CAP, 16, 2731, spot("c"))
    for wanted, rank, out in ((ek, rk, keep_ref), (es, rs, send_ref)):
        hit, first = placement(ids, wanted, rank)
        scale = jnp.sum(
            jnp.where(hit, jnp.where(first, weights[0:1, :], weights[1:2, :]), 0.0),
            axis=1,
            keepdims=True,
        )
        take = jnp.where(hit, 1.0, 0.0).astype(BF)
        out[:, 0 : 2 * CAP, :] = mm(take, inp).reshape(NZ, 2 * CAP, COL).astype(BF)
        out[:, 2 * CAP : 4 * CAP, :] = (
            (mm(take, cot) * scale).reshape(NZ, 2 * CAP, COL).astype(BF)
        )


def early_kernel(
    ids_ref, rate_ref, q_ref, k_ref, v_ref,
    keep_ref, send_ref, piece_ref, weight_ref, mixed_ref, scores_ref, kv_ref,
):
    ek, rk, es, rs = rows_of(32, 5, 1, spot("c"))
    ids = ids_ref[...]
    for wanted, rank, out in ((ek, rk, keep_ref), (es, rs, send_ref)):
        hit, _ = placement(ids, wanted, rank)
        out[...] = jnp.where(hit, 1.0, 0.0).astype(BF)
    rates = rate_ref[...]
    upto = lax.broadcasted_iota(jnp.int32, (TOK, TOK), 1) <= lax.broadcasted_iota(
        jnp.int32, (TOK, TOK), 0
    )
    col = jnp.broadcast_to(
        jnp.sum(jnp.where(upto, rates, 0.0), axis=1, keepdims=True), (TOK, TOK)
    )
    row = col.T
    total = jnp.sum(rates, axis=1, keepdims=True)
    prefix = row[0:1, :]
    start = jnp.exp(-prefix)
    end = jnp.exp(jnp.minimum(prefix - total, 0.0))
    mixed = KD ** (-0.5) * jnp.exp(-jnp.abs(col - row))
    mixed_ref[...] = mixed
    query, key, value = q_ref[...], k_ref[...], v_ref[...]
    scores_ref[...] = mm(query, key, TN) * mixed
    weight_ref[...] = jnp.concatenate(
        [start, end, jnp.broadcast_to(total, (1, TOK)), jnp.zeros((5, TOK), F32)], axis=0
    )
    keys = key.astype(F32)
    values = value.astype(F32)
    kv_ref[0] = exact(keys * end, values, NTR)
    kv_ref[1] = exact(keys * start, values, NTR)
    hi = jnp.broadcast_to(total, (8, TOK)).astype(BF).astype(F32)
    mid = (total - hi).astype(BF).astype(F32)
    low = total - hi - mid
    number = lax.broadcasted_iota(jnp.int32, (8, TOK), 0)
    piece_ref[...] = jnp.where(
        number == 0, hi, jnp.where(number == 1, mid, jnp.where(number == 2, low, 0.0))
    ).astype(BF)


def expert_kernel(x_ref, gw_ref, uw_ref, dw_ref, part_ref, hid_ref, both_ref):
    inp = jnp.concatenate([x_ref[held_at(t), 0] for t in range(NT)], axis=1)
    cot = jnp.concatenate([x_ref[held_at(t), 1] for t in range(NT)], axis=1)
    both_w = jnp.concatenate([gw_ref[...], uw_ref[...]], axis=1)
    pre = mm(inp, both_w)
    gate, up = pre[:, :128], pre[:, 128:]
    hidden_grad = mm(cot, dw_ref[...], NTR)
    sig = jax.nn.sigmoid(gate)
    act = gate * sig
    hid_ref[...] = (act * up).astype(BF)
    gate_grad = (hidden_grad * up * sig * (1.0 + gate * (1.0 - sig))).astype(BF)
    up_grad = (hidden_grad * act).astype(BF)
    both = jnp.concatenate([gate_grad, up_grad], axis=1)
    both_ref[...] = both
    for t in range(0, NT, 2):
        out = mm(both, both_w[t * COL : (t + 2) * COL], NTR).astype(BF)
        part_ref[t] = out[:, :COL]
        part_ref[t + 1] = out[:, COL:]


def weight_kernel(x_ref, hid_ref, both_ref, gg_ref, gu_ref, gd_ref):
    both = both_ref[...]
    hidden = hid_ref[...]
    for t in range(0, NT, 2):
        rows = slice(t * COL, (t + 2) * COL)
        inp = jnp.concatenate([x_ref[held_at(t), 0], x_ref[held_at(t + 1), 0]], axis=1)
        cot = jnp.concatenate([x_ref[held_at(t), 1], x_ref[held_at(t + 1), 1]], axis=1)
        out = mm(inp, both, TN).astype(BF)
        gg_ref[rows, :] = out[:, :128]
        gu_ref[rows, :] = out[:, 128:]
        gd_ref[:, rows] = mm(hidden, cot, TN).astype(BF)


def sum_kernel(part_ref, piece_ref, out_ref):
    total = part_ref[0].astype(F32)
    for t in range(1, NT):
        total = total + part_ref[t].astype(F32)
    out_ref[:, 0 : 2 * CAP, :] = total.reshape(NZ, 2 * CAP, COL).astype(BF)
    out_ref[:, 2 * CAP : 32, :] = jnp.broadcast_to(piece_ref[...][None], (NZ, 8, COL))


def resid_kernel(keep_ref, send_ref, own_ref, other_ref, cot_ref, out_ref):
    moe = mm(keep_ref[...], own_ref[...], TN) + mm(send_ref[...], other_ref[...], TN)
    resid = (cot_ref[...].astype(F32) + moe).astype(BF)
    for t in range(NT):
        out_ref[t] = resid


def proj_kernel(
    r_ref, p_ref, mixer_ref, q_ref, weight_ref, kv_ref,
    og_ref, keep_ref, send_ref, state_ref,
):
    core = spot("c")
    resid = jnp.concatenate([r_ref[t] for t in range(NT)], axis=1)
    out_grad = mm(resid, p_ref[...])
    og_ref[...] = out_grad
    query = q_ref[...].astype(F32)
    early = exact(query * weight_ref[1:2, :], out_grad)
    late = exact(query * weight_ref[0:1, :], out_grad)
    state_ref[0] = early
    state_ref[1] = late
    send_ref[16] = early.astype(BF)
    send_ref[17] = late.astype(BF)
    send_ref[18] = kv_ref[0].astype(BF)
    send_ref[19] = kv_ref[1].astype(BF)
    mixer = mixer_ref[...]
    for t in range(NT):
        share = mm(r_ref[t], mixer, TN)
        low, high = share[:64], share[64:]
        keep_ref[t] = jnp.where(core == 0, low, high)
        send_ref[t] = jnp.where(core == 0, high, low).astype(BF)


def decays(own_ref, other_ref):
    def total(ref):
        rows = ref[:, 2 * CAP : 32, :].astype(F32)
        return rows[:, 0, :] + rows[:, 1, :] + rows[:, 2, :]

    return total(own_ref), total(other_ref)


def row_at(table, place):
    number = lax.broadcasted_iota(jnp.int32, table.shape, 0)
    return jnp.sum(jnp.where(number == place, table, 0.0), axis=0, keepdims=True)


def chip_kernel(keep_ref, got_ref, state_ref, kv_ref, own_ref, other_ref, out_ref):
    place, core = spot("z"), spot("c")
    own, other = decays(own_ref, other_ref)
    mine = jnp.exp(-row_at(own, place))
    theirs = jnp.exp(-row_at(other, place))
    is_first = core == 0
    early_own, early_other = jnp.where(is_first, theirs, 1.0), jnp.where(is_first, 1.0, mine)
    late_own, late_other = jnp.where(is_first, 1.0, theirs), jnp.where(is_first, mine, 1.0)

    def halves(mine_ref, at):
        early = mine_ref[0] * early_own + got_ref[at].astype(F32) * early_other
        late = mine_ref[1] * late_own + got_ref[at + 1].astype(F32) * late_other
        return [jnp.where(is_first, a[:32], a[32:]) for a in (early, late)]

    pairs = [jnp.concatenate(p, axis=0).astype(BF) for p in zip(halves(state_ref, 16), halves(kv_ref, 18))]
    for z in range(NZ):
        out_ref[z, 0:64, :] = (keep_ref[z] + got_ref[z].astype(F32)).astype(BF)
        out_ref[z, 64:128, :] = jnp.where(z > place, pairs[0], pairs[1])


def gather_kernel(got_ref, own_ref, other_ref, proj_ref, state_ref):
    place = spot("z")
    own, other = decays(own_ref, other_ref)
    chip = own + other
    number = lax.broadcasted_iota(jnp.int32, (NZ, COL), 0)
    between = jnp.zeros((NZ, COL), F32)
    for u in range(NZ):
        inside = ((number < u) & (u < place)) | ((number > u) & (u > place))
        between = between + jnp.where(inside, chip[u : u + 1, :], 0.0)
    weight = jnp.exp(-between)
    early_w = jnp.where(number < place, weight, 0.0)
    late_w = jnp.where(number > place, weight, 0.0)
    share = got_ref[0, 0:64, :].astype(F32)
    state = got_ref[0, 64:128, :].astype(F32)
    early, late = state * early_w[0:1, :], state * late_w[0:1, :]
    for z in range(1, NZ):
        share = share + got_ref[z, 0:64, :].astype(F32)
        state = got_ref[z, 64:128, :].astype(F32)
        early = early + state * early_w[z : z + 1, :]
        late = late + state * late_w[z : z + 1, :]
    proj_ref[...] = share
    state_ref[0] = early
    state_ref[1] = late


def final_kernel(
    far_ref, got_ref, og_ref, mixed_ref, scores_ref, weight_ref, q_ref, k_ref, v_ref,
    own_ref, other_ref, gq_ref, gk_ref, gv_ref,
):
    place, core = spot("z"), spot("c")
    is_first = core == 0
    _, other = decays(own_ref, other_ref)
    theirs = jnp.exp(-row_at(other, place))
    early_w, late_w = jnp.where(is_first, 1.0, theirs), jnp.where(is_first, theirs, 1.0)
    early_add, late_add = jnp.where(is_first, 0.0, 1.0), jnp.where(is_first, 1.0, 0.0)

    def state(way, at, w, add):
        far = jnp.concatenate([far_ref[0, way, at : at + 32], far_ref[1, way, at : at + 32]], axis=0)
        near = got_ref[(16 if at == 0 else 18) + way].astype(F32)
        return far * w + near * add

    qd_early, kv_early = [state(0, at, early_w, early_add) for at in (0, 32)]
    qd_late, kv_late = [state(1, at, late_w, late_add) for at in (0, 32)]
    scale = KD ** (-0.5)
    low = scale * weight_ref[0:1, :]
    high = scale * weight_ref[1:2, :]
    out_grad = og_ref[...]
    query, key, value = [r[...].astype(F32) for r in (q_ref, k_ref, v_ref)]
    score_grad = exact(out_grad, value) * mixed_ref[...]
    gq_ref[...] = (
        exact(key, score_grad, NTR)
        + low * exact(kv_early, out_grad, NTR)
        + high * exact(kv_late, out_grad, NTR)
    )
    gk_ref[...] = (
        exact(query, score_grad) + low * exact(qd_early, value) + high * exact(qd_late, value)
    )
    gv_ref[...] = (
        exact(out_grad, scores_ref[...], TN)
        + low * exact(qd_early, key, TN)
        + high * exact(qd_late, key, TN)
    )


def groups(step, stride, step_other, stride_other):
    first = [[stride * g + step * k for k in range(4)] for g in range(4)]
    second = [[16 + stride_other * g + step_other * k for k in range(4)] for g in range(4)]
    return first + second


def to_all(shard, axis, sets):
    copies = jnp.broadcast_to(shard, (len(sets[0]), *shard.shape))
    return lax.all_to_all(
        copies, axis, split_axis=0, concat_axis=0, axis_index_groups=sets, tiled=True
    )


def exchange(blocks, axis):
    return lax.all_to_all(blocks, axis, split_axis=0, concat_axis=0, tiled=True)


def held_at(t):
    return jnp.where(spot("c") == 0, (t % 4) * 4 + t // 4, t)


def on_device(
    cotangent, moe_input, expert_ids, group_weight, expert_weight, mixer_out,
    queries, key_vectors, value_vectors, decay_rates, proj_weight,
    gate_weight, up_weight, down_weight,
):
    ids = expert_ids.T
    keep, send, cot = call(
        pack_kernel,
        [arr((NZ, 4 * CAP, COL), BF)] * 2 + [arr((TOK, COL), BF)],
        (ids, group_weight.reshape(1, TOK), expert_weight.T, cotangent, moe_input),
        "pack",
    )
    rows = keep + lax.ppermute(send, "c", SWAP)
    rows = exchange(rows, "z")
    rows = rows.reshape(NZ, 2, 2 * CAP, COL).transpose(1, 0, 2, 3).reshape(2, NZ * 2 * CAP, COL)
    rows = to_all(rows, ("c", "tp"), groups(4, 1, 1, 4))
    rows = to_all(rows, ("c", "tp"), groups(1, 4, 4, 1))
    rows = rows.reshape(NT, 2, NZ * 2 * CAP, COL)

    pick_keep, pick_send, piece, weight, mixed, scores, kv = call(
        early_kernel,
        [
            arr((NZ * 32, TOK), BF), arr((NZ * 32, TOK), BF), arr((8, TOK), BF), arr((8, TOK), F32),
            arr((TOK, TOK), F32), arr((TOK, TOK), F32), arr((2, KD, VD), F32),
        ],
        (ids, decay_rates, queries, key_vectors, value_vectors),
        "early",
    )

    shares, hidden, both = call(
        expert_kernel,
        [arr((NT, 384, COL), BF), arr((384, 128), BF), arr((384, 256), BF)],
        (rows, gate_weight[0], up_weight[0], down_weight[0]),
        "expert",
        20,
    )
    grad_gate, grad_up, grad_down = call(
        weight_kernel,
        [arr((2048, 128), BF), arr((2048, 128), BF), arr((128, 2048), BF)],
        (rows, hidden, both),
        "weights",
        16,
        1 << 29,
    )
    shares = exchange(shares, "tp")
    back = call(sum_kernel, arr((NZ, 32, COL), BF), (shares, piece), "sums", 6)
    own = exchange(back, "z")
    other = lax.ppermute(own, "c", SWAP)
    resid = call(
        resid_kernel,
        arr((NT, TOK, COL), BF),
        (
            pick_keep, pick_send,
            own.reshape(NZ * 32, COL), other.reshape(NZ * 32, COL), cot,
        ),
        "resid",
        4,
    )
    resid = exchange(resid, "tp")
    out_grad, proj_keep, proj_send, state = call(
        proj_kernel,
        [
            arr((TOK, VD), F32), arr((NZ, 64, COL), F32), arr((20, 64, COL), BF),
            arr((2, KD, VD), F32),
        ],
        (resid, proj_weight, mixer_out, queries, weight, kv),
        "proj",
        8,
    )
    got = lax.ppermute(proj_send, "c", SWAP)
    chip = call(
        chip_kernel,
        arr((NZ, 128, COL), BF),
        (proj_keep, got, state, kv, own, other),
        "chip",
    )
    chip = exchange(chip, "z")
    grad_proj, far = call(
        gather_kernel,
        [arr((64, COL), F32), arr((2, 64, COL), F32)],
        (chip, own, other),
        "gather",
    )
    far = lax.all_gather(far, "c")
    grad_queries, grad_keys, grad_values = call(
        final_kernel,
        [arr((KD, TOK), F32), arr((KD, TOK), F32), arr((VD, TOK), F32)],
        (
            far, got, out_grad, mixed, scores, weight,
            queries, key_vectors, value_vectors, own, other,
        ),
        "final",
    )
    return (
        grad_gate[None], grad_up[None], grad_down[None],
        grad_proj, grad_queries, grad_keys, grad_values,
    )


def solution(mesh):
    finer = Mesh(mesh.devices.reshape(NZ, 2, NT), ("z", "c", "tp"))
    in_specs = (
        P(SP, None), P(SP, None), P(SP, None), P(SP), P(SP, None), P(SP, "tp"),
        P("tp", SP), P("tp", SP), P("tp", SP), P("tp", SP), P(None, "tp"),
        P(SP, None, "tp"), P(SP, None, "tp"), P(SP, "tp", None),
    )
    out_specs = (
        P(SP, None, "tp"), P(SP, None, "tp"), P(SP, "tp", None), P(SP, "tp"),
        P("tp", SP), P("tp", SP), P("tp", SP),
    )
    return jax.shard_map(
        on_device, mesh=finer, in_specs=in_specs, out_specs=out_specs, check_vma=False
    )
```

```python
import jax
import jax.numpy as jnp
from jax import lax
from jax.experimental import pallas as pl
from jax.experimental.pallas import tpu as pltpu
from jax.sharding import Mesh
from jax.sharding import PartitionSpec as P

BF = jnp.bfloat16
F32 = jnp.float32
NZ = 16
NT = 16
CAP = 12
TOK = 128
COL = 128
KD = 64
VD = 128
SP = ("z", "c")
HIGHEST = lax.Precision.HIGHEST
SWAP = [(0, 1), (1, 0)]

NN = (((1,), (0,)), ((), ()))
NTR = (((1,), (1,)), ((), ()))
TN = (((0,), (0,)), ((), ()))


def mm(a, b, dims=NN):
    return lax.dot_general(a, b, dims, preferred_element_type=F32)


def exact(a, b, dims=NN):
    return lax.dot_general(a, b, dims, precision=HIGHEST, preferred_element_type=F32)


def vmem():
    return pl.BlockSpec(memory_space=pltpu.VMEM)


def hbm():
    return pl.BlockSpec(memory_space=pltpu.HBM)


def call(kernel, outs, args, name, mib=4, flops=1 << 27, stay=0, scratch=()):
    return pl.pallas_call(
        kernel,
        out_shape=outs,
        in_specs=[hbm()] * stay + [vmem()] * (len(args) - stay),
        out_specs=jax.tree.map(lambda _: vmem(), outs),
        scratch_shapes=scratch,
        name=name,
        compiler_params=pltpu.CompilerParams(vmem_limit_bytes=mib << 20),
        cost_estimate=pl.CostEstimate(flops=flops, bytes_accessed=1 << 20, transcendentals=0),
    )(*args)


def spot(axis):
    return lax.axis_index(axis).astype(jnp.int32)


def fetch(sources, targets, sems):
    copies = [
        pltpu.make_async_copy(src, dst, sems.at[n])
        for n, (src, dst) in enumerate(zip(sources, targets))
    ]
    for copy in copies:
        copy.start()
    for copy in copies:
        copy.wait()


def arr(shape, dtype):
    return jax.ShapeDtypeStruct(shape, dtype)


def placement(ids, wanted, rank):
    first = ids[0:1, :] == wanted
    match = first | (ids[1:2, :] == wanted)
    tok = TOK
    before = lax.broadcasted_iota(jnp.int32, (tok, tok), 0) < lax.broadcasted_iota(
        jnp.int32, (tok, tok), 1
    )
    ranks = mm(jnp.where(match, 1.0, 0.0).astype(BF), jnp.where(before, 1.0, 0.0).astype(BF))
    return match & (ranks == rank.astype(F32)), first


def rows_of(stride, shift, mul, core):
    n = lax.broadcasted_iota(jnp.int32, (NZ * stride, TOK), 0)
    z = lax.shift_right_logical(n * mul, shift)
    q = n - stride * z
    keep = jnp.where(q < CAP, 2 * z + core, -1)
    send = jnp.where((q >= CAP) & (q < 2 * CAP), 2 * z + 1 - core, -1)
    return keep, q, send, q - CAP


def decay_parts(rates):
    upto = lax.broadcasted_iota(jnp.int32, (TOK, TOK), 1) <= lax.broadcasted_iota(
        jnp.int32, (TOK, TOK), 0
    )
    col = jnp.broadcast_to(
        jnp.sum(jnp.where(upto, rates, 0.0), axis=1, keepdims=True), (TOK, TOK)
    )
    row = col.T
    total = jnp.sum(rates, axis=1, keepdims=True)
    prefix = row[0:1, :]
    start = jnp.exp(-prefix)
    end = jnp.exp(jnp.minimum(prefix - total, 0.0))
    return col, row, start, end, jnp.broadcast_to(total, (1, TOK))


def in_pieces(total):
    hi = jnp.broadcast_to(total, (8, TOK)).astype(BF).astype(F32)
    mid = (total - hi).astype(BF).astype(F32)
    low = total - hi - mid
    number = lax.broadcasted_iota(jnp.int32, (8, TOK), 0)
    return jnp.where(
        number == 0, hi, jnp.where(number == 1, mid, jnp.where(number == 2, low, 0.0))
    ).astype(BF)


def pack_kernel(
    ids_in, gw_in, ew_in, cot_in, inp_in, rate_in, k_in, v_in,
    keep_ref, send_ref, cols_ref, mine_ref,
    ids_ref, gw_ref, ew_ref, inp_ref, rate_ref, k_ref, v_ref, sems,
):
    here = pl.ds(pl.multiple_of(spot("tp") * COL, COL), COL)
    fetch(
        (ids_in, gw_in, ew_in, cot_in.at[:, here], inp_in.at[:, here], rate_in, k_in, v_in),
        (ids_ref, gw_ref, ew_ref, cols_ref, inp_ref, rate_ref, k_ref, v_ref),
        sems,
    )
    ids = ids_ref[...]
    weights = gw_ref[...] * ew_ref[...]
    cot, inp = cols_ref[...], inp_ref[...]
    ek, rk, es, rs = rows_of(2 * CAP, 16, 2731, spot("c"))
    for wanted, rank, out in ((ek, rk, keep_ref), (es, rs, send_ref)):
        hit, first = placement(ids, wanted, rank)
        scale = jnp.sum(
            jnp.where(hit, jnp.where(first, weights[0:1, :], weights[1:2, :]), 0.0),
            axis=1,
            keepdims=True,
        )
        take = jnp.where(hit, 1.0, 0.0).astype(BF)
        inp_rows = mm(take, inp)
        cot_rows = mm(take, cot) * scale
        for z in range(NZ):
            part = slice(2 * CAP * z, 2 * CAP * (z + 1))
            at = 4 * CAP * z
            out[at : at + 2 * CAP, :] = inp_rows[part].astype(BF)
            out[at + 2 * CAP : at + 4 * CAP, :] = cot_rows[part].astype(BF)
    _, _, start, end, total = decay_parts(rate_ref[...])
    keys, values = k_ref[...].astype(F32), v_ref[...].astype(F32)
    early = exact(keys * end, values, NTR)
    late = exact(keys * start, values, NTR)
    mine_ref[0:64, :] = early
    mine_ref[64:128, :] = late
    mine_ref[128:136, :] = jnp.broadcast_to(total, (8, TOK))
    send_ref[768:832, :] = early.astype(BF)
    send_ref[832:896, :] = late.astype(BF)
    send_ref[896:904, :] = in_pieces(total)
    send_ref[904:912, :] = jnp.zeros((8, TOK), BF)


def table_kernel(ids_in, rate_in, q_in, k_in, picks_ref, table_ref, ids_ref, rate_ref, q_ref, k_ref, sems):
    fetch((ids_in, rate_in, q_in, k_in), (ids_ref, rate_ref, q_ref, k_ref), sems)
    ek, rk, es, rs = rows_of(32, 5, 1, spot("c"))
    ids = ids_ref[...]
    for wanted, rank, at in ((ek, rk, 0), (es, rs, 512)):
        hit, _ = placement(ids, wanted, rank)
        picks_ref[at : at + 512, :] = jnp.where(hit, 1.0, 0.0).astype(BF)
    col, row, start, end, _ = decay_parts(rate_ref[...])
    mixed = KD ** (-0.5) * jnp.exp(-jnp.abs(col - row))
    table_ref[0:128, :] = mixed
    table_ref[128:256, :] = mm(q_ref[...], k_ref[...], TN) * mixed
    table_ref[256:264, :] = jnp.concatenate([start, end, jnp.zeros((6, TOK), F32)], axis=0)


def expert_kernel(x_ref, gw_ref, uw_ref, dw_ref, part_ref, hid_ref, both_ref):
    inp = jnp.concatenate([x_ref[held_at(t), 0] for t in range(NT)], axis=1)
    cot = jnp.concatenate([x_ref[held_at(t), 1] for t in range(NT)], axis=1)
    both_w = jnp.concatenate([gw_ref[...], uw_ref[...]], axis=1)
    pre = mm(inp, both_w)
    gate, up = pre[:, :128], pre[:, 128:]
    hidden_grad = mm(cot, dw_ref[...], NTR)
    sig = jax.nn.sigmoid(gate)
    act = gate * sig
    hid_ref[...] = (act * up).astype(BF)
    gate_grad = (hidden_grad * up * sig * (1.0 + gate * (1.0 - sig))).astype(BF)
    up_grad = (hidden_grad * act).astype(BF)
    both = jnp.concatenate([gate_grad, up_grad], axis=1)
    both_ref[...] = both
    for t in range(0, NT, 2):
        out = mm(both, both_w[t * COL : (t + 2) * COL], NTR).astype(BF)
        part_ref[t] = out[:, :COL]
        part_ref[t + 1] = out[:, COL:]


def weight_kernel(x_ref, hid_ref, both_ref, gg_ref, gu_ref, gd_ref):
    both = both_ref[...]
    hidden = hid_ref[...]
    for t in range(0, NT, 2):
        rows = slice(t * COL, (t + 2) * COL)
        inp = jnp.concatenate([x_ref[held_at(t), 0], x_ref[held_at(t + 1), 0]], axis=1)
        cot = jnp.concatenate([x_ref[held_at(t), 1], x_ref[held_at(t + 1), 1]], axis=1)
        out = mm(inp, both, TN).astype(BF)
        gg_ref[rows, :] = out[:, :128]
        gu_ref[rows, :] = out[:, 128:]
        gd_ref[:, rows] = mm(hidden, cot, TN).astype(BF)


def chip_states(early, late, early_other, late_other, mine, theirs):
    is_first = spot("c") == 0
    both_early = early * jnp.where(is_first, theirs, 1.0) + early_other * jnp.where(
        is_first, 1.0, mine
    )
    both_late = late * jnp.where(is_first, 1.0, theirs) + late_other * jnp.where(
        is_first, mine, 1.0
    )
    return [jnp.where(is_first, a[:32], a[32:]).astype(BF) for a in (both_early, both_late)]


def sum_kernel(part_ref, mine_ref, extra_ref, out_ref):
    total = part_ref[0].astype(F32)
    for t in range(1, NT):
        total = total + part_ref[t].astype(F32)
    out_ref[:, 0 : 2 * CAP, :] = total.reshape(NZ, 2 * CAP, COL).astype(BF)
    decay = mine_ref[128:129, :]
    out_ref[:, 2 * CAP : 32, :] = jnp.broadcast_to(in_pieces(decay)[None], (NZ, 8, COL))
    pieces = extra_ref[128:136, :].astype(F32)
    theirs = pieces[0:1, :] + pieces[1:2, :] + pieces[2:3, :]
    early, late = chip_states(
        mine_ref[0:64, :], mine_ref[64:128, :],
        extra_ref[0:64, :].astype(F32), extra_ref[64:128, :].astype(F32),
        jnp.exp(-decay), jnp.exp(-theirs),
    )
    place = spot("z")
    for z in range(NZ):
        out_ref[z, 32:64, :] = jnp.where(z > place, early, late)


def resid_kernel(picks_ref, own_ref, other_ref, cols_ref, out_ref):
    own = own_ref[:, 0:32, :].reshape(512, COL)
    other = other_ref[:, 0:32, :].reshape(512, COL)
    moe = mm(picks_ref[0:512, :], own, TN) + mm(picks_ref[512:1024, :], other, TN)
    resid = (cols_ref[...].astype(F32) + moe).astype(BF)
    for t in range(NT):
        out_ref[t] = resid


def proj_kernel(r_ref, p_ref, mixer_ref, q_ref, table_ref, og_ref, keep_ref, send_ref, state_ref):
    core = spot("c")
    resid = jnp.concatenate([r_ref[t] for t in range(NT)], axis=1)
    out_grad = mm(resid, p_ref[...])
    og_ref[...] = out_grad
    query = q_ref[...].astype(F32)
    early = exact(query * table_ref[257:258, :], out_grad)
    late = exact(query * table_ref[256:257, :], out_grad)
    state_ref[0] = early
    state_ref[1] = late
    send_ref[16] = early.astype(BF)
    send_ref[17] = late.astype(BF)
    mixer = mixer_ref[...]
    for t in range(NT):
        share = mm(r_ref[t], mixer, TN)
        low, high = share[:64], share[64:]
        keep_ref[t] = jnp.where(core == 0, low, high)
        send_ref[t] = jnp.where(core == 0, high, low).astype(BF)


def decays(own_ref, other_ref):
    def total(ref):
        rows = ref[:, 2 * CAP : 32, :].astype(F32)
        return rows[:, 0, :] + rows[:, 1, :] + rows[:, 2, :]

    return total(own_ref), total(other_ref)


def row_at(table, place):
    number = lax.broadcasted_iota(jnp.int32, table.shape, 0)
    return jnp.sum(jnp.where(number == place, table, 0.0), axis=0, keepdims=True)


def at_block(far_early, far_late, near, theirs):
    is_first = spot("c") == 0
    early = far_early * jnp.where(is_first, 1.0, theirs) + jnp.where(is_first, 0.0, near)
    late = far_late * jnp.where(is_first, theirs, 1.0) + jnp.where(is_first, near, 0.0)
    return early, late


def intra_kernel(
    og_ref, table_ref, q_ref, k_ref, v_ref, own_ref, other_ref, extra_ref,
    gq_ref, part_ref, weight_ref,
):
    place, core = spot("z"), spot("c")
    own, other = decays(own_ref, other_ref)
    chip = own + other
    number = lax.broadcasted_iota(jnp.int32, (NZ, COL), 0)
    between = jnp.zeros((NZ, COL), F32)
    for u in range(NZ):
        inside = ((number < u) & (u < place)) | ((number > u) & (u > place))
        between = between + jnp.where(inside, chip[u : u + 1, :], 0.0)
    weight = jnp.exp(-between)
    early_w = jnp.where(number < place, weight, 0.0)
    late_w = jnp.where(number > place, weight, 0.0)
    weight_ref[0:16, :] = early_w
    weight_ref[16:32, :] = late_w

    def far(ref):
        early = late = jnp.zeros((32, COL), F32)
        for z in range(NZ):
            state = ref[z, 32:64, :].astype(F32)
            early = early + state * early_w[z : z + 1, :]
            late = late + state * late_w[z : z + 1, :]
        return early, late

    is_first = core == 0
    here, there = far(own_ref), far(other_ref)
    far_early, far_late = [
        jnp.concatenate([jnp.where(is_first, a, b), jnp.where(is_first, b, a)], axis=0)
        for a, b in zip(here, there)
    ]
    near = jnp.where(is_first, extra_ref[64:128, :], extra_ref[0:64, :]).astype(F32)
    theirs = jnp.exp(-row_at(other, place))
    kv_early, kv_late = at_block(far_early, far_late, near, theirs)
    scale = KD ** (-0.5)
    low = scale * table_ref[256:257, :]
    high = scale * table_ref[257:258, :]
    out_grad = og_ref[...]
    query, key, value = [r[...].astype(F32) for r in (q_ref, k_ref, v_ref)]
    score_grad = exact(out_grad, value) * table_ref[0:128, :]
    gq_ref[...] = (
        exact(key, score_grad, NTR)
        + low * exact(kv_early, out_grad, NTR)
        + high * exact(kv_late, out_grad, NTR)
    )
    part_ref[0:64, :] = exact(query, score_grad)
    part_ref[64:192, :] = exact(out_grad, table_ref[128:256, :], TN)
    part_ref[192:256, :] = key
    part_ref[256:384, :] = value
    part_ref[384:392, :] = jnp.concatenate([low, high, theirs, jnp.zeros((5, TOK), F32)], axis=0)


def chip_kernel(keep_ref, got_ref, state_ref, own_ref, other_ref, out_ref, near_ref):
    place, core = spot("z"), spot("c")
    own, other = decays(own_ref, other_ref)
    mine = jnp.exp(-row_at(own, place))
    theirs = jnp.exp(-row_at(other, place))
    early_other, late_other = got_ref[16].astype(F32), got_ref[17].astype(F32)
    early, late = chip_states(state_ref[0], state_ref[1], early_other, late_other, mine, theirs)
    near_ref[...] = jnp.where(core == 0, late_other, early_other)
    for z in range(NZ):
        out_ref[z, 0:64, :] = (keep_ref[z] + got_ref[z].astype(F32)).astype(BF)
        out_ref[z, 64:96, :] = jnp.where(z > place, early, late)


def gather_kernel(got_ref, weight_ref, proj_ref, state_ref):
    share = jnp.zeros((64, COL), F32)
    early = late = jnp.zeros((32, COL), F32)
    for z in range(NZ):
        share = share + got_ref[z, 0:64, :].astype(F32)
        state = got_ref[z, 64:96, :].astype(F32)
        early = early + state * weight_ref[z : z + 1, :]
        late = late + state * weight_ref[16 + z : 17 + z, :]
    proj_ref[...] = share
    state_ref[0] = early
    state_ref[1] = late


def final_kernel(far_ref, near_ref, part_ref, gk_ref, gv_ref):
    early, late = at_block(
        jnp.concatenate([far_ref[0, 0], far_ref[1, 0]], axis=0),
        jnp.concatenate([far_ref[0, 1], far_ref[1, 1]], axis=0),
        near_ref[...],
        part_ref[386:387, :],
    )
    low, high = part_ref[384:385, :], part_ref[385:386, :]
    key, value = part_ref[192:256, :], part_ref[256:384, :]
    gk_ref[...] = part_ref[0:64, :] + low * exact(early, value) + high * exact(late, value)
    gv_ref[...] = part_ref[64:192, :] + low * exact(early, key, TN) + high * exact(late, key, TN)


def groups(step, stride, step_other, stride_other):
    first = [[stride * g + step * k for k in range(4)] for g in range(4)]
    second = [[16 + stride_other * g + step_other * k for k in range(4)] for g in range(4)]
    return first + second


def to_all(shard, axis, sets):
    copies = jnp.broadcast_to(shard, (len(sets[0]), *shard.shape))
    return lax.all_to_all(
        copies, axis, split_axis=0, concat_axis=0, axis_index_groups=sets, tiled=True
    )


def exchange(blocks, axis):
    return lax.all_to_all(blocks, axis, split_axis=0, concat_axis=0, tiled=True)


def held_at(t):
    return jnp.where(spot("c") == 0, (t % 4) * 4 + t // 4, t)


def on_device(
    cotangent, moe_input, expert_ids, group_weight, expert_weight, mixer_out,
    queries, key_vectors, value_vectors, decay_rates, proj_weight,
    gate_weight, up_weight, down_weight,
):
    ids = expert_ids.T
    keep, send, cols, mine = call(
        pack_kernel,
        [arr((768, COL), BF), arr((912, COL), BF), arr((TOK, COL), BF), arr((136, TOK), F32)],
        (
            ids, group_weight.reshape(1, TOK), expert_weight.T, cotangent, moe_input,
            decay_rates, key_vectors, value_vectors,
        ),
        "pack",
        60,
        stay=8,
        scratch=[
            pltpu.VMEM((2, TOK), jnp.int32), pltpu.VMEM((1, TOK), F32), pltpu.VMEM((2, TOK), F32),
            pltpu.VMEM((TOK, COL), BF), pltpu.VMEM((1, TOK), F32), pltpu.VMEM((KD, TOK), BF),
            pltpu.VMEM((VD, TOK), BF), pltpu.SemaphoreType.DMA((8,)),
        ],
    )
    picks, table = call(
        table_kernel,
        [arr((1024, TOK), BF), arr((264, TOK), F32)],
        (ids, decay_rates, queries, key_vectors),
        "table",
        60,
        stay=4,
        scratch=[
            pltpu.VMEM((2, TOK), jnp.int32), pltpu.VMEM((1, TOK), F32), pltpu.VMEM((KD, TOK), BF),
            pltpu.VMEM((KD, TOK), BF), pltpu.SemaphoreType.DMA((4,)),
        ],
    )
    swapped = lax.ppermute(send, "c", SWAP)
    extra = swapped[768:]
    rows = (keep + swapped[:768]).reshape(NZ, 4 * CAP, COL)
    rows, picks, table, extra = lax.optimization_barrier((rows, picks, table, extra))
    rows = exchange(rows, "z")
    rows = rows.reshape(NZ, 2, 2 * CAP, COL).transpose(1, 0, 2, 3).reshape(2, NZ * 2 * CAP, COL)
    rows = to_all(rows, ("c", "tp"), groups(4, 1, 1, 4))
    rows = to_all(rows, ("c", "tp"), groups(1, 4, 4, 1))
    rows = rows.reshape(NT, 2, NZ * 2 * CAP, COL)
    shares, hidden, both = call(
        expert_kernel,
        [arr((NT, 384, COL), BF), arr((384, 128), BF), arr((384, 256), BF)],
        (rows, gate_weight[0], up_weight[0], down_weight[0]),
        "expert",
        20,
    )
    shares = exchange(shares, "tp")
    back = call(sum_kernel, arr((NZ, 64, COL), BF), (shares, mine, extra), "sums", 6)
    own = exchange(back, "z")
    own, rows, hidden, both = lax.optimization_barrier((own, rows, hidden, both))
    other = lax.ppermute(own, "c", SWAP)
    grad_gate, grad_up, grad_down = call(
        weight_kernel,
        [arr((2048, 128), BF), arr((2048, 128), BF), arr((128, 2048), BF)],
        (rows, hidden, both),
        "weights",
        16,
        1 << 29,
    )
    resid = call(resid_kernel, arr((NT, TOK, COL), BF), (picks, own, other, cols), "resid")
    resid, grad_gate, grad_up, grad_down = lax.optimization_barrier(
        (resid, grad_gate, grad_up, grad_down)
    )
    resid = exchange(resid, "tp")
    out_grad, proj_keep, proj_send, state = call(
        proj_kernel,
        [
            arr((TOK, VD), F32), arr((NZ, 64, COL), F32), arr((18, 64, COL), BF),
            arr((2, KD, VD), F32),
        ],
        (resid, proj_weight, mixer_out, queries, table),
        "proj",
        8,
    )
    got = lax.ppermute(proj_send, "c", SWAP)
    grad_queries, part, weight = call(
        intra_kernel,
        [arr((KD, TOK), F32), arr((392, TOK), F32), arr((32, TOK), F32)],
        (out_grad, table, queries, key_vectors, value_vectors, own, other, extra),
        "intra",
    )
    chip, near = call(
        chip_kernel,
        [arr((NZ, 96, COL), BF), arr((KD, VD), F32)],
        (proj_keep, got, state, own, other),
        "chip",
    )
    chip, grad_queries, part, weight = lax.optimization_barrier((chip, grad_queries, part, weight))
    chip = exchange(chip, "z")
    grad_proj, far = call(
        gather_kernel,
        [arr((64, COL), F32), arr((2, 32, COL), F32)],
        (chip, weight),
        "gather",
    )
    far = lax.all_gather(far, "c")
    grad_keys, grad_values = call(
        final_kernel,
        [arr((KD, TOK), F32), arr((VD, TOK), F32)],
        (far, near, part),
        "final",
    )
    return (
        grad_gate[None], grad_up[None], grad_down[None],
        grad_proj, grad_queries, grad_keys, grad_values,
    )


def solution(mesh):
    finer = Mesh(mesh.devices.reshape(NZ, 2, NT), ("z", "c", "tp"))
    in_specs = (
        P(SP, None), P(SP, None), P(SP, None), P(SP), P(SP, None), P(SP, "tp"),
        P("tp", SP), P("tp", SP), P("tp", SP), P("tp", SP), P(None, "tp"),
        P(SP, None, "tp"), P(SP, None, "tp"), P(SP, "tp", None),
    )
    out_specs = (
        P(SP, None, "tp"), P(SP, None, "tp"), P(SP, "tp", None), P(SP, "tp"),
        P("tp", SP), P("tp", SP), P("tp", SP),
    )
    return jax.shard_map(
        on_device, mesh=finer, in_specs=in_specs, out_specs=out_specs, check_vma=False
    )
```

```python
import jax
import jax.numpy as jnp
from jax import lax
from jax.experimental import pallas as pl
from jax.experimental.pallas import tpu as pltpu
from jax.sharding import Mesh
from jax.sharding import PartitionSpec as P

BF = jnp.bfloat16
F32 = jnp.float32
NZ = 16
NT = 16
CAP = 12
TOK = 128
COL = 128
KD = 64
VD = 128
SP = ("z", "c")
SWAP = [(0, 1), (1, 0)]

NN = (((1,), (0,)), ((), ()))
NTR = (((1,), (1,)), ((), ()))
TN = (((0,), (0,)), ((), ()))


def mm(a, b, dims=NN):
    return lax.dot_general(a, b, dims, preferred_element_type=F32)


def halves(a):
    high = a.astype(BF)
    return high, (a - high.astype(F32)).astype(BF)


def exact(a, b, dims=NN):
    if a.dtype == BF:
        high, low = halves(b)
        return mm(a, high, dims) + mm(a, low, dims)
    high, low = halves(a)
    if b.dtype == BF:
        return mm(high, b, dims) + mm(low, b, dims)
    other, rest = halves(b)
    return mm(high, other, dims) + (mm(high, rest, dims) + mm(low, other, dims))


def vmem():
    return pl.BlockSpec(memory_space=pltpu.VMEM)


def hbm():
    return pl.BlockSpec(memory_space=pltpu.HBM)


def call(kernel, outs, args, name, mib=4, flops=1 << 27, stay=0, scratch=()):
    return pl.pallas_call(
        kernel,
        out_shape=outs,
        in_specs=[hbm()] * stay + [vmem()] * (len(args) - stay),
        out_specs=jax.tree.map(lambda _: vmem(), outs),
        scratch_shapes=scratch,
        name=name,
        compiler_params=pltpu.CompilerParams(vmem_limit_bytes=mib << 20),
        cost_estimate=pl.CostEstimate(flops=flops, bytes_accessed=1 << 20, transcendentals=0),
    )(*args)


def spot(axis):
    return lax.axis_index(axis).astype(jnp.int32)


def fetch(sources, targets, sems):
    copies = [
        pltpu.make_async_copy(src, dst, sems.at[n])
        for n, (src, dst) in enumerate(zip(sources, targets))
    ]
    for copy in copies:
        copy.start()
    for copy in copies:
        copy.wait()


def arr(shape, dtype):
    return jax.ShapeDtypeStruct(shape, dtype)


def placement(ids, wanted, rank):
    first = ids[0:1, :] == wanted
    match = first | (ids[1:2, :] == wanted)
    tok = TOK
    before = lax.broadcasted_iota(jnp.int32, (tok, tok), 0) < lax.broadcasted_iota(
        jnp.int32, (tok, tok), 1
    )
    ranks = mm(jnp.where(match, 1.0, 0.0).astype(BF), jnp.where(before, 1.0, 0.0).astype(BF))
    return match & (ranks == rank.astype(F32)), first


def rows_of(stride, shift, mul, core):
    n = lax.broadcasted_iota(jnp.int32, (NZ * stride, TOK), 0)
    z = lax.shift_right_logical(n * mul, shift)
    q = n - stride * z
    keep = jnp.where(q < CAP, 2 * z + core, -1)
    send = jnp.where((q >= CAP) & (q < 2 * CAP), 2 * z + 1 - core, -1)
    return keep, q, send, q - CAP


def decay_parts(rates):
    upto = lax.broadcasted_iota(jnp.int32, (TOK, TOK), 1) <= lax.broadcasted_iota(
        jnp.int32, (TOK, TOK), 0
    )
    col = jnp.broadcast_to(
        jnp.sum(jnp.where(upto, rates, 0.0), axis=1, keepdims=True), (TOK, TOK)
    )
    row = col.T
    total = jnp.sum(rates, axis=1, keepdims=True)
    prefix = row[0:1, :]
    start = jnp.exp(-prefix)
    end = jnp.exp(jnp.minimum(prefix - total, 0.0))
    return col, row, start, end, jnp.broadcast_to(total, (1, TOK))


def in_pieces(total):
    hi = jnp.broadcast_to(total, (8, TOK)).astype(BF).astype(F32)
    mid = (total - hi).astype(BF).astype(F32)
    low = total - hi - mid
    number = lax.broadcasted_iota(jnp.int32, (8, TOK), 0)
    return jnp.where(
        number == 0, hi, jnp.where(number == 1, mid, jnp.where(number == 2, low, 0.0))
    ).astype(BF)


def pack_kernel(
    ids_in, gw_in, ew_in, cot_in, inp_in, rate_in, k_in, v_in,
    keep_ref, send_ref, cols_ref, mine_ref,
    ids_ref, gw_ref, ew_ref, inp_ref, rate_ref, k_ref, v_ref, sems,
):
    here = pl.ds(pl.multiple_of(spot("tp") * COL, COL), COL)
    fetch(
        (ids_in, gw_in, ew_in, cot_in.at[:, here], inp_in.at[:, here], rate_in, k_in, v_in),
        (ids_ref, gw_ref, ew_ref, cols_ref, inp_ref, rate_ref, k_ref, v_ref),
        sems,
    )
    ids = ids_ref[...]
    weights = gw_ref[...] * ew_ref[...]
    cot, inp = cols_ref[...], inp_ref[...]
    ek, rk, es, rs = rows_of(2 * CAP, 16, 2731, spot("c"))
    for wanted, rank, out in ((ek, rk, keep_ref), (es, rs, send_ref)):
        hit, first = placement(ids, wanted, rank)
        scale = jnp.sum(
            jnp.where(hit, jnp.where(first, weights[0:1, :], weights[1:2, :]), 0.0),
            axis=1,
            keepdims=True,
        )
        take = jnp.where(hit, 1.0, 0.0).astype(BF)
        inp_rows = mm(take, inp)
        cot_rows = mm(take, cot) * scale
        for z in range(NZ):
            part = slice(2 * CAP * z, 2 * CAP * (z + 1))
            at = 4 * CAP * z
            out[at : at + 2 * CAP, :] = inp_rows[part].astype(BF)
            out[at + 2 * CAP : at + 4 * CAP, :] = cot_rows[part].astype(BF)
    _, _, start, end, total = decay_parts(rate_ref[...])
    keys, values = k_ref[...].astype(F32), v_ref[...]
    early = exact(keys * end, values, NTR)
    late = exact(keys * start, values, NTR)
    mine_ref[0:64, :] = early
    mine_ref[64:128, :] = late
    mine_ref[128:136, :] = jnp.concatenate([total, start, end, jnp.zeros((5, TOK), F32)], axis=0)
    send_ref[768:832, :] = early.astype(BF)
    send_ref[832:896, :] = late.astype(BF)
    send_ref[896:904, :] = in_pieces(total)
    send_ref[904:912, :] = jnp.zeros((8, TOK), BF)


def merge_kernel(keep_ref, got_ref, rows_ref, extra_ref):
    for z in range(NZ):
        part = slice(4 * CAP * z, 4 * CAP * (z + 1))
        rows_ref[z] = keep_ref[part, :] + got_ref[part, :]
    extra_ref[...] = got_ref[768:912, :]


def picks_kernel(keep_in, ids_ref, picks_ref, keep_ref, sem):
    copy = pltpu.make_async_copy(keep_in, keep_ref, sem)
    copy.start()
    ek, rk, es, rs = rows_of(32, 5, 1, spot("c"))
    ids = ids_ref[...]
    for wanted, rank, at in ((ek, rk, 0), (es, rs, 512)):
        hit, _ = placement(ids, wanted, rank)
        picks_ref[at : at + 512, :] = jnp.where(hit, 1.0, 0.0).astype(BF)
    copy.wait()


def expert_kernel(x_ref, gw_ref, uw_ref, dw_ref, part_ref, hid_ref, both_ref):
    inp = jnp.concatenate([x_ref[held_at(t), 0] for t in range(NT)], axis=1)
    cot = jnp.concatenate([x_ref[held_at(t), 1] for t in range(NT)], axis=1)
    both_w = jnp.concatenate([gw_ref[...], uw_ref[...]], axis=1)
    pre = mm(inp, both_w)
    gate, up = pre[:, :128], pre[:, 128:]
    hidden_grad = mm(cot, dw_ref[...], NTR)
    sig = jax.nn.sigmoid(gate)
    act = gate * sig
    hid_ref[...] = (act * up).astype(BF)
    gate_grad = (hidden_grad * up * sig * (1.0 + gate * (1.0 - sig))).astype(BF)
    up_grad = (hidden_grad * act).astype(BF)
    both = jnp.concatenate([gate_grad, up_grad], axis=1)
    both_ref[...] = both
    for t in range(0, NT, 2):
        out = mm(both, both_w[t * COL : (t + 2) * COL], NTR).astype(BF)
        part_ref[t] = out[:, :COL]
        part_ref[t + 1] = out[:, COL:]


def weight_kernel(x_ref, hid_ref, both_ref, gg_ref, gu_ref, gd_ref):
    both = both_ref[...]
    hidden = hid_ref[...]
    for t in range(0, NT, 2):
        rows = slice(t * COL, (t + 2) * COL)
        inp = jnp.concatenate([x_ref[held_at(t), 0], x_ref[held_at(t + 1), 0]], axis=1)
        cot = jnp.concatenate([x_ref[held_at(t), 1], x_ref[held_at(t + 1), 1]], axis=1)
        out = mm(inp, both, TN).astype(BF)
        gg_ref[rows, :] = out[:, :128]
        gu_ref[rows, :] = out[:, 128:]
        gd_ref[:, rows] = mm(hidden, cot, TN).astype(BF)


def chip_states(early, late, early_other, late_other, mine, theirs):
    is_first = spot("c") == 0
    both_early = early * jnp.where(is_first, theirs, 1.0) + early_other * jnp.where(
        is_first, 1.0, mine
    )
    both_late = late * jnp.where(is_first, 1.0, theirs) + late_other * jnp.where(
        is_first, mine, 1.0
    )
    return [jnp.where(is_first, a[:32], a[32:]).astype(BF) for a in (both_early, both_late)]


def sum_kernel(part_ref, mine_ref, extra_ref, out_ref):
    total = part_ref[0].astype(F32)
    for t in range(1, NT):
        total = total + part_ref[t].astype(F32)
    out_ref[:, 0 : 2 * CAP, :] = total.reshape(NZ, 2 * CAP, COL).astype(BF)
    decay = mine_ref[128:129, :]
    out_ref[:, 2 * CAP : 32, :] = jnp.broadcast_to(in_pieces(decay)[None], (NZ, 8, COL))
    pieces = extra_ref[128:136, :].astype(F32)
    theirs = pieces[0:1, :] + pieces[1:2, :] + pieces[2:3, :]
    early, late = chip_states(
        mine_ref[0:64, :], mine_ref[64:128, :],
        extra_ref[0:64, :].astype(F32), extra_ref[64:128, :].astype(F32),
        jnp.exp(-decay), jnp.exp(-theirs),
    )
    place = spot("z")
    for z in range(NZ):
        out_ref[z, 32:64, :] = jnp.where(z > place, early, late)


def resid_kernel(picks_ref, own_ref, other_ref, cols_ref, out_ref):
    own = own_ref[:, 0:32, :].reshape(512, COL)
    other = other_ref[:, 0:32, :].reshape(512, COL)
    moe = mm(picks_ref[0:512, :], own, TN) + mm(picks_ref[512:1024, :], other, TN)
    resid = (cols_ref[...].astype(F32) + moe).astype(BF)
    for t in range(NT):
        out_ref[t] = resid


def proj_kernel(r_ref, p_ref, mixer_ref, q_ref, mine_ref, og_ref, keep_ref, send_ref, state_ref):
    core = spot("c")
    resid = jnp.concatenate([r_ref[t] for t in range(NT)], axis=1)
    out_grad = mm(resid, p_ref[...])
    og_ref[...] = out_grad
    query = q_ref[...].astype(F32)
    early = exact(query * mine_ref[130:131, :], out_grad)
    late = exact(query * mine_ref[129:130, :], out_grad)
    state_ref[0] = early
    state_ref[1] = late
    send_ref[16] = early.astype(BF)
    send_ref[17] = late.astype(BF)
    mixer = mixer_ref[...]
    for t in range(NT):
        share = mm(r_ref[t], mixer, TN)
        low, high = share[:64], share[64:]
        keep_ref[t] = jnp.where(core == 0, low, high)
        send_ref[t] = jnp.where(core == 0, high, low).astype(BF)


def decays(own_ref, other_ref):
    def total(ref):
        rows = ref[:, 2 * CAP : 32, :].astype(F32)
        return rows[:, 0, :] + rows[:, 1, :] + rows[:, 2, :]

    return total(own_ref), total(other_ref)


def row_at(table, place):
    number = lax.broadcasted_iota(jnp.int32, table.shape, 0)
    return jnp.sum(jnp.where(number == place, table, 0.0), axis=0, keepdims=True)


def at_block(far_early, far_late, near, theirs):
    is_first = spot("c") == 0
    early = far_early * jnp.where(is_first, 1.0, theirs) + jnp.where(is_first, 0.0, near)
    late = far_late * jnp.where(is_first, theirs, 1.0) + jnp.where(is_first, near, 0.0)
    return early, late


def intra_kernel(
    og_ref, rate_ref, q_ref, k_ref, v_ref, own_ref, other_ref, extra_ref,
    gq_ref, part_ref, weight_ref,
):
    place, core = spot("z"), spot("c")
    own, other = decays(own_ref, other_ref)
    chip = own + other
    number = lax.broadcasted_iota(jnp.int32, (NZ, COL), 0)
    between = jnp.zeros((NZ, COL), F32)
    for u in range(NZ):
        inside = ((number < u) & (u < place)) | ((number > u) & (u > place))
        between = between + jnp.where(inside, chip[u : u + 1, :], 0.0)
    weight = jnp.exp(-between)
    early_w = jnp.where(number < place, weight, 0.0)
    late_w = jnp.where(number > place, weight, 0.0)
    weight_ref[0:16, :] = early_w
    weight_ref[16:32, :] = late_w

    def far(ref):
        early = late = jnp.zeros((32, COL), F32)
        for z in range(NZ):
            state = ref[z, 32:64, :].astype(F32)
            early = early + state * early_w[z : z + 1, :]
            late = late + state * late_w[z : z + 1, :]
        return early, late

    is_first = core == 0
    here, there = far(own_ref), far(other_ref)
    far_early, far_late = [
        jnp.concatenate([jnp.where(is_first, a, b), jnp.where(is_first, b, a)], axis=0)
        for a, b in zip(here, there)
    ]
    near = jnp.where(is_first, extra_ref[64:128, :], extra_ref[0:64, :]).astype(F32)
    theirs = jnp.exp(-row_at(other, place))
    kv_early, kv_late = at_block(far_early, far_late, near, theirs)
    scale = KD ** (-0.5)
    col, row, start, end, _ = decay_parts(rate_ref[...])
    low, high = scale * start, scale * end
    mixed = scale * jnp.exp(-jnp.abs(col - row))
    out_grad = og_ref[...]
    query, key, value = q_ref[...], k_ref[...], v_ref[...]
    score_grad = exact(out_grad, value) * mixed
    gq_ref[...] = (
        exact(key, score_grad, NTR)
        + low * exact(kv_early, out_grad, NTR)
        + high * exact(kv_late, out_grad, NTR)
    )
    part_ref[0:64, :] = exact(query, score_grad)
    part_ref[64:192, :] = exact(out_grad, mm(query, key, TN) * mixed, TN)
    part_ref[192:256, :] = key.astype(F32)
    part_ref[256:384, :] = value.astype(F32)
    part_ref[384:392, :] = jnp.concatenate([low, high, theirs, jnp.zeros((5, TOK), F32)], axis=0)


def chip_kernel(keep_ref, got_ref, state_ref, own_ref, other_ref, out_ref, near_ref):
    place, core = spot("z"), spot("c")
    own, other = decays(own_ref, other_ref)
    mine = jnp.exp(-row_at(own, place))
    theirs = jnp.exp(-row_at(other, place))
    early_other, late_other = got_ref[16].astype(F32), got_ref[17].astype(F32)
    early, late = chip_states(state_ref[0], state_ref[1], early_other, late_other, mine, theirs)
    near_ref[...] = jnp.where(core == 0, late_other, early_other)
    for z in range(NZ):
        out_ref[z, 0:64, :] = (keep_ref[z] + got_ref[z].astype(F32)).astype(BF)
        out_ref[z, 64:96, :] = jnp.where(z > place, early, late)


def gather_kernel(got_ref, weight_ref, state_ref):
    early = late = jnp.zeros((32, COL), F32)
    for z in range(NZ):
        state = got_ref[z, 64:96, :].astype(F32)
        early = early + state * weight_ref[z : z + 1, :]
        late = late + state * weight_ref[16 + z : 17 + z, :]
    state_ref[0] = early
    state_ref[1] = late


def final_kernel(far_ref, near_ref, part_ref, got_ref, proj_ref, gk_ref, gv_ref):
    share = jnp.zeros((64, COL), F32)
    for z in range(NZ):
        share = share + got_ref[z, 0:64, :].astype(F32)
    proj_ref[...] = share
    early, late = at_block(
        jnp.concatenate([far_ref[0, 0], far_ref[1, 0]], axis=0),
        jnp.concatenate([far_ref[0, 1], far_ref[1, 1]], axis=0),
        near_ref[...],
        part_ref[386:387, :],
    )
    low, high = part_ref[384:385, :], part_ref[385:386, :]
    key, value = part_ref[192:256, :].astype(BF), part_ref[256:384, :].astype(BF)
    gk_ref[...] = part_ref[0:64, :] + low * exact(early, value) + high * exact(late, value)
    gv_ref[...] = part_ref[64:192, :] + low * exact(early, key, TN) + high * exact(late, key, TN)


def groups(step, stride, step_other, stride_other):
    first = [[stride * g + step * k for k in range(4)] for g in range(4)]
    second = [[16 + stride_other * g + step_other * k for k in range(4)] for g in range(4)]
    return first + second


def to_all(shard, axis, sets):
    copies = jnp.broadcast_to(shard, (len(sets[0]), *shard.shape))
    return lax.all_to_all(
        copies, axis, split_axis=0, concat_axis=0, axis_index_groups=sets, tiled=True
    )


def exchange(blocks, axis):
    return lax.all_to_all(blocks, axis, split_axis=0, concat_axis=0, tiled=True)


def held_at(t):
    return jnp.where(spot("c") == 0, (t % 4) * 4 + t // 4, t)


def on_device(
    cotangent, moe_input, expert_ids, group_weight, expert_weight, mixer_out,
    queries, key_vectors, value_vectors, decay_rates, proj_weight,
    gate_weight, up_weight, down_weight,
):
    ids = expert_ids.T
    keep, send, cols, mine = call(
        pack_kernel,
        [arr((768, COL), BF), arr((912, COL), BF), arr((TOK, COL), BF), arr((136, TOK), F32)],
        (
            ids, group_weight.reshape(1, TOK), expert_weight.T, cotangent, moe_input,
            decay_rates, key_vectors, value_vectors,
        ),
        "pack",
        60,
        stay=8,
        scratch=[
            pltpu.VMEM((2, TOK), jnp.int32), pltpu.VMEM((1, TOK), F32), pltpu.VMEM((2, TOK), F32),
            pltpu.VMEM((TOK, COL), BF), pltpu.VMEM((1, TOK), F32), pltpu.VMEM((KD, TOK), BF),
            pltpu.VMEM((VD, TOK), BF), pltpu.SemaphoreType.DMA((8,)),
        ],
    )
    picks, keep = call(
        picks_kernel,
        [arr((1024, TOK), BF), arr((768, COL), BF)],
        (keep, ids),
        "picks",
        stay=1,
        scratch=[pltpu.SemaphoreType.DMA(())],
    )
    swapped = lax.ppermute(send, "c", SWAP)
    rows, extra = call(
        merge_kernel, [arr((NZ, 4 * CAP, COL), BF), arr((144, COL), BF)], (keep, swapped), "merge"
    )
    rows, picks, extra = lax.optimization_barrier((rows, picks, extra))
    rows = exchange(rows, "z")
    rows = rows.reshape(NZ, 2, 2 * CAP, COL).transpose(1, 0, 2, 3).reshape(2, NZ * 2 * CAP, COL)
    rows = to_all(rows, ("c", "tp"), groups(4, 1, 1, 4))
    rows = to_all(rows, ("c", "tp"), groups(1, 4, 4, 1))
    rows = rows.reshape(NT, 2, NZ * 2 * CAP, COL)
    shares, hidden, both = call(
        expert_kernel,
        [arr((NT, 384, COL), BF), arr((384, 128), BF), arr((384, 256), BF)],
        (rows, gate_weight[0], up_weight[0], down_weight[0]),
        "expert",
        20,
    )
    shares = exchange(shares, "tp")
    back = call(sum_kernel, arr((NZ, 64, COL), BF), (shares, mine, extra), "sums", 6)
    own = exchange(back, "z")
    own, rows, hidden, both = lax.optimization_barrier((own, rows, hidden, both))
    other = lax.ppermute(own, "c", SWAP)
    grad_gate, grad_up, grad_down = call(
        weight_kernel,
        [arr((2048, 128), BF), arr((2048, 128), BF), arr((128, 2048), BF)],
        (rows, hidden, both),
        "weights",
        16,
        1 << 29,
    )
    resid = call(resid_kernel, arr((NT, TOK, COL), BF), (picks, own, other, cols), "resid")
    resid, grad_gate, grad_up, grad_down = lax.optimization_barrier(
        (resid, grad_gate, grad_up, grad_down)
    )
    resid = exchange(resid, "tp")
    out_grad, proj_keep, proj_send, state = call(
        proj_kernel,
        [
            arr((TOK, VD), F32), arr((NZ, 64, COL), F32), arr((18, 64, COL), BF),
            arr((2, KD, VD), F32),
        ],
        (resid, proj_weight, mixer_out, queries, mine),
        "proj",
        8,
    )
    got = lax.ppermute(proj_send, "c", SWAP)
    grad_queries, part, weight = call(
        intra_kernel,
        [arr((KD, TOK), F32), arr((392, TOK), F32), arr((32, TOK), F32)],
        (out_grad, decay_rates, queries, key_vectors, value_vectors, own, other, extra),
        "intra",
    )
    chip, near = call(
        chip_kernel,
        [arr((NZ, 96, COL), BF), arr((KD, VD), F32)],
        (proj_keep, got, state, own, other),
        "chip",
    )
    chip, grad_queries, part, weight = lax.optimization_barrier((chip, grad_queries, part, weight))
    chip = exchange(chip, "z")
    far = call(gather_kernel, arr((2, 32, COL), F32), (chip, weight), "gather")
    far = lax.all_gather(far, "c")
    grad_proj, grad_keys, grad_values = call(
        final_kernel,
        [arr((64, COL), F32), arr((KD, TOK), F32), arr((VD, TOK), F32)],
        (far, near, part, chip),
        "final",
    )
    return (
        grad_gate[None], grad_up[None], grad_down[None],
        grad_proj, grad_queries, grad_keys, grad_values,
    )


def solution(mesh):
    finer = Mesh(mesh.devices.reshape(NZ, 2, NT), ("z", "c", "tp"))
    in_specs = (
        P(SP, None), P(SP, None), P(SP, None), P(SP), P(SP, None), P(SP, "tp"),
        P("tp", SP), P("tp", SP), P("tp", SP), P("tp", SP), P(None, "tp"),
        P(SP, None, "tp"), P(SP, None, "tp"), P(SP, "tp", None),
    )
    out_specs = (
        P(SP, None, "tp"), P(SP, None, "tp"), P(SP, "tp", None), P(SP, "tp"),
        P("tp", SP), P("tp", SP), P("tp", SP),
    )
    return jax.shard_map(
        on_device, mesh=finer, in_specs=in_specs, out_specs=out_specs, check_vma=False
    )
```

```python
import jax
import jax.numpy as jnp
from jax import lax
from jax.experimental import pallas as pl
from jax.experimental.pallas import tpu as pltpu
from jax.sharding import Mesh
from jax.sharding import PartitionSpec as P

BF = jnp.bfloat16
F32 = jnp.float32
NZ = 16
NT = 16
CAP = 12
TOK = 128
COL = 128
KD = 64
VD = 128
SP = ("z", "c")
SWAP = [(0, 1), (1, 0)]

NN = (((1,), (0,)), ((), ()))
NTR = (((1,), (1,)), ((), ()))
TN = (((0,), (0,)), ((), ()))


def mm(a, b, dims=NN):
    return lax.dot_general(a, b, dims, preferred_element_type=F32)


def halves(a):
    high = a.astype(BF)
    return high, (a - high.astype(F32)).astype(BF)


def exact(a, b, dims=NN):
    if a.dtype == BF:
        high, low = halves(b)
        return mm(a, high, dims) + mm(a, low, dims)
    high, low = halves(a)
    if b.dtype == BF:
        return mm(high, b, dims) + mm(low, b, dims)
    other, rest = halves(b)
    return mm(high, other, dims) + (mm(high, rest, dims) + mm(low, other, dims))


def vmem():
    return pl.BlockSpec(memory_space=pltpu.VMEM)


def hbm():
    return pl.BlockSpec(memory_space=pltpu.HBM)


def call(kernel, outs, args, name, mib=4, flops=1 << 27, stay=0, scratch=()):
    return pl.pallas_call(
        kernel,
        out_shape=outs,
        in_specs=[hbm()] * stay + [vmem()] * (len(args) - stay),
        out_specs=jax.tree.map(lambda _: vmem(), outs),
        scratch_shapes=scratch,
        name=name,
        compiler_params=pltpu.CompilerParams(vmem_limit_bytes=mib << 20),
        cost_estimate=pl.CostEstimate(flops=flops, bytes_accessed=1 << 20, transcendentals=0),
    )(*args)


def spot(axis):
    return lax.axis_index(axis).astype(jnp.int32)


def fetch(sources, targets, sems):
    copies = [
        pltpu.make_async_copy(src, dst, sems.at[n])
        for n, (src, dst) in enumerate(zip(sources, targets))
    ]
    for copy in copies:
        copy.start()
    for copy in copies:
        copy.wait()


def arr(shape, dtype):
    return jax.ShapeDtypeStruct(shape, dtype)


def placement(ids, wanted, rank):
    first = ids[0:1, :] == wanted
    match = first | (ids[1:2, :] == wanted)
    tok = TOK
    before = lax.broadcasted_iota(jnp.int32, (tok, tok), 0) < lax.broadcasted_iota(
        jnp.int32, (tok, tok), 1
    )
    ranks = mm(jnp.where(match, 1.0, 0.0).astype(BF), jnp.where(before, 1.0, 0.0).astype(BF))
    return match & (ranks == rank.astype(F32)), first


def rows_of(stride, shift, mul, core):
    n = lax.broadcasted_iota(jnp.int32, (NZ * stride, TOK), 0)
    z = lax.shift_right_logical(n * mul, shift)
    q = n - stride * z
    keep = jnp.where(q < CAP, 2 * z + core, -1)
    send = jnp.where((q >= CAP) & (q < 2 * CAP), 2 * z + 1 - core, -1)
    return keep, q, send, q - CAP


def decay_parts(rates):
    upto = lax.broadcasted_iota(jnp.int32, (TOK, TOK), 1) <= lax.broadcasted_iota(
        jnp.int32, (TOK, TOK), 0
    )
    col = jnp.broadcast_to(
        jnp.sum(jnp.where(upto, rates, 0.0), axis=1, keepdims=True), (TOK, TOK)
    )
    row = col.T
    total = jnp.sum(rates, axis=1, keepdims=True)
    prefix = row[0:1, :]
    start = jnp.exp(-prefix)
    end = jnp.exp(jnp.minimum(prefix - total, 0.0))
    return col, row, start, end, jnp.broadcast_to(total, (1, TOK))


def in_pieces(total):
    hi = jnp.broadcast_to(total, (8, TOK)).astype(BF).astype(F32)
    mid = (total - hi).astype(BF).astype(F32)
    low = total - hi - mid
    number = lax.broadcasted_iota(jnp.int32, (8, TOK), 0)
    return jnp.where(
        number == 0, hi, jnp.where(number == 1, mid, jnp.where(number == 2, low, 0.0))
    ).astype(BF)


def pack_kernel(
    ids_in, gw_in, ew_in, cot_in, inp_in, rate_in, k_in, v_in,
    keep_ref, send_ref, cols_ref, mine_ref,
    ids_ref, gw_ref, ew_ref, inp_ref, rate_ref, k_ref, v_ref, sems,
):
    here = pl.ds(pl.multiple_of(spot("tp") * COL, COL), COL)
    fetch(
        (ids_in, gw_in, ew_in, cot_in.at[:, here], inp_in.at[:, here], rate_in, k_in, v_in),
        (ids_ref, gw_ref, ew_ref, cols_ref, inp_ref, rate_ref, k_ref, v_ref),
        sems,
    )
    ids = ids_ref[...]
    weights = gw_ref[...] * ew_ref[...]
    cot, inp = cols_ref[...], inp_ref[...]
    ek, rk, es, rs = rows_of(2 * CAP, 16, 2731, spot("c"))
    for wanted, rank, out in ((ek, rk, keep_ref), (es, rs, send_ref)):
        hit, first = placement(ids, wanted, rank)
        scale = jnp.sum(
            jnp.where(hit, jnp.where(first, weights[0:1, :], weights[1:2, :]), 0.0),
            axis=1,
            keepdims=True,
        )
        take = jnp.where(hit, 1.0, 0.0).astype(BF)
        inp_rows = mm(take, inp)
        cot_rows = mm(take, cot) * scale
        for z in range(NZ):
            part = slice(2 * CAP * z, 2 * CAP * (z + 1))
            at = 4 * CAP * z
            out[at : at + 2 * CAP, :] = inp_rows[part].astype(BF)
            out[at + 2 * CAP : at + 4 * CAP, :] = cot_rows[part].astype(BF)
    _, _, start, end, total = decay_parts(rate_ref[...])
    keys, values = k_ref[...].astype(F32), v_ref[...]
    early = exact(keys * end, values, NTR)
    late = exact(keys * start, values, NTR)
    mine_ref[...] = jnp.concatenate([total, start, end, jnp.zeros((5, TOK), F32)], axis=0)
    for out in (keep_ref, send_ref):
        out[768:832, :] = early.astype(BF)
        out[832:896, :] = late.astype(BF)
        out[896:904, :] = in_pieces(total)
        out[904:912, :] = jnp.concatenate(
            [ids.astype(F32), jnp.zeros((6, TOK), F32)], axis=0
        ).astype(BF)


def in_one(pieces):
    pieces = pieces.astype(F32)
    return pieces[0:1, :] + pieces[1:2, :] + pieces[2:3, :]


def merge_kernel(keep_ref, got_ref, rows_ref, extra_ref):
    extra_ref[...] = got_ref[768:912, :]
    early, late = chip_states(
        *[
            ref[at : at + 64, :].astype(F32)
            for ref in (keep_ref, got_ref)
            for at in (768, 832)
        ],
        jnp.exp(-in_one(keep_ref[896:904, :])),
        jnp.exp(-in_one(got_ref[896:904, :])),
    )
    place = spot("z")
    for z in range(NZ):
        part = slice(4 * CAP * z, 4 * CAP * (z + 1))
        rows_ref[z, 0 : 4 * CAP, :] = keep_ref[part, :] + got_ref[part, :]
        rows_ref[z, 48:80, :] = jnp.where(z > place, early, late)
        rows_ref[z, 80:88, :] = keep_ref[896:904, :]


def picks_kernel(keep_ref, picks_ref):
    ek, rk, es, rs = rows_of(32, 5, 1, spot("c"))
    ids = keep_ref[904:912, :].astype(F32).astype(jnp.int32)
    for wanted, rank, at in ((ek, rk, 0), (es, rs, 512)):
        hit, _ = placement(ids, wanted, rank)
        picks_ref[at : at + 512, :] = jnp.where(hit, 1.0, 0.0).astype(BF)


def spread_kernel(got_ref, rows_ref, states_ref):
    states_ref[...] = got_ref[:, 48:88, :]
    for z in range(NZ):
        for kind in range(2):
            part = got_ref[z, 24 * kind : 24 * (kind + 1), :]
            for k in range(4):
                rows_ref[k, kind, 24 * z : 24 * (z + 1), :] = part


def expert_kernel(x_ref, gw_ref, uw_ref, dw_ref, part_ref, hid_ref, both_ref):
    inp = jnp.concatenate([x_ref[held_at(t), 0] for t in range(NT)], axis=1)
    cot = jnp.concatenate([x_ref[held_at(t), 1] for t in range(NT)], axis=1)
    both_w = jnp.concatenate([gw_ref[...], uw_ref[...]], axis=1)
    pre = mm(inp, both_w)
    gate, up = pre[:, :128], pre[:, 128:]
    hidden_grad = mm(cot, dw_ref[...], NTR)
    sig = jax.nn.sigmoid(gate)
    act = gate * sig
    hid_ref[...] = (act * up).astype(BF)
    gate_grad = (hidden_grad * up * sig * (1.0 + gate * (1.0 - sig))).astype(BF)
    up_grad = (hidden_grad * act).astype(BF)
    both = jnp.concatenate([gate_grad, up_grad], axis=1)
    both_ref[...] = both
    for t in range(0, NT, 2):
        out = mm(both, both_w[t * COL : (t + 2) * COL], NTR).astype(BF)
        part_ref[t] = out[:, :COL]
        part_ref[t + 1] = out[:, COL:]


def weight_kernel(x_ref, hid_ref, both_ref, gg_ref, gu_ref, gd_ref):
    both = both_ref[...]
    hidden = hid_ref[...]
    for t in range(0, NT, 2):
        rows = slice(t * COL, (t + 2) * COL)
        inp = jnp.concatenate([x_ref[held_at(t), 0], x_ref[held_at(t + 1), 0]], axis=1)
        cot = jnp.concatenate([x_ref[held_at(t), 1], x_ref[held_at(t + 1), 1]], axis=1)
        out = mm(inp, both, TN).astype(BF)
        gg_ref[rows, :] = out[:, :128]
        gu_ref[rows, :] = out[:, 128:]
        gd_ref[:, rows] = mm(hidden, cot, TN).astype(BF)


def chip_states(early, late, early_other, late_other, mine, theirs):
    is_first = spot("c") == 0
    both_early = early * jnp.where(is_first, theirs, 1.0) + early_other * jnp.where(
        is_first, 1.0, mine
    )
    both_late = late * jnp.where(is_first, 1.0, theirs) + late_other * jnp.where(
        is_first, mine, 1.0
    )
    return [jnp.where(is_first, a[:32], a[32:]).astype(BF) for a in (both_early, both_late)]


def sum_kernel(part_ref, out_ref):
    total = part_ref[0].astype(F32)
    for t in range(1, NT):
        total = total + part_ref[t].astype(F32)
    out_ref[...] = total.reshape(NZ, 2 * CAP, COL).astype(BF)


def resid_kernel(picks_ref, own_ref, other_ref, cols_ref, out_ref):
    own = own_ref[:, 0:32, :].reshape(512, COL)
    other = other_ref[:, 0:32, :].reshape(512, COL)
    moe = mm(picks_ref[0:512, :], own, TN) + mm(picks_ref[512:1024, :], other, TN)
    resid = (cols_ref[...].astype(F32) + moe).astype(BF)
    for t in range(NT):
        out_ref[t] = resid


def proj_kernel(r_ref, p_ref, mixer_ref, q_ref, mine_ref, og_ref, keep_ref, send_ref, state_ref):
    core = spot("c")
    resid = jnp.concatenate([r_ref[t] for t in range(NT)], axis=1)
    out_grad = mm(resid, p_ref[...])
    og_ref[...] = out_grad
    query = q_ref[...].astype(F32)
    early = exact(query * mine_ref[2:3, :], out_grad)
    late = exact(query * mine_ref[1:2, :], out_grad)
    state_ref[0] = early
    state_ref[1] = late
    send_ref[16] = early.astype(BF)
    send_ref[17] = late.astype(BF)
    mixer = mixer_ref[...]
    for t in range(NT):
        share = mm(r_ref[t], mixer, TN)
        low, high = share[:64], share[64:]
        keep_ref[t] = jnp.where(core == 0, low, high)
        send_ref[t] = jnp.where(core == 0, high, low).astype(BF)


def decays(own_ref, other_ref):
    def total(ref):
        rows = ref[:, 56:64, :].astype(F32)
        return rows[:, 0, :] + rows[:, 1, :] + rows[:, 2, :]

    return total(own_ref), total(other_ref)


def row_at(table, place):
    number = lax.broadcasted_iota(jnp.int32, table.shape, 0)
    return jnp.sum(jnp.where(number == place, table, 0.0), axis=0, keepdims=True)


def at_block(far_early, far_late, near, theirs):
    is_first = spot("c") == 0
    early = far_early * jnp.where(is_first, 1.0, theirs) + jnp.where(is_first, 0.0, near)
    late = far_late * jnp.where(is_first, theirs, 1.0) + jnp.where(is_first, near, 0.0)
    return early, late


def intra_kernel(
    og_ref, rate_ref, q_ref, k_ref, v_ref, own_ref, other_ref, extra_ref,
    gq_ref, part_ref, weight_ref,
):
    place, core = spot("z"), spot("c")
    own, other = decays(own_ref, other_ref)
    chip = own + other
    number = lax.broadcasted_iota(jnp.int32, (NZ, COL), 0)
    between = jnp.zeros((NZ, COL), F32)
    for u in range(NZ):
        inside = ((number < u) & (u < place)) | ((number > u) & (u > place))
        between = between + jnp.where(inside, chip[u : u + 1, :], 0.0)
    weight = jnp.exp(-between)
    early_w = jnp.where(number < place, weight, 0.0)
    late_w = jnp.where(number > place, weight, 0.0)
    weight_ref[0:16, :] = early_w
    weight_ref[16:32, :] = late_w

    def far(ref):
        early = late = jnp.zeros((32, COL), F32)
        for z in range(NZ):
            state = ref[z, 24:56, :].astype(F32)
            early = early + state * early_w[z : z + 1, :]
            late = late + state * late_w[z : z + 1, :]
        return early, late

    is_first = core == 0
    here, there = far(own_ref), far(other_ref)
    far_early, far_late = [
        jnp.concatenate([jnp.where(is_first, a, b), jnp.where(is_first, b, a)], axis=0)
        for a, b in zip(here, there)
    ]
    near = jnp.where(is_first, extra_ref[64:128, :], extra_ref[0:64, :]).astype(F32)
    theirs = jnp.exp(-row_at(other, place))
    kv_early, kv_late = at_block(far_early, far_late, near, theirs)
    scale = KD ** (-0.5)
    col, row, start, end, _ = decay_parts(rate_ref[...])
    low, high = scale * start, scale * end
    mixed = scale * jnp.exp(-jnp.abs(col - row))
    out_grad = og_ref[...]
    query, key, value = q_ref[...], k_ref[...], v_ref[...]
    score_grad = exact(out_grad, value) * mixed
    gq_ref[...] = (
        exact(key, score_grad, NTR)
        + low * exact(kv_early, out_grad, NTR)
        + high * exact(kv_late, out_grad, NTR)
    )
    part_ref[0:64, :] = exact(query, score_grad)
    part_ref[64:192, :] = exact(out_grad, mm(query, key, TN) * mixed, TN)
    part_ref[192:256, :] = key.astype(F32)
    part_ref[256:384, :] = value.astype(F32)
    part_ref[384:392, :] = jnp.concatenate([low, high, theirs, jnp.zeros((5, TOK), F32)], axis=0)


def chip_kernel(keep_ref, got_ref, state_ref, own_ref, other_ref, out_ref, near_ref):
    place, core = spot("z"), spot("c")
    own, other = decays(own_ref, other_ref)
    mine = jnp.exp(-row_at(own, place))
    theirs = jnp.exp(-row_at(other, place))
    early_other, late_other = got_ref[16].astype(F32), got_ref[17].astype(F32)
    early, late = chip_states(state_ref[0], state_ref[1], early_other, late_other, mine, theirs)
    near_ref[...] = jnp.where(core == 0, late_other, early_other)
    for z in range(NZ):
        out_ref[z, 0:64, :] = (keep_ref[z] + got_ref[z].astype(F32)).astype(BF)
        out_ref[z, 64:96, :] = jnp.where(z > place, early, late)


def gather_kernel(got_ref, weight_ref, state_ref):
    early = late = jnp.zeros((32, COL), F32)
    for z in range(NZ):
        state = got_ref[z, 64:96, :].astype(F32)
        early = early + state * weight_ref[z : z + 1, :]
        late = late + state * weight_ref[16 + z : 17 + z, :]
    state_ref[0] = early
    state_ref[1] = late


def final_kernel(far_ref, near_ref, part_ref, got_ref, proj_ref, gk_ref, gv_ref):
    share = jnp.zeros((64, COL), F32)
    for z in range(NZ):
        share = share + got_ref[z, 0:64, :].astype(F32)
    proj_ref[...] = share
    early, late = at_block(
        jnp.concatenate([far_ref[0, 0], far_ref[1, 0]], axis=0),
        jnp.concatenate([far_ref[0, 1], far_ref[1, 1]], axis=0),
        near_ref[...],
        part_ref[386:387, :],
    )
    low, high = part_ref[384:385, :], part_ref[385:386, :]
    key, value = part_ref[192:256, :].astype(BF), part_ref[256:384, :].astype(BF)
    gk_ref[...] = part_ref[0:64, :] + low * exact(early, value) + high * exact(late, value)
    gv_ref[...] = part_ref[64:192, :] + low * exact(early, key, TN) + high * exact(late, key, TN)


def groups(step, stride, step_other, stride_other):
    first = [[stride * g + step * k for k in range(4)] for g in range(4)]
    second = [[16 + stride_other * g + step_other * k for k in range(4)] for g in range(4)]
    return first + second


def within(blocks, axis, sets):
    return lax.all_to_all(
        blocks, axis, split_axis=0, concat_axis=0, axis_index_groups=sets, tiled=True
    )


def to_all(shard, axis, sets):
    return within(jnp.broadcast_to(shard, (len(sets[0]), *shard.shape)), axis, sets)


def exchange(blocks, axis):
    return lax.all_to_all(blocks, axis, split_axis=0, concat_axis=0, tiled=True)


def held_at(t):
    return jnp.where(spot("c") == 0, (t % 4) * 4 + t // 4, t)


def on_device(
    cotangent, moe_input, expert_ids, group_weight, expert_weight, mixer_out,
    queries, key_vectors, value_vectors, decay_rates, proj_weight,
    gate_weight, up_weight, down_weight,
):
    ids = expert_ids.T
    keep, send, cols, mine = call(
        pack_kernel,
        [arr((912, COL), BF), arr((912, COL), BF), arr((TOK, COL), BF), arr((8, TOK), F32)],
        (
            ids, group_weight.reshape(1, TOK), expert_weight.T, cotangent, moe_input,
            decay_rates, key_vectors, value_vectors,
        ),
        "pack",
        60,
        stay=8,
        scratch=[
            pltpu.VMEM((2, TOK), jnp.int32), pltpu.VMEM((1, TOK), F32), pltpu.VMEM((2, TOK), F32),
            pltpu.VMEM((TOK, COL), BF), pltpu.VMEM((1, TOK), F32), pltpu.VMEM((KD, TOK), BF),
            pltpu.VMEM((VD, TOK), BF), pltpu.SemaphoreType.DMA((8,)),
        ],
    )
    picks = call(picks_kernel, arr((1024, TOK), BF), (keep,), "picks")
    swapped = lax.ppermute(send, "c", SWAP)
    rows, extra = call(
        merge_kernel,
        [arr((NZ, 88, COL), BF), arr((144, COL), BF)],
        (keep, swapped),
        "merge",
    )
    rows, picks, extra = lax.optimization_barrier((rows, picks, extra))
    rows = exchange(rows, "z")
    copies, states = call(
        spread_kernel,
        [arr((4, 2, NZ * 2 * CAP, COL), BF), arr((NZ, 40, COL), BF)],
        (rows,),
        "spread",
    )
    rows = within(copies, ("c", "tp"), groups(4, 1, 1, 4))
    rows = to_all(rows.reshape(4, 2, NZ * 2 * CAP, COL), ("c", "tp"), groups(1, 4, 4, 1))
    rows = rows.reshape(NT, 2, NZ * 2 * CAP, COL)
    shares, hidden, both = call(
        expert_kernel,
        [arr((NT, 384, COL), BF), arr((384, 128), BF), arr((384, 256), BF)],
        (rows, gate_weight[0], up_weight[0], down_weight[0]),
        "expert",
        20,
    )
    shares = exchange(shares, "tp")
    back = call(sum_kernel, arr((NZ, 2 * CAP, COL), BF), (shares,), "sums", 6)
    own = jnp.concatenate([exchange(back, "z"), states], axis=1)
    own, rows, hidden, both = lax.optimization_barrier((own, rows, hidden, both))
    other = lax.ppermute(own, "c", SWAP)
    grad_gate, grad_up, grad_down = call(
        weight_kernel,
        [arr((2048, 128), BF), arr((2048, 128), BF), arr((128, 2048), BF)],
        (rows, hidden, both),
        "weights",
        16,
        1 << 29,
    )
    resid = call(resid_kernel, arr((NT, TOK, COL), BF), (picks, own, other, cols), "resid")
    resid, grad_gate, grad_up, grad_down = lax.optimization_barrier(
        (resid, grad_gate, grad_up, grad_down)
    )
    resid = exchange(resid, "tp")
    out_grad, proj_keep, proj_send, state = call(
        proj_kernel,
        [
            arr((TOK, VD), F32), arr((NZ, 64, COL), F32), arr((18, 64, COL), BF),
            arr((2, KD, VD), F32),
        ],
        (resid, proj_weight, mixer_out, queries, mine),
        "proj",
        8,
    )
    got = lax.ppermute(proj_send, "c", SWAP)
    grad_queries, part, weight = call(
        intra_kernel,
        [arr((KD, TOK), F32), arr((392, TOK), F32), arr((32, TOK), F32)],
        (out_grad, decay_rates, queries, key_vectors, value_vectors, own, other, extra),
        "intra",
    )
    chip, near = call(
        chip_kernel,
        [arr((NZ, 96, COL), BF), arr((KD, VD), F32)],
        (proj_keep, got, state, own, other),
        "chip",
    )
    chip, grad_queries, part, weight = lax.optimization_barrier((chip, grad_queries, part, weight))
    chip = exchange(chip, "z")
    far = call(gather_kernel, arr((2, 32, COL), F32), (chip, weight), "gather")
    far = lax.all_gather(far, "c")
    grad_proj, grad_keys, grad_values = call(
        final_kernel,
        [arr((64, COL), F32), arr((KD, TOK), F32), arr((VD, TOK), F32)],
        (far, near, part, chip),
        "final",
    )
    return (
        grad_gate[None], grad_up[None], grad_down[None],
        grad_proj, grad_queries, grad_keys, grad_values,
    )


def solution(mesh):
    finer = Mesh(mesh.devices.reshape(NZ, 2, NT), ("z", "c", "tp"))
    in_specs = (
        P(SP, None), P(SP, None), P(SP, None), P(SP), P(SP, None), P(SP, "tp"),
        P("tp", SP), P("tp", SP), P("tp", SP), P("tp", SP), P(None, "tp"),
        P(SP, None, "tp"), P(SP, None, "tp"), P(SP, "tp", None),
    )
    out_specs = (
        P(SP, None, "tp"), P(SP, None, "tp"), P(SP, "tp", None), P(SP, "tp"),
        P("tp", SP), P("tp", SP), P("tp", SP),
    )
    return jax.shard_map(
        on_device, mesh=finer, in_specs=in_specs, out_specs=out_specs, check_vma=False
    )
```

```python
import jax
import jax.numpy as jnp
from jax import lax
from jax.experimental import pallas as pl
from jax.experimental.pallas import tpu as pltpu
from jax.sharding import Mesh
from jax.sharding import PartitionSpec as P

BF = jnp.bfloat16
F32 = jnp.float32
NZ = 16
NT = 16
CAP = 12
TOK = 128
COL = 128
KD = 64
VD = 128
SP = ("z", "c")
SWAP = [(0, 1), (1, 0)]

NN = (((1,), (0,)), ((), ()))
NTR = (((1,), (1,)), ((), ()))
TN = (((0,), (0,)), ((), ()))


def mm(a, b, dims=NN):
    return lax.dot_general(a, b, dims, preferred_element_type=F32)


def halves(a):
    high = a.astype(BF)
    return high, (a - high.astype(F32)).astype(BF)


def exact(a, b, dims=NN):
    if a.dtype == BF:
        high, low = halves(b)
        return mm(a, high, dims) + mm(a, low, dims)
    high, low = halves(a)
    if b.dtype == BF:
        return mm(high, b, dims) + mm(low, b, dims)
    other, rest = halves(b)
    return mm(high, other, dims) + (mm(high, rest, dims) + mm(low, other, dims))


def vmem():
    return pl.BlockSpec(memory_space=pltpu.VMEM)


def hbm():
    return pl.BlockSpec(memory_space=pltpu.HBM)


def call(kernel, outs, args, name, mib=4, flops=1 << 27, stay=0, scratch=()):
    return pl.pallas_call(
        kernel,
        out_shape=outs,
        in_specs=[hbm()] * stay + [vmem()] * (len(args) - stay),
        out_specs=jax.tree.map(lambda _: vmem(), outs),
        scratch_shapes=scratch,
        name=name,
        compiler_params=pltpu.CompilerParams(vmem_limit_bytes=mib << 20),
        cost_estimate=pl.CostEstimate(flops=flops, bytes_accessed=1 << 20, transcendentals=0),
    )(*args)


def spot(axis):
    return lax.axis_index(axis).astype(jnp.int32)


def fetch(sources, targets, sems):
    copies = [
        pltpu.make_async_copy(src, dst, sems.at[n])
        for n, (src, dst) in enumerate(zip(sources, targets))
    ]
    for copy in copies:
        copy.start()
    for copy in copies:
        copy.wait()


def arr(shape, dtype):
    return jax.ShapeDtypeStruct(shape, dtype)


def placement(ids, wanted, rank):
    first = ids[0:1, :] == wanted
    match = first | (ids[1:2, :] == wanted)
    tok = TOK
    before = lax.broadcasted_iota(jnp.int32, (tok, tok), 0) < lax.broadcasted_iota(
        jnp.int32, (tok, tok), 1
    )
    ranks = mm(jnp.where(match, 1.0, 0.0).astype(BF), jnp.where(before, 1.0, 0.0).astype(BF))
    return match & (ranks == rank.astype(F32)), first


def decay_parts(rates):
    upto = lax.broadcasted_iota(jnp.int32, (TOK, TOK), 1) <= lax.broadcasted_iota(
        jnp.int32, (TOK, TOK), 0
    )
    col = jnp.broadcast_to(
        jnp.sum(jnp.where(upto, rates, 0.0), axis=1, keepdims=True), (TOK, TOK)
    )
    row = col.T
    total = jnp.sum(rates, axis=1, keepdims=True)
    prefix = row[0:1, :]
    start = jnp.exp(-prefix)
    end = jnp.exp(jnp.minimum(prefix - total, 0.0))
    return col, row, start, end, jnp.broadcast_to(total, (1, TOK))


def in_pieces(row):
    hi = row.astype(BF).astype(F32)
    mid = (row - hi).astype(BF).astype(F32)
    return jnp.concatenate([hi, mid, row - hi - mid], axis=0)


def in_one(pieces):
    pieces = pieces.astype(F32)
    return pieces[0:1, :] + pieces[1:2, :] + pieces[2:3, :]


def ids_of(rows):
    return rows[IDS - ROUTE : IDS - ROUTE + 2, :].astype(jnp.int32)


def rates_of(g_ref, block):
    return in_one(g_ref[block, ROUTE:HELD, :].astype(F32)[RATE - ROUTE : IDS - ROUTE])


COT, INP, KEY, VALUE, ROUTE, RATE, IDS, HELD = 0, 128, 256, 320, 448, 456, 459, 464


def load_kernel(
    ids_in, gw_in, ew_in, cot_in, inp_in, rate_in, k_in, v_in,
    out_ref, ids_ref, gw_ref, ew_ref, rate_ref, sems,
):
    here = pl.ds(pl.multiple_of(spot("tp") * COL, COL), COL)
    fetch(
        (ids_in, gw_in, ew_in, cot_in.at[:, here], inp_in.at[:, here], rate_in, k_in, v_in),
        (
            ids_ref, gw_ref, ew_ref, out_ref.at[pl.ds(COT, TOK)], out_ref.at[pl.ds(INP, TOK)],
            rate_ref, out_ref.at[pl.ds(KEY, KD)], out_ref.at[pl.ds(VALUE, VD)],
        ),
        sems,
    )
    weights = gw_ref[...] * ew_ref[...]
    none = jnp.zeros((2, TOK), F32)
    out_ref[ROUTE:HELD, :] = jnp.concatenate(
        [in_pieces(weights[0:1, :]), in_pieces(weights[1:2, :]), none]
        + [in_pieces(rate_ref[...]), ids_ref[...].astype(F32), none, none[0:1, :]],
        axis=0,
    ).astype(BF)


def pack_kernel(g_ref, rows_ref, picks_ref, small_ref, mine_ref):
    core = spot("c")
    number = lax.broadcasted_iota(jnp.int32, (NZ * 2 * CAP, TOK), 0)
    z = lax.shift_right_logical(number * 2731, 16)
    q = number - 2 * CAP * z
    first_half = q < CAP
    inp_rows = cot_rows = 0.0
    for block, wanted, rank in (
        (core, jnp.where(first_half, 2 * z + core, -1), q),
        (1 - core, jnp.where(first_half, -1, 2 * z + core), q - CAP),
    ):
        rows = g_ref[block, ROUTE:HELD, :].astype(F32)
        hit, first = placement(ids_of(rows), wanted, rank)
        scale = jnp.sum(
            jnp.where(hit, jnp.where(first, in_one(rows[0:3]), in_one(rows[3:6])), 0.0),
            axis=1,
            keepdims=True,
        )
        take = jnp.where(hit, 1.0, 0.0).astype(BF)
        if block is core:
            picks_ref[0:384, :] = take
        inp_rows = inp_rows + mm(take, g_ref[block, INP : INP + TOK, :])
        cot_rows = cot_rows + mm(take, g_ref[block, COT : COT + TOK, :]) * scale
    for z in range(NZ):
        part = slice(2 * CAP * z, 2 * CAP * (z + 1))
        rows_ref[z, 0 : 2 * CAP, :] = inp_rows[part].astype(BF)
        rows_ref[z, 2 * CAP : 4 * CAP, :] = cot_rows[part].astype(BF)
    z = lax.shift_right_logical(number * 2731, 16)
    hit, _ = placement(
        ids_of(g_ref[core, ROUTE:HELD, :].astype(F32)),
        jnp.where(first_half, -1, 2 * z + 1 - core),
        q - CAP,
    )
    picks_ref[384:768, :] = jnp.where(hit, 1.0, 0.0).astype(BF)

    _, _, start_a, end_a, total_a = decay_parts(rates_of(g_ref, 0))
    _, _, start_b, end_b, total_b = decay_parts(rates_of(g_ref, 1))
    half = pl.ds(pl.multiple_of(KEY + 32 * core, 32), 32)
    keys = jnp.concatenate([g_ref[0, half, :], g_ref[1, half, :]], axis=1).astype(F32)
    values = jnp.concatenate([g_ref[k, VALUE : VALUE + VD, :] for k in (0, 1)], axis=1)
    early = jnp.concatenate([end_a * jnp.exp(-total_b), end_b], axis=1)
    late = jnp.concatenate([start_a, start_b * jnp.exp(-total_a)], axis=1)
    small_ref[0:32, :] = exact(keys * early, values, NTR).astype(BF)
    small_ref[32:64, :] = exact(keys * late, values, NTR).astype(BF)
    small_ref[64:72, :] = jnp.concatenate(
        [in_pieces(total_a + total_b), jnp.zeros((5, TOK), F32)], axis=0
    ).astype(BF)
    is_first = core == 0
    mine_ref[...] = jnp.concatenate(
        [
            jnp.where(is_first, start_a, start_b), jnp.where(is_first, end_a, end_b),
            jnp.where(is_first, total_a, total_b), jnp.where(is_first, total_b, total_a),
            jnp.zeros((4, TOK), F32),
        ],
        axis=0,
    )


def spread_kernel(got_ref, rows_ref):
    for z in range(NZ):
        for kind in range(2):
            part = got_ref[z, 24 * kind : 24 * (kind + 1), :]
            for k in range(4):
                rows_ref[k, kind, 24 * z : 24 * (z + 1), :] = part


def expert_kernel(x_ref, gw_ref, uw_ref, dw_ref, part_ref, hid_ref, both_ref):
    inp = jnp.concatenate([x_ref[held_at(t), 0] for t in range(NT)], axis=1)
    cot = jnp.concatenate([x_ref[held_at(t), 1] for t in range(NT)], axis=1)
    both_w = jnp.concatenate([gw_ref[...], uw_ref[...]], axis=1)
    pre = mm(inp, both_w)
    gate, up = pre[:, :128], pre[:, 128:]
    hidden_grad = mm(cot, dw_ref[...], NTR)
    sig = jax.nn.sigmoid(gate)
    act = gate * sig
    hid_ref[...] = (act * up).astype(BF)
    gate_grad = (hidden_grad * up * sig * (1.0 + gate * (1.0 - sig))).astype(BF)
    up_grad = (hidden_grad * act).astype(BF)
    both = jnp.concatenate([gate_grad, up_grad], axis=1)
    both_ref[...] = both
    for t in range(0, NT, 2):
        out = mm(both, both_w[t * COL : (t + 2) * COL], NTR).astype(BF)
        part_ref[t] = out[:, :COL]
        part_ref[t + 1] = out[:, COL:]


def weight_kernel(x_ref, hid_ref, both_ref, gg_ref, gu_ref, gd_ref):
    both = both_ref[...]
    hidden = hid_ref[...]
    for t in range(0, NT, 2):
        rows = slice(t * COL, (t + 2) * COL)
        inp = jnp.concatenate([x_ref[held_at(t), 0], x_ref[held_at(t + 1), 0]], axis=1)
        cot = jnp.concatenate([x_ref[held_at(t), 1], x_ref[held_at(t + 1), 1]], axis=1)
        out = mm(inp, both, TN).astype(BF)
        gg_ref[rows, :] = out[:, :128]
        gu_ref[rows, :] = out[:, 128:]
        gd_ref[:, rows] = mm(hidden, cot, TN).astype(BF)


def chip_states(early, late, early_other, late_other, mine, theirs):
    is_first = spot("c") == 0
    both_early = early * jnp.where(is_first, theirs, 1.0) + early_other * jnp.where(
        is_first, 1.0, mine
    )
    both_late = late * jnp.where(is_first, 1.0, theirs) + late_other * jnp.where(
        is_first, mine, 1.0
    )
    return [jnp.where(is_first, a[:32], a[32:]).astype(BF) for a in (both_early, both_late)]


def sum_kernel(part_ref, small_ref, out_ref):
    total = part_ref[0].astype(F32)
    for t in range(1, NT):
        total = total + part_ref[t].astype(F32)
    out_ref[:, 0 : 2 * CAP, :] = total.reshape(NZ, 2 * CAP, COL).astype(BF)
    early, late, pieces = small_ref[0:32, :], small_ref[32:64, :], small_ref[64:72, :]
    place = spot("z")
    for z in range(NZ):
        out_ref[z, 24:56, :] = jnp.where(z > place, early, late)
        out_ref[z, 56:64, :] = pieces


def resid_kernel(picks_ref, own_ref, other_ref, g_ref, out_ref):
    own, other = [
        r[:, 0 : 2 * CAP, :].astype(F32).reshape(384, COL).astype(BF) for r in (own_ref, other_ref)
    ]
    moe = mm(picks_ref[0:384, :], own, TN) + mm(picks_ref[384:768, :], other, TN)
    cot = g_ref[spot("c"), COT : COT + TOK, :]
    resid = (cot.astype(F32) + moe).astype(BF)
    for t in range(NT):
        out_ref[t] = resid


def proj_kernel(r_ref, p_ref, mixer_ref, q_ref, mine_ref, og_ref, keep_ref, send_ref, state_ref):
    core = spot("c")
    resid = jnp.concatenate([r_ref[t] for t in range(NT)], axis=1)
    out_grad = mm(resid, p_ref[...])
    og_ref[...] = out_grad
    query = q_ref[...].astype(F32)
    early = exact(query * mine_ref[1:2, :], out_grad)
    late = exact(query * mine_ref[0:1, :], out_grad)
    state_ref[0] = early
    state_ref[1] = late
    send_ref[16] = early.astype(BF)
    send_ref[17] = late.astype(BF)
    mixer = mixer_ref[...]
    for t in range(NT):
        share = mm(r_ref[t], mixer, TN)
        low, high = share[:64], share[64:]
        keep_ref[t] = jnp.where(core == 0, low, high)
        send_ref[t] = jnp.where(core == 0, high, low).astype(BF)


def at_block(far_early, far_late, near, theirs):
    is_first = spot("c") == 0
    early = far_early * jnp.where(is_first, 1.0, theirs) + jnp.where(is_first, 0.0, near)
    late = far_late * jnp.where(is_first, theirs, 1.0) + jnp.where(is_first, near, 0.0)
    return early, late


def intra_kernel(
    og_ref, q_ref, g_ref, mine_ref, own_ref, other_ref, gq_ref, part_ref, weight_ref
):
    place, core = spot("z"), spot("c")
    rows = own_ref[:, 56:64, :].astype(F32)
    chip = rows[:, 0, :] + rows[:, 1, :] + rows[:, 2, :]
    number = lax.broadcasted_iota(jnp.int32, (NZ, COL), 0)
    between = jnp.zeros((NZ, COL), F32)
    for u in range(NZ):
        inside = ((number < u) & (u < place)) | ((number > u) & (u > place))
        between = between + jnp.where(inside, chip[u : u + 1, :], 0.0)
    weight = jnp.exp(-between)
    early_w = jnp.where(number < place, weight, 0.0)
    late_w = jnp.where(number > place, weight, 0.0)
    weight_ref[0:16, :] = early_w
    weight_ref[16:32, :] = late_w

    def far(ref):
        early = late = jnp.zeros((32, COL), F32)
        for z in range(NZ):
            state = ref[z, 24:56, :].astype(F32)
            early = early + state * early_w[z : z + 1, :]
            late = late + state * late_w[z : z + 1, :]
        return early, late

    is_first = core == 0
    here, there = far(own_ref), far(other_ref)
    far_early, far_late = [
        jnp.concatenate([jnp.where(is_first, a, b), jnp.where(is_first, b, a)], axis=0)
        for a, b in zip(here, there)
    ]
    _, _, start, end, _ = decay_parts(rates_of(g_ref, 1 - core))
    there = g_ref[1 - core, KEY : KEY + KD, :].astype(F32) * jnp.where(is_first, start, end)
    near = exact(there, g_ref[1 - core, VALUE : VALUE + VD, :], NTR)
    theirs = jnp.exp(-mine_ref[3:4, :])
    kv_early, kv_late = at_block(far_early, far_late, near, theirs)
    scale = KD ** (-0.5)
    col, row, start, end, _ = decay_parts(rates_of(g_ref, core))
    low, high = scale * start, scale * end
    mixed = scale * jnp.exp(-jnp.abs(col - row))
    out_grad = og_ref[...]
    query, key = q_ref[...], g_ref[core, KEY : KEY + KD, :]
    value = g_ref[core, VALUE : VALUE + VD, :]
    score_grad = exact(out_grad, value) * mixed
    gq_ref[...] = (
        exact(key, score_grad, NTR)
        + low * exact(kv_early, out_grad, NTR)
        + high * exact(kv_late, out_grad, NTR)
    )
    part_ref[0:64, :] = exact(query, score_grad)
    part_ref[64:192, :] = exact(out_grad, mm(query, key, TN) * mixed, TN)
    part_ref[192:256, :] = key.astype(F32)
    part_ref[256:384, :] = value.astype(F32)
    part_ref[384:392, :] = jnp.concatenate([low, high, theirs, jnp.zeros((5, TOK), F32)], axis=0)


def chip_kernel(keep_ref, got_ref, state_ref, mine_ref, out_ref, near_ref):
    place, core = spot("z"), spot("c")
    mine, theirs = jnp.exp(-mine_ref[2:3, :]), jnp.exp(-mine_ref[3:4, :])
    early_other, late_other = got_ref[16].astype(F32), got_ref[17].astype(F32)
    early, late = chip_states(state_ref[0], state_ref[1], early_other, late_other, mine, theirs)
    near_ref[...] = jnp.where(core == 0, late_other, early_other)
    for z in range(NZ):
        out_ref[z, 0:64, :] = (keep_ref[z] + got_ref[z].astype(F32)).astype(BF)
        out_ref[z, 64:96, :] = jnp.where(z > place, early, late)


def gather_kernel(got_ref, weight_ref, state_ref):
    early = late = jnp.zeros((32, COL), F32)
    for z in range(NZ):
        state = got_ref[z, 64:96, :].astype(F32)
        early = early + state * weight_ref[z : z + 1, :]
        late = late + state * weight_ref[16 + z : 17 + z, :]
    state_ref[0] = early
    state_ref[1] = late


def final_kernel(far_ref, near_ref, part_ref, got_ref, proj_ref, gk_ref, gv_ref):
    share = jnp.zeros((64, COL), F32)
    for z in range(NZ):
        share = share + got_ref[z, 0:64, :].astype(F32)
    proj_ref[...] = share
    early, late = at_block(
        jnp.concatenate([far_ref[0, 0], far_ref[1, 0]], axis=0),
        jnp.concatenate([far_ref[0, 1], far_ref[1, 1]], axis=0),
        near_ref[...],
        part_ref[386:387, :],
    )
    low, high = part_ref[384:385, :], part_ref[385:386, :]
    key, value = part_ref[192:256, :].astype(BF), part_ref[256:384, :].astype(BF)
    gk_ref[...] = part_ref[0:64, :] + low * exact(early, value) + high * exact(late, value)
    gv_ref[...] = part_ref[64:192, :] + low * exact(early, key, TN) + high * exact(late, key, TN)


def groups(step, stride, step_other, stride_other):
    first = [[stride * g + step * k for k in range(4)] for g in range(4)]
    second = [[16 + stride_other * g + step_other * k for k in range(4)] for g in range(4)]
    return first + second


def within(blocks, axis, sets):
    return lax.all_to_all(
        blocks, axis, split_axis=0, concat_axis=0, axis_index_groups=sets, tiled=True
    )


def to_all(shard, axis, sets):
    return within(jnp.broadcast_to(shard, (len(sets[0]), *shard.shape)), axis, sets)


def exchange(blocks, axis):
    return lax.all_to_all(blocks, axis, split_axis=0, concat_axis=0, tiled=True)


def held_at(t):
    return jnp.where(spot("c") == 0, (t % 4) * 4 + t // 4, t)


def on_device(
    cotangent, moe_input, expert_ids, group_weight, expert_weight, mixer_out,
    queries, key_vectors, value_vectors, decay_rates, proj_weight,
    gate_weight, up_weight, down_weight,
):
    ids = expert_ids.T
    held = call(
        load_kernel,
        arr((HELD, COL), BF),
        (
            ids, group_weight.reshape(1, TOK), expert_weight.T, cotangent, moe_input,
            decay_rates, key_vectors, value_vectors,
        ),
        "load",
        60,
        stay=8,
        scratch=[
            pltpu.VMEM((2, TOK), jnp.int32), pltpu.VMEM((1, TOK), F32), pltpu.VMEM((2, TOK), F32),
            pltpu.VMEM((1, TOK), F32), pltpu.SemaphoreType.DMA((8,)),
        ],
    )
    held = lax.all_gather(held, "c")
    rows, picks, small, mine = call(
        pack_kernel,
        [
            arr((NZ, 4 * CAP, COL), BF), arr((768, TOK), BF), arr((72, COL), BF),
            arr((8, TOK), F32),
        ],
        (held,),
        "pack",
    )
    rows = exchange(rows, "z")
    copies = call(spread_kernel, arr((4, 2, NZ * 2 * CAP, COL), BF), (rows,), "spread")
    rows = within(copies, ("c", "tp"), groups(4, 1, 1, 4))
    rows = to_all(rows.reshape(4, 2, NZ * 2 * CAP, COL), ("c", "tp"), groups(1, 4, 4, 1))
    rows = rows.reshape(NT, 2, NZ * 2 * CAP, COL)
    shares, hidden, both = call(
        expert_kernel,
        [arr((NT, 384, COL), BF), arr((384, 128), BF), arr((384, 256), BF)],
        (rows, gate_weight[0], up_weight[0], down_weight[0]),
        "expert",
        20,
    )
    shares = exchange(shares, "tp")
    back = call(sum_kernel, arr((NZ, 64, COL), BF), (shares, small), "sums", 6)
    own = exchange(back, "z")
    own, rows, hidden, both = lax.optimization_barrier((own, rows, hidden, both))
    other = lax.ppermute(own, "c", SWAP)
    grad_gate, grad_up, grad_down = call(
        weight_kernel,
        [arr((2048, 128), BF), arr((2048, 128), BF), arr((128, 2048), BF)],
        (rows, hidden, both),
        "weights",
        16,
        1 << 29,
    )
    resid = call(resid_kernel, arr((NT, TOK, COL), BF), (picks, own, other, held), "resid")
    resid, grad_gate, grad_up, grad_down = lax.optimization_barrier(
        (resid, grad_gate, grad_up, grad_down)
    )
    resid = exchange(resid, "tp")
    out_grad, proj_keep, proj_send, state = call(
        proj_kernel,
        [
            arr((TOK, VD), F32), arr((NZ, 64, COL), F32), arr((18, 64, COL), BF),
            arr((2, KD, VD), F32),
        ],
        (resid, proj_weight, mixer_out, queries, mine),
        "proj",
        8,
    )
    got = lax.ppermute(proj_send, "c", SWAP)
    grad_queries, part, weight = call(
        intra_kernel,
        [arr((KD, TOK), F32), arr((392, TOK), F32), arr((32, TOK), F32)],
        (out_grad, queries, held, mine, own, other),
        "intra",
    )
    chip, near = call(
        chip_kernel,
        [arr((NZ, 96, COL), BF), arr((KD, VD), F32)],
        (proj_keep, got, state, mine),
        "chip",
    )
    chip, grad_queries, part, weight = lax.optimization_barrier((chip, grad_queries, part, weight))
    chip = exchange(chip, "z")
    far = call(gather_kernel, arr((2, 32, COL), F32), (chip, weight), "gather")
    far = lax.all_gather(far, "c")
    grad_proj, grad_keys, grad_values = call(
        final_kernel,
        [arr((64, COL), F32), arr((KD, TOK), F32), arr((VD, TOK), F32)],
        (far, near, part, chip),
        "final",
    )
    return (
        grad_gate[None], grad_up[None], grad_down[None],
        grad_proj, grad_queries, grad_keys, grad_values,
    )


def solution(mesh):
    finer = Mesh(mesh.devices.reshape(NZ, 2, NT), ("z", "c", "tp"))
    in_specs = (
        P(SP, None), P(SP, None), P(SP, None), P(SP), P(SP, None), P(SP, "tp"),
        P("tp", SP), P("tp", SP), P("tp", SP), P("tp", SP), P(None, "tp"),
        P(SP, None, "tp"), P(SP, None, "tp"), P(SP, "tp", None),
    )
    out_specs = (
        P(SP, None, "tp"), P(SP, None, "tp"), P(SP, "tp", None), P(SP, "tp"),
        P("tp", SP), P("tp", SP), P("tp", SP),
    )
    return jax.shard_map(
        on_device, mesh=finer, in_specs=in_specs, out_specs=out_specs, check_vma=False
    )
```

```python
import jax
import jax.numpy as jnp
from jax import lax
from jax.experimental import pallas as pl
from jax.experimental.pallas import tpu as pltpu
from jax.sharding import Mesh
from jax.sharding import PartitionSpec as P

BF = jnp.bfloat16
F32 = jnp.float32
NZ = 16
NT = 16
CAP = 12
TOK = 128
COL = 128
KD = 64
VD = 128
SP = ("z", "c")
SWAP = [(0, 1), (1, 0)]

NN = (((1,), (0,)), ((), ()))
NTR = (((1,), (1,)), ((), ()))
TN = (((0,), (0,)), ((), ()))


def mm(a, b, dims=NN):
    return lax.dot_general(a, b, dims, preferred_element_type=F32)


def halves(a):
    high = a.astype(BF)
    return high, (a - high.astype(F32)).astype(BF)


def exact(a, b, dims=NN):
    if a.dtype == BF:
        high, low = halves(b)
        return mm(a, high, dims) + mm(a, low, dims)
    high, low = halves(a)
    if b.dtype == BF:
        return mm(high, b, dims) + mm(low, b, dims)
    other, rest = halves(b)
    return mm(high, other, dims) + (mm(high, rest, dims) + mm(low, other, dims))


def vmem():
    return pl.BlockSpec(memory_space=pltpu.VMEM)


def hbm():
    return pl.BlockSpec(memory_space=pltpu.HBM)


def call(kernel, outs, args, name, mib=4, flops=1 << 27, stay=0, scratch=(), out=None):
    return pl.pallas_call(
        kernel,
        out_shape=outs,
        in_specs=[hbm()] * stay + [vmem()] * (len(args) - stay),
        out_specs=jax.tree.map(lambda _: (out or vmem)(), outs),
        scratch_shapes=scratch,
        name=name,
        compiler_params=pltpu.CompilerParams(vmem_limit_bytes=mib << 20),
        cost_estimate=pl.CostEstimate(flops=flops, bytes_accessed=1 << 20, transcendentals=0),
    )(*args)


def spot(axis):
    return lax.axis_index(axis).astype(jnp.int32)


def fetch(sources, targets, sems):
    copies = [
        pltpu.make_async_copy(src, dst, sems.at[n])
        for n, (src, dst) in enumerate(zip(sources, targets))
    ]
    for copy in copies:
        copy.start()
    for copy in copies:
        copy.wait()


def arr(shape, dtype):
    return jax.ShapeDtypeStruct(shape, dtype)


def placement(ids, wanted, rank):
    first = ids[0:1, :] == wanted
    match = first | (ids[1:2, :] == wanted)
    tok = TOK
    before = lax.broadcasted_iota(jnp.int32, (tok, tok), 0) < lax.broadcasted_iota(
        jnp.int32, (tok, tok), 1
    )
    ranks = mm(jnp.where(match, 1.0, 0.0).astype(BF), jnp.where(before, 1.0, 0.0).astype(BF))
    return match & (ranks == rank.astype(F32)), first


def decay_parts(rates):
    upto = lax.broadcasted_iota(jnp.int32, (TOK, TOK), 1) <= lax.broadcasted_iota(
        jnp.int32, (TOK, TOK), 0
    )
    col = jnp.broadcast_to(
        jnp.sum(jnp.where(upto, rates, 0.0), axis=1, keepdims=True), (TOK, TOK)
    )
    row = col.T
    total = jnp.sum(rates, axis=1, keepdims=True)
    prefix = row[0:1, :]
    start = jnp.exp(-prefix)
    end = jnp.exp(jnp.minimum(prefix - total, 0.0))
    return col, row, start, end, jnp.broadcast_to(total, (1, TOK))


def in_pieces(row):
    hi = row.astype(BF).astype(F32)
    mid = (row - hi).astype(BF).astype(F32)
    return jnp.concatenate([hi, mid, row - hi - mid], axis=0)


def in_one(pieces):
    pieces = pieces.astype(F32)
    return pieces[0:1, :] + pieces[1:2, :] + pieces[2:3, :]


def ids_of(rows):
    return rows[IDS - ROUTE : IDS - ROUTE + 2, :].astype(jnp.int32)


def rates_of(g_ref, block):
    return in_one(g_ref[block, ROUTE:HELD, :].astype(F32)[RATE - ROUTE : IDS - ROUTE])


COT, INP, KEY, VALUE, ROUTE, RATE, IDS, HELD = 0, 128, 256, 320, 448, 456, 459, 464


def load_kernel(
    ids_in, gw_in, ew_in, cot_in, inp_in, rate_in, k_in, v_in,
    out_ref, ids_ref, gw_ref, ew_ref, rate_ref, sems,
):
    here = pl.ds(pl.multiple_of(spot("tp") * COL, COL), COL)
    fetch(
        (ids_in, gw_in, ew_in, cot_in.at[:, here], inp_in.at[:, here], rate_in, k_in, v_in),
        (
            ids_ref, gw_ref, ew_ref, out_ref.at[pl.ds(COT, TOK)], out_ref.at[pl.ds(INP, TOK)],
            rate_ref, out_ref.at[pl.ds(KEY, KD)], out_ref.at[pl.ds(VALUE, VD)],
        ),
        sems,
    )
    weights = gw_ref[...] * ew_ref[...]
    none = jnp.zeros((2, TOK), F32)
    out_ref[ROUTE:HELD, :] = jnp.concatenate(
        [in_pieces(weights[0:1, :]), in_pieces(weights[1:2, :]), none]
        + [in_pieces(rate_ref[...]), ids_ref[...].astype(F32), none, none[0:1, :]],
        axis=0,
    ).astype(BF)


def pack_kernel(g_ref, rows_ref, picks_ref, small_ref, mine_ref):
    core = spot("c")
    number = lax.broadcasted_iota(jnp.int32, (NZ * 2 * CAP, TOK), 0)
    z = lax.shift_right_logical(number * 2731, 16)
    q = number - 2 * CAP * z
    first_half = q < CAP
    inp_rows = cot_rows = 0.0
    for block, wanted, rank in (
        (core, jnp.where(first_half, 2 * z + core, -1), q),
        (1 - core, jnp.where(first_half, -1, 2 * z + core), q - CAP),
    ):
        rows = g_ref[block, ROUTE:HELD, :].astype(F32)
        hit, first = placement(ids_of(rows), wanted, rank)
        scale = jnp.sum(
            jnp.where(hit, jnp.where(first, in_one(rows[0:3]), in_one(rows[3:6])), 0.0),
            axis=1,
            keepdims=True,
        )
        take = jnp.where(hit, 1.0, 0.0).astype(BF)
        if block is core:
            picks_ref[0:384, :] = take
        inp_rows = inp_rows + mm(take, g_ref[block, INP : INP + TOK, :])
        cot_rows = cot_rows + mm(take, g_ref[block, COT : COT + TOK, :]) * scale
    for z in range(NZ):
        part = slice(2 * CAP * z, 2 * CAP * (z + 1))
        rows_ref[z, 0 : 2 * CAP, :] = inp_rows[part].astype(BF)
        rows_ref[z, 2 * CAP : 4 * CAP, :] = cot_rows[part].astype(BF)
    z = lax.shift_right_logical(number * 2731, 16)
    hit, _ = placement(
        ids_of(g_ref[core, ROUTE:HELD, :].astype(F32)),
        jnp.where(first_half, -1, 2 * z + 1 - core),
        q - CAP,
    )
    picks_ref[384:768, :] = jnp.where(hit, 1.0, 0.0).astype(BF)

    _, _, start_a, end_a, total_a = decay_parts(rates_of(g_ref, 0))
    _, _, start_b, end_b, total_b = decay_parts(rates_of(g_ref, 1))
    half = pl.ds(pl.multiple_of(KEY + 32 * core, 32), 32)
    keys = jnp.concatenate([g_ref[0, half, :], g_ref[1, half, :]], axis=1).astype(F32)
    values = jnp.concatenate([g_ref[k, VALUE : VALUE + VD, :] for k in (0, 1)], axis=1)
    early = jnp.concatenate([end_a * jnp.exp(-total_b), end_b], axis=1)
    late = jnp.concatenate([start_a, start_b * jnp.exp(-total_a)], axis=1)
    small_ref[0:32, :] = exact(keys * early, values, NTR).astype(BF)
    small_ref[32:64, :] = exact(keys * late, values, NTR).astype(BF)
    small_ref[64:72, :] = jnp.concatenate(
        [in_pieces(total_a + total_b), jnp.zeros((5, TOK), F32)], axis=0
    ).astype(BF)
    is_first = core == 0
    mine_ref[...] = jnp.concatenate(
        [
            jnp.where(is_first, start_a, start_b), jnp.where(is_first, end_a, end_b),
            jnp.where(is_first, total_a, total_b), jnp.where(is_first, total_b, total_a),
            jnp.zeros((4, TOK), F32),
        ],
        axis=0,
    )


def spread_kernel(got_ref, rows_ref):
    for z in range(NZ):
        for kind in range(2):
            part = got_ref[z, 24 * kind : 24 * (kind + 1), :]
            for k in range(4):
                rows_ref[k, kind, 24 * z : 24 * (z + 1), :] = part


def expert_kernel(x_ref, gw_ref, uw_ref, dw_ref, part_ref, hid_ref, both_ref):
    inp = jnp.concatenate([x_ref[held_at(t), 0] for t in range(NT)], axis=1)
    cot = jnp.concatenate([x_ref[held_at(t), 1] for t in range(NT)], axis=1)
    both_w = jnp.concatenate([gw_ref[...], uw_ref[...]], axis=1)
    pre = mm(inp, both_w)
    gate, up = pre[:, :128], pre[:, 128:]
    hidden_grad = mm(cot, dw_ref[...], NTR)
    sig = jax.nn.sigmoid(gate)
    act = gate * sig
    hid_ref[...] = (act * up).astype(BF)
    gate_grad = (hidden_grad * up * sig * (1.0 + gate * (1.0 - sig))).astype(BF)
    up_grad = (hidden_grad * act).astype(BF)
    both = jnp.concatenate([gate_grad, up_grad], axis=1)
    both_ref[...] = both
    for t in range(0, NT, 2):
        out = mm(both, both_w[t * COL : (t + 2) * COL], NTR).astype(BF)
        part_ref[t] = out[:, :COL]
        part_ref[t + 1] = out[:, COL:]


def weight_kernel(
    x_ref, hid_ref, both_ref, gg_out, gu_out, gd_out, gg_ref, gu_ref, gd_ref, sems
):
    both = both_ref[...].T
    hidden = hid_ref[...].T
    copies = []
    for t in range(0, NT, 2):
        rows = slice(t * COL, (t + 2) * COL)
        inp = jnp.concatenate([x_ref[held_at(t), 0], x_ref[held_at(t + 1), 0]], axis=1)
        cot = jnp.concatenate([x_ref[held_at(t), 1], x_ref[held_at(t + 1), 1]], axis=1)
        out = mm(both, inp).astype(BF).T
        gg_ref[rows, :] = out[:, :128]
        gu_ref[rows, :] = out[:, 128:]
        gd_ref[:, rows] = mm(hidden, cot).astype(BF)
        if t % 4 == 2:
            done = pl.ds((t - 2) * COL, 4 * COL)
            for n, (src, dst) in enumerate(
                (
                    (gg_ref.at[done], gg_out.at[done]), (gu_ref.at[done], gu_out.at[done]),
                    (gd_ref.at[:, done], gd_out.at[:, done]),
                )
            ):
                copies.append(pltpu.make_async_copy(src, dst, sems.at[t // 4, n]))
                copies[-1].start()
    for copy in copies:
        copy.wait()


def chip_states(early, late, early_other, late_other, mine, theirs):
    is_first = spot("c") == 0
    both_early = early * jnp.where(is_first, theirs, 1.0) + early_other * jnp.where(
        is_first, 1.0, mine
    )
    both_late = late * jnp.where(is_first, 1.0, theirs) + late_other * jnp.where(
        is_first, mine, 1.0
    )
    return [jnp.where(is_first, a[:32], a[32:]).astype(BF) for a in (both_early, both_late)]


def sum_kernel(part_ref, small_ref, out_ref):
    total = part_ref[0].astype(F32)
    for t in range(1, NT):
        total = total + part_ref[t].astype(F32)
    out_ref[:, 0 : 2 * CAP, :] = total.reshape(NZ, 2 * CAP, COL).astype(BF)
    early, late, pieces = small_ref[0:32, :], small_ref[32:64, :], small_ref[64:72, :]
    place = spot("z")
    for z in range(NZ):
        out_ref[z, 24:56, :] = jnp.where(z > place, early, late)
        out_ref[z, 56:64, :] = pieces


def resid_kernel(picks_ref, own_ref, other_ref, g_ref, out_ref):
    own, other = [
        r[:, 0 : 2 * CAP, :].astype(F32).reshape(384, COL).astype(BF) for r in (own_ref, other_ref)
    ]
    moe = mm(picks_ref[0:384, :], own, TN) + mm(picks_ref[384:768, :], other, TN)
    cot = g_ref[spot("c"), COT : COT + TOK, :]
    resid = (cot.astype(F32) + moe).astype(BF)
    for t in range(NT):
        out_ref[t] = resid


def proj_kernel(r_ref, p_ref, mixer_ref, q_ref, mine_ref, og_ref, keep_ref, send_ref, state_ref):
    core = spot("c")
    resid = jnp.concatenate([r_ref[t] for t in range(NT)], axis=1)
    out_grad = mm(resid, p_ref[...])
    og_ref[...] = out_grad
    query = q_ref[...].astype(F32)
    early = exact(query * mine_ref[1:2, :], out_grad)
    late = exact(query * mine_ref[0:1, :], out_grad)
    state_ref[0] = early
    state_ref[1] = late
    send_ref[16] = early.astype(BF)
    send_ref[17] = late.astype(BF)
    mixer = mixer_ref[...]
    for t in range(NT):
        share = mm(r_ref[t], mixer, TN)
        low, high = share[:64], share[64:]
        keep_ref[t] = jnp.where(core == 0, low, high)
        send_ref[t] = jnp.where(core == 0, high, low).astype(BF)


def at_block(far_early, far_late, near, theirs):
    is_first = spot("c") == 0
    early = far_early * jnp.where(is_first, 1.0, theirs) + jnp.where(is_first, 0.0, near)
    late = far_late * jnp.where(is_first, theirs, 1.0) + jnp.where(is_first, near, 0.0)
    return early, late


def intra_kernel(
    og_ref, q_ref, g_ref, mine_ref, own_ref, other_ref, gq_ref, part_ref, weight_ref
):
    place, core = spot("z"), spot("c")
    rows = own_ref[:, 56:64, :].astype(F32)
    chip = rows[:, 0, :] + rows[:, 1, :] + rows[:, 2, :]
    number = lax.broadcasted_iota(jnp.int32, (NZ, COL), 0)
    between = jnp.zeros((NZ, COL), F32)
    for u in range(NZ):
        inside = ((number < u) & (u < place)) | ((number > u) & (u > place))
        between = between + jnp.where(inside, chip[u : u + 1, :], 0.0)
    weight = jnp.exp(-between)
    early_w = jnp.where(number < place, weight, 0.0)
    late_w = jnp.where(number > place, weight, 0.0)
    weight_ref[0:16, :] = early_w
    weight_ref[16:32, :] = late_w

    def far(ref):
        early = late = jnp.zeros((32, COL), F32)
        for z in range(NZ):
            state = ref[z, 24:56, :].astype(F32)
            early = early + state * early_w[z : z + 1, :]
            late = late + state * late_w[z : z + 1, :]
        return early, late

    is_first = core == 0
    here, there = far(own_ref), far(other_ref)
    far_early, far_late = [
        jnp.concatenate([jnp.where(is_first, a, b), jnp.where(is_first, b, a)], axis=0)
        for a, b in zip(here, there)
    ]
    _, _, start, end, _ = decay_parts(rates_of(g_ref, 1 - core))
    there = g_ref[1 - core, KEY : KEY + KD, :].astype(F32) * jnp.where(is_first, start, end)
    near = exact(there, g_ref[1 - core, VALUE : VALUE + VD, :], NTR)
    theirs = jnp.exp(-mine_ref[3:4, :])
    kv_early, kv_late = at_block(far_early, far_late, near, theirs)
    scale = KD ** (-0.5)
    col, row, start, end, _ = decay_parts(rates_of(g_ref, core))
    low, high = scale * start, scale * end
    mixed = scale * jnp.exp(-jnp.abs(col - row))
    out_grad = og_ref[...]
    query, key = q_ref[...], g_ref[core, KEY : KEY + KD, :]
    value = g_ref[core, VALUE : VALUE + VD, :]
    score_grad = exact(out_grad, value) * mixed
    gq_ref[...] = (
        exact(key, score_grad, NTR)
        + low * exact(kv_early, out_grad, NTR)
        + high * exact(kv_late, out_grad, NTR)
    )
    part_ref[0:64, :] = exact(query, score_grad)
    part_ref[64:192, :] = exact(out_grad, mm(query, key, TN) * mixed, TN)
    part_ref[192:256, :] = key.astype(F32)
    part_ref[256:384, :] = value.astype(F32)
    part_ref[384:392, :] = jnp.concatenate([low, high, theirs, jnp.zeros((5, TOK), F32)], axis=0)


def chip_kernel(keep_ref, got_ref, state_ref, mine_ref, out_ref, near_ref):
    place, core = spot("z"), spot("c")
    mine, theirs = jnp.exp(-mine_ref[2:3, :]), jnp.exp(-mine_ref[3:4, :])
    early_other, late_other = got_ref[16].astype(F32), got_ref[17].astype(F32)
    early, late = chip_states(state_ref[0], state_ref[1], early_other, late_other, mine, theirs)
    near_ref[...] = jnp.where(core == 0, late_other, early_other)
    for z in range(NZ):
        out_ref[z, 0:64, :] = (keep_ref[z] + got_ref[z].astype(F32)).astype(BF)
        out_ref[z, 64:96, :] = jnp.where(z > place, early, late)


def gather_kernel(got_ref, weight_ref, state_ref):
    early = late = jnp.zeros((32, COL), F32)
    for z in range(NZ):
        state = got_ref[z, 64:96, :].astype(F32)
        early = early + state * weight_ref[z : z + 1, :]
        late = late + state * weight_ref[16 + z : 17 + z, :]
    state_ref[0] = early
    state_ref[1] = late


def final_kernel(far_ref, near_ref, part_ref, got_ref, proj_ref, gk_ref, gv_ref):
    share = jnp.zeros((64, COL), F32)
    for z in range(NZ):
        share = share + got_ref[z, 0:64, :].astype(F32)
    proj_ref[...] = share
    early, late = at_block(
        jnp.concatenate([far_ref[0, 0], far_ref[1, 0]], axis=0),
        jnp.concatenate([far_ref[0, 1], far_ref[1, 1]], axis=0),
        near_ref[...],
        part_ref[386:387, :],
    )
    low, high = part_ref[384:385, :], part_ref[385:386, :]
    key, value = part_ref[192:256, :].astype(BF), part_ref[256:384, :].astype(BF)
    gk_ref[...] = part_ref[0:64, :] + low * exact(early, value) + high * exact(late, value)
    gv_ref[...] = part_ref[64:192, :] + low * exact(early, key, TN) + high * exact(late, key, TN)


def groups(step, stride, step_other, stride_other):
    first = [[stride * g + step * k for k in range(4)] for g in range(4)]
    second = [[16 + stride_other * g + step_other * k for k in range(4)] for g in range(4)]
    return first + second


def within(blocks, axis, sets):
    return lax.all_to_all(
        blocks, axis, split_axis=0, concat_axis=0, axis_index_groups=sets, tiled=True
    )


def to_all(shard, axis, sets):
    return within(jnp.broadcast_to(shard, (len(sets[0]), *shard.shape)), axis, sets)


def exchange(blocks, axis):
    return lax.all_to_all(blocks, axis, split_axis=0, concat_axis=0, tiled=True)


def held_at(t):
    return jnp.where(spot("c") == 0, (t % 4) * 4 + t // 4, t)


def on_device(
    cotangent, moe_input, expert_ids, group_weight, expert_weight, mixer_out,
    queries, key_vectors, value_vectors, decay_rates, proj_weight,
    gate_weight, up_weight, down_weight,
):
    ids = expert_ids.T
    held = call(
        load_kernel,
        arr((HELD, COL), BF),
        (
            ids, group_weight.reshape(1, TOK), expert_weight.T, cotangent, moe_input,
            decay_rates, key_vectors, value_vectors,
        ),
        "load",
        60,
        stay=8,
        scratch=[
            pltpu.VMEM((2, TOK), jnp.int32), pltpu.VMEM((1, TOK), F32), pltpu.VMEM((2, TOK), F32),
            pltpu.VMEM((1, TOK), F32), pltpu.SemaphoreType.DMA((8,)),
        ],
    )
    held = lax.all_gather(held, "c")
    rows, picks, small, mine = call(
        pack_kernel,
        [
            arr((NZ, 4 * CAP, COL), BF), arr((768, TOK), BF), arr((72, COL), BF),
            arr((8, TOK), F32),
        ],
        (held,),
        "pack",
    )
    rows = exchange(rows, "z")
    copies = call(spread_kernel, arr((4, 2, NZ * 2 * CAP, COL), BF), (rows,), "spread")
    rows = within(copies, ("c", "tp"), groups(4, 1, 1, 4))
    rows = to_all(rows.reshape(4, 2, NZ * 2 * CAP, COL), ("c", "tp"), groups(1, 4, 4, 1))
    rows = rows.reshape(NT, 2, NZ * 2 * CAP, COL)
    shares, hidden, both = call(
        expert_kernel,
        [arr((NT, 384, COL), BF), arr((384, 128), BF), arr((384, 256), BF)],
        (rows, gate_weight[0], up_weight[0], down_weight[0]),
        "expert",
        20,
    )
    shares = exchange(shares, "tp")
    back = call(sum_kernel, arr((NZ, 64, COL), BF), (shares, small), "sums", 6)
    own = exchange(back, "z")
    own, rows, hidden, both = lax.optimization_barrier((own, rows, hidden, both))
    other = lax.ppermute(own, "c", SWAP)
    shapes = [arr((2048, 128), BF), arr((2048, 128), BF), arr((128, 2048), BF)]
    grad_gate, grad_up, grad_down = call(
        weight_kernel,
        shapes,
        (rows, hidden, both),
        "weights",
        16,
        1 << 29,
        scratch=[pltpu.VMEM(a.shape, BF) for a in shapes] + [pltpu.SemaphoreType.DMA((4, 3))],
        out=hbm,
    )
    resid = call(resid_kernel, arr((NT, TOK, COL), BF), (picks, own, other, held), "resid")
    resid, grad_gate, grad_up, grad_down = lax.optimization_barrier(
        (resid, grad_gate, grad_up, grad_down)
    )
    resid = exchange(resid, "tp")
    out_grad, proj_keep, proj_send, state = call(
        proj_kernel,
        [
            arr((TOK, VD), F32), arr((NZ, 64, COL), F32), arr((18, 64, COL), BF),
            arr((2, KD, VD), F32),
        ],
        (resid, proj_weight, mixer_out, queries, mine),
        "proj",
        8,
    )
    got = lax.ppermute(proj_send, "c", SWAP)
    grad_queries, part, weight = call(
        intra_kernel,
        [arr((KD, TOK), F32), arr((392, TOK), F32), arr((32, TOK), F32)],
        (out_grad, queries, held, mine, own, other),
        "intra",
    )
    chip, near = call(
        chip_kernel,
        [arr((NZ, 96, COL), BF), arr((KD, VD), F32)],
        (proj_keep, got, state, mine),
        "chip",
    )
    chip, grad_queries, part, weight = lax.optimization_barrier((chip, grad_queries, part, weight))
    chip = exchange(chip, "z")
    far = call(gather_kernel, arr((2, 32, COL), F32), (chip, weight), "gather")
    far = lax.all_gather(far, "c")
    grad_proj, grad_keys, grad_values = call(
        final_kernel,
        [arr((64, COL), F32), arr((KD, TOK), F32), arr((VD, TOK), F32)],
        (far, near, part, chip),
        "final",
    )
    return (
        grad_gate[None], grad_up[None], grad_down[None],
        grad_proj, grad_queries, grad_keys, grad_values,
    )


def solution(mesh):
    finer = Mesh(mesh.devices.reshape(NZ, 2, NT), ("z", "c", "tp"))
    in_specs = (
        P(SP, None), P(SP, None), P(SP, None), P(SP), P(SP, None), P(SP, "tp"),
        P("tp", SP), P("tp", SP), P("tp", SP), P("tp", SP), P(None, "tp"),
        P(SP, None, "tp"), P(SP, None, "tp"), P(SP, "tp", None),
    )
    out_specs = (
        P(SP, None, "tp"), P(SP, None, "tp"), P(SP, "tp", None), P(SP, "tp"),
        P("tp", SP), P("tp", SP), P("tp", SP),
    )
    return jax.shard_map(
        on_device, mesh=finer, in_specs=in_specs, out_specs=out_specs, check_vma=False
    )
```

```python
import jax
import jax.numpy as jnp
from jax import lax
from jax.experimental import pallas as pl
from jax.experimental.pallas import tpu as pltpu
from jax.sharding import Mesh
from jax.sharding import PartitionSpec as P

BF = jnp.bfloat16
F32 = jnp.float32
NZ = 16
NT = 16
CAP = 12
TOK = 128
COL = 128
KD = 64
VD = 128
SP = ("z", "c")
SWAP = [(0, 1), (1, 0)]

NN = (((1,), (0,)), ((), ()))
NTR = (((1,), (1,)), ((), ()))
TN = (((0,), (0,)), ((), ()))


def mm(a, b, dims=NN):
    return lax.dot_general(a, b, dims, preferred_element_type=F32)


def halves(a):
    high = a.astype(BF)
    return high, (a - high.astype(F32)).astype(BF)


def exact(a, b, dims=NN):
    if a.dtype == BF:
        high, low = halves(b)
        return mm(a, high, dims) + mm(a, low, dims)
    high, low = halves(a)
    if b.dtype == BF:
        return mm(high, b, dims) + mm(low, b, dims)
    other, rest = halves(b)
    return mm(high, other, dims) + (mm(high, rest, dims) + mm(low, other, dims))


def vmem():
    return pl.BlockSpec(memory_space=pltpu.VMEM)


def hbm():
    return pl.BlockSpec(memory_space=pltpu.HBM)


def call(kernel, outs, args, name, mib=4, flops=1 << 27, stay=0, scratch=()):
    return pl.pallas_call(
        kernel,
        out_shape=outs,
        in_specs=[hbm()] * stay + [vmem()] * (len(args) - stay),
        out_specs=jax.tree.map(lambda _: vmem(), outs),
        scratch_shapes=scratch,
        name=name,
        compiler_params=pltpu.CompilerParams(vmem_limit_bytes=mib << 20),
        cost_estimate=pl.CostEstimate(flops=flops, bytes_accessed=1 << 20, transcendentals=0),
    )(*args)


def spot(axis):
    return lax.axis_index(axis).astype(jnp.int32)


def fetch(sources, targets, sems):
    copies = [
        pltpu.make_async_copy(src, dst, sems.at[n])
        for n, (src, dst) in enumerate(zip(sources, targets))
    ]
    for copy in copies:
        copy.start()
    for copy in copies:
        copy.wait()


def arr(shape, dtype):
    return jax.ShapeDtypeStruct(shape, dtype)


def placement(ids, wanted, rank):
    first = ids[0:1, :] == wanted
    match = first | (ids[1:2, :] == wanted)
    tok = TOK
    before = lax.broadcasted_iota(jnp.int32, (tok, tok), 0) < lax.broadcasted_iota(
        jnp.int32, (tok, tok), 1
    )
    ranks = mm(jnp.where(match, 1.0, 0.0).astype(BF), jnp.where(before, 1.0, 0.0).astype(BF))
    return match & (ranks == rank.astype(F32)), first


def decay_parts(rates):
    upto = lax.broadcasted_iota(jnp.int32, (TOK, TOK), 1) <= lax.broadcasted_iota(
        jnp.int32, (TOK, TOK), 0
    )
    col = jnp.broadcast_to(
        jnp.sum(jnp.where(upto, rates, 0.0), axis=1, keepdims=True), (TOK, TOK)
    )
    row = col.T
    total = jnp.sum(rates, axis=1, keepdims=True)
    prefix = row[0:1, :]
    start = jnp.exp(-prefix)
    end = jnp.exp(jnp.minimum(prefix - total, 0.0))
    return col, row, start, end, jnp.broadcast_to(total, (1, TOK))


def in_pieces(row):
    hi = row.astype(BF).astype(F32)
    mid = (row - hi).astype(BF).astype(F32)
    return jnp.concatenate([hi, mid, row - hi - mid], axis=0)


def in_one(pieces):
    pieces = pieces.astype(F32)
    return pieces[0:1, :] + pieces[1:2, :] + pieces[2:3, :]


def ids_of(rows):
    return rows[IDS - ROUTE : IDS - ROUTE + 2, :].astype(jnp.int32)


def rates_of(g_ref, block):
    return in_one(g_ref[block, ROUTE:HELD, :].astype(F32)[RATE - ROUTE : IDS - ROUTE])


COT, INP, KEY, VALUE, ROUTE, RATE, IDS, HELD = 0, 128, 256, 320, 448, 456, 459, 464


def load_kernel(
    ids_in, gw_in, ew_in, cot_in, inp_in, rate_in, k_in, v_in,
    out_ref, ids_ref, gw_ref, ew_ref, rate_ref, sems,
):
    here = pl.ds(pl.multiple_of(spot("tp") * COL, COL), COL)
    fetch(
        (ids_in, gw_in, ew_in, cot_in.at[:, here], inp_in.at[:, here], rate_in, k_in, v_in),
        (
            ids_ref, gw_ref, ew_ref, out_ref.at[pl.ds(COT, TOK)], out_ref.at[pl.ds(INP, TOK)],
            rate_ref, out_ref.at[pl.ds(KEY, KD)], out_ref.at[pl.ds(VALUE, VD)],
        ),
        sems,
    )
    weights = gw_ref[...] * ew_ref[...]
    none = jnp.zeros((2, TOK), F32)
    out_ref[ROUTE:HELD, :] = jnp.concatenate(
        [in_pieces(weights[0:1, :]), in_pieces(weights[1:2, :]), none]
        + [in_pieces(rate_ref[...]), ids_ref[...].astype(F32), none, none[0:1, :]],
        axis=0,
    ).astype(BF)


def pack_kernel(g_ref, rows_ref, picks_ref, small_ref, mine_ref):
    core = spot("c")
    number = lax.broadcasted_iota(jnp.int32, (NZ * 2 * CAP, TOK), 0)
    z = lax.shift_right_logical(number * 2731, 16)
    q = number - 2 * CAP * z
    first_half = q < CAP
    inp_rows = cot_rows = 0.0
    for block, wanted, rank in (
        (core, jnp.where(first_half, 2 * z + core, -1), q),
        (1 - core, jnp.where(first_half, -1, 2 * z + core), q - CAP),
    ):
        rows = g_ref[block, ROUTE:HELD, :].astype(F32)
        hit, first = placement(ids_of(rows), wanted, rank)
        scale = jnp.sum(
            jnp.where(hit, jnp.where(first, in_one(rows[0:3]), in_one(rows[3:6])), 0.0),
            axis=1,
            keepdims=True,
        )
        take = jnp.where(hit, 1.0, 0.0).astype(BF)
        if block is core:
            picks_ref[0:384, :] = take
        inp_rows = inp_rows + mm(take, g_ref[block, INP : INP + TOK, :])
        cot_rows = cot_rows + mm(take, g_ref[block, COT : COT + TOK, :]) * scale
    for z in range(NZ):
        part = slice(2 * CAP * z, 2 * CAP * (z + 1))
        rows_ref[z, 0 : 2 * CAP, :] = inp_rows[part].astype(BF)
        rows_ref[z, 2 * CAP : 4 * CAP, :] = cot_rows[part].astype(BF)
    z = lax.shift_right_logical(number * 2731, 16)
    hit, _ = placement(
        ids_of(g_ref[core, ROUTE:HELD, :].astype(F32)),
        jnp.where(first_half, -1, 2 * z + 1 - core),
        q - CAP,
    )
    picks_ref[384:768, :] = jnp.where(hit, 1.0, 0.0).astype(BF)

    _, _, start_a, end_a, total_a = decay_parts(rates_of(g_ref, 0))
    _, _, start_b, end_b, total_b = decay_parts(rates_of(g_ref, 1))
    half = pl.ds(pl.multiple_of(KEY + 32 * core, 32), 32)
    keys = jnp.concatenate([g_ref[0, half, :], g_ref[1, half, :]], axis=1).astype(F32)
    values = jnp.concatenate([g_ref[k, VALUE : VALUE + VD, :] for k in (0, 1)], axis=1)
    early = jnp.concatenate([end_a * jnp.exp(-total_b), end_b], axis=1)
    late = jnp.concatenate([start_a, start_b * jnp.exp(-total_a)], axis=1)
    small_ref[0:32, :] = exact(keys * early, values, NTR).astype(BF)
    small_ref[32:64, :] = exact(keys * late, values, NTR).astype(BF)
    small_ref[64:72, :] = jnp.concatenate(
        [in_pieces(total_a + total_b), jnp.zeros((5, TOK), F32)], axis=0
    ).astype(BF)
    is_first = core == 0
    mine_ref[...] = jnp.concatenate(
        [
            jnp.where(is_first, start_a, start_b), jnp.where(is_first, end_a, end_b),
            jnp.where(is_first, total_a, total_b), jnp.where(is_first, total_b, total_a),
            jnp.zeros((4, TOK), F32),
        ],
        axis=0,
    )


def spread_kernel(got_ref, rows_ref):
    for z in range(NZ):
        for kind in range(2):
            part = got_ref[z, 24 * kind : 24 * (kind + 1), :]
            for k in range(4):
                rows_ref[k, kind, 24 * z : 24 * (z + 1), :] = part


def expert_kernel(x_ref, gw_ref, uw_ref, dw_ref, part_ref, hid_ref, both_ref):
    inp = jnp.concatenate([x_ref[held_at(t), 0] for t in range(NT)], axis=1)
    cot = jnp.concatenate([x_ref[held_at(t), 1] for t in range(NT)], axis=1)
    both_w = jnp.concatenate([gw_ref[...], uw_ref[...]], axis=1)
    pre = mm(inp, both_w)
    gate, up = pre[:, :128], pre[:, 128:]
    hidden_grad = mm(cot, dw_ref[...], NTR)
    sig = jax.nn.sigmoid(gate)
    act = gate * sig
    hid_ref[...] = (act * up).astype(BF)
    gate_grad = (hidden_grad * up * sig * (1.0 + gate * (1.0 - sig))).astype(BF)
    up_grad = (hidden_grad * act).astype(BF)
    both = jnp.concatenate([gate_grad, up_grad], axis=1)
    both_ref[...] = both
    for t in range(0, NT, 2):
        out = mm(both, both_w[t * COL : (t + 2) * COL], NTR).astype(BF)
        part_ref[t] = out[:, :COL]
        part_ref[t + 1] = out[:, COL:]


def weight_kernel(x_ref, hid_ref, both_ref, gg_ref, gu_ref, gd_ref):
    both = both_ref[...]
    hidden = hid_ref[...]
    for t in range(0, NT, 2):
        rows = slice(t * COL, (t + 2) * COL)
        inp = jnp.concatenate([x_ref[held_at(t), 0], x_ref[held_at(t + 1), 0]], axis=1)
        cot = jnp.concatenate([x_ref[held_at(t), 1], x_ref[held_at(t + 1), 1]], axis=1)
        out = mm(inp, both, TN).astype(BF)
        gg_ref[rows, :] = out[:, :128]
        gu_ref[rows, :] = out[:, 128:]
        gd_ref[:, rows] = mm(hidden, cot, TN).astype(BF)


def chip_states(early, late, early_other, late_other, mine, theirs):
    is_first = spot("c") == 0
    both_early = early * jnp.where(is_first, theirs, 1.0) + early_other * jnp.where(
        is_first, 1.0, mine
    )
    both_late = late * jnp.where(is_first, 1.0, theirs) + late_other * jnp.where(
        is_first, mine, 1.0
    )
    return [jnp.where(is_first, a[:32], a[32:]).astype(BF) for a in (both_early, both_late)]


def sum_kernel(part_ref, small_ref, out_ref):
    total = part_ref[0].astype(F32)
    for t in range(1, NT):
        total = total + part_ref[t].astype(F32)
    out_ref[:, 0 : 2 * CAP, :] = total.reshape(NZ, 2 * CAP, COL).astype(BF)
    early, late, pieces = small_ref[0:32, :], small_ref[32:64, :], small_ref[64:72, :]
    place = spot("z")
    for z in range(NZ):
        out_ref[z, 24:56, :] = jnp.where(z > place, early, late)
        out_ref[z, 56:64, :] = pieces


def resid_kernel(picks_ref, own_ref, other_ref, g_ref, out_ref):
    own, other = [
        r[:, 0 : 2 * CAP, :].astype(F32).reshape(384, COL).astype(BF) for r in (own_ref, other_ref)
    ]
    moe = mm(picks_ref[0:384, :], own, TN) + mm(picks_ref[384:768, :], other, TN)
    cot = g_ref[spot("c"), COT : COT + TOK, :]
    resid = (cot.astype(F32) + moe).astype(BF)
    for t in range(NT):
        out_ref[t] = resid


def proj_kernel(r_ref, p_ref, mixer_ref, q_ref, mine_ref, og_ref, keep_ref, send_ref, state_ref):
    core = spot("c")
    resid = jnp.concatenate([r_ref[t] for t in range(NT)], axis=1)
    out_grad = mm(resid, p_ref[...])
    og_ref[...] = out_grad
    query = q_ref[...].astype(F32)
    early = exact(query * mine_ref[1:2, :], out_grad)
    late = exact(query * mine_ref[0:1, :], out_grad)
    state_ref[0] = early
    state_ref[1] = late
    send_ref[16] = early.astype(BF)
    send_ref[17] = late.astype(BF)
    mixer = mixer_ref[...]
    for t in range(NT):
        share = mm(r_ref[t], mixer, TN)
        low, high = share[:64], share[64:]
        keep_ref[t] = jnp.where(core == 0, low, high)
        send_ref[t] = jnp.where(core == 0, high, low).astype(BF)


def at_block(far_early, far_late, near, theirs):
    is_first = spot("c") == 0
    early = far_early * jnp.where(is_first, 1.0, theirs) + jnp.where(is_first, 0.0, near)
    late = far_late * jnp.where(is_first, theirs, 1.0) + jnp.where(is_first, near, 0.0)
    return early, late


def intra_kernel(
    og_ref, q_ref, g_ref, mine_ref, own_ref, other_ref, gq_ref, part_ref, weight_ref
):
    place, core = spot("z"), spot("c")
    rows = own_ref[:, 56:64, :].astype(F32)
    chip = rows[:, 0, :] + rows[:, 1, :] + rows[:, 2, :]
    number = lax.broadcasted_iota(jnp.int32, (NZ, COL), 0)
    between = jnp.zeros((NZ, COL), F32)
    for u in range(NZ):
        inside = ((number < u) & (u < place)) | ((number > u) & (u > place))
        between = between + jnp.where(inside, chip[u : u + 1, :], 0.0)
    weight = jnp.exp(-between)
    early_w = jnp.where(number < place, weight, 0.0)
    late_w = jnp.where(number > place, weight, 0.0)
    weight_ref[0:16, :] = early_w
    weight_ref[16:32, :] = late_w

    def far(ref):
        early = late = jnp.zeros((32, COL), F32)
        for z in range(NZ):
            state = ref[z, 24:56, :].astype(F32)
            early = early + state * early_w[z : z + 1, :]
            late = late + state * late_w[z : z + 1, :]
        return early, late

    is_first = core == 0
    here, there = far(own_ref), far(other_ref)
    far_early, far_late = [
        jnp.concatenate([jnp.where(is_first, a, b), jnp.where(is_first, b, a)], axis=0)
        for a, b in zip(here, there)
    ]
    _, _, start, end, _ = decay_parts(rates_of(g_ref, 1 - core))
    there = g_ref[1 - core, KEY : KEY + KD, :].astype(F32) * jnp.where(is_first, start, end)
    near = exact(there, g_ref[1 - core, VALUE : VALUE + VD, :], NTR)
    theirs = jnp.exp(-mine_ref[3:4, :])
    kv_early, kv_late = at_block(far_early, far_late, near, theirs)
    scale = KD ** (-0.5)
    col, row, start, end, _ = decay_parts(rates_of(g_ref, core))
    low, high = scale * start, scale * end
    mixed = scale * jnp.exp(-jnp.abs(col - row))
    out_grad = og_ref[...]
    query, key = q_ref[...], g_ref[core, KEY : KEY + KD, :]
    value = g_ref[core, VALUE : VALUE + VD, :]
    score_grad = exact(out_grad, value) * mixed
    gq_ref[...] = (
        exact(key, score_grad, NTR)
        + low * exact(kv_early, out_grad, NTR)
        + high * exact(kv_late, out_grad, NTR)
    )
    part_ref[0:64, :] = exact(query, score_grad)
    part_ref[64:192, :] = exact(out_grad, mm(query, key, TN) * mixed, TN)
    part_ref[192:256, :] = key.astype(F32)
    part_ref[256:384, :] = value.astype(F32)
    part_ref[384:392, :] = jnp.concatenate([low, high, theirs, jnp.zeros((5, TOK), F32)], axis=0)


def chip_kernel(keep_ref, got_ref, state_ref, mine_ref, out_ref, near_ref):
    place, core = spot("z"), spot("c")
    mine, theirs = jnp.exp(-mine_ref[2:3, :]), jnp.exp(-mine_ref[3:4, :])
    early_other, late_other = got_ref[16].astype(F32), got_ref[17].astype(F32)
    early, late = chip_states(state_ref[0], state_ref[1], early_other, late_other, mine, theirs)
    near_ref[...] = jnp.where(core == 0, late_other, early_other)
    for z in range(NZ):
        out_ref[z, 0:64, :] = (keep_ref[z] + got_ref[z].astype(F32)).astype(BF)
        out_ref[z, 64:96, :] = jnp.where(z > place, early, late)


def gather_kernel(got_ref, weight_ref, state_ref):
    early = late = jnp.zeros((32, COL), F32)
    for z in range(NZ):
        state = got_ref[z, 64:96, :].astype(F32)
        early = early + state * weight_ref[z : z + 1, :]
        late = late + state * weight_ref[16 + z : 17 + z, :]
    state_ref[0] = early
    state_ref[1] = late


def final_kernel(far_ref, near_ref, part_ref, got_ref, proj_ref, gk_ref, gv_ref):
    share = jnp.zeros((64, COL), F32)
    for z in range(NZ):
        share = share + got_ref[z, 0:64, :].astype(F32)
    proj_ref[...] = share
    early, late = at_block(
        jnp.concatenate([far_ref[0, 0], far_ref[1, 0]], axis=0),
        jnp.concatenate([far_ref[0, 1], far_ref[1, 1]], axis=0),
        near_ref[...],
        part_ref[386:387, :],
    )
    low, high = part_ref[384:385, :], part_ref[385:386, :]
    key, value = part_ref[192:256, :].astype(BF), part_ref[256:384, :].astype(BF)
    gk_ref[...] = part_ref[0:64, :] + low * exact(early, value) + high * exact(late, value)
    gv_ref[...] = part_ref[64:192, :] + low * exact(early, key, TN) + high * exact(late, key, TN)


def groups(step, stride, step_other, stride_other):
    first = [[stride * g + step * k for k in range(4)] for g in range(4)]
    second = [[16 + stride_other * g + step_other * k for k in range(4)] for g in range(4)]
    return first + second


def within(blocks, axis, sets):
    return lax.all_to_all(
        blocks, axis, split_axis=0, concat_axis=0, axis_index_groups=sets, tiled=True
    )


def to_all(shard, axis, sets):
    return within(jnp.broadcast_to(shard, (len(sets[0]), *shard.shape)), axis, sets)


def exchange(blocks, axis):
    return lax.all_to_all(blocks, axis, split_axis=0, concat_axis=0, tiled=True)


def held_at(t):
    return jnp.where(spot("c") == 1, (t % 4) * 4 + t // 4, t)


def on_device(
    cotangent, moe_input, expert_ids, group_weight, expert_weight, mixer_out,
    queries, key_vectors, value_vectors, decay_rates, proj_weight,
    gate_weight, up_weight, down_weight,
):
    ids = expert_ids.T
    held = call(
        load_kernel,
        arr((HELD, COL), BF),
        (
            ids, group_weight.reshape(1, TOK), expert_weight.T, cotangent, moe_input,
            decay_rates, key_vectors, value_vectors,
        ),
        "load",
        60,
        stay=8,
        scratch=[
            pltpu.VMEM((2, TOK), jnp.int32), pltpu.VMEM((1, TOK), F32), pltpu.VMEM((2, TOK), F32),
            pltpu.VMEM((1, TOK), F32), pltpu.SemaphoreType.DMA((8,)),
        ],
    )
    held = lax.all_gather(held, "c")
    rows, picks, small, mine = call(
        pack_kernel,
        [
            arr((NZ, 4 * CAP, COL), BF), arr((768, TOK), BF), arr((72, COL), BF),
            arr((8, TOK), F32),
        ],
        (held,),
        "pack",
    )
    rows = exchange(rows, "z")
    copies = call(spread_kernel, arr((4, 2, NZ * 2 * CAP, COL), BF), (rows,), "spread")
    rows = within(copies, ("c", "tp"), groups(1, 4, 4, 1))
    rows = to_all(rows.reshape(4, 2, NZ * 2 * CAP, COL), ("c", "tp"), groups(4, 1, 1, 4))
    rows = rows.reshape(NT, 2, NZ * 2 * CAP, COL)
    shares, hidden, both = call(
        expert_kernel,
        [arr((NT, 384, COL), BF), arr((384, 128), BF), arr((384, 256), BF)],
        (rows, gate_weight[0], up_weight[0], down_weight[0]),
        "expert",
        20,
    )
    shares = exchange(shares, "tp")
    back = call(sum_kernel, arr((NZ, 64, COL), BF), (shares, small), "sums", 6)
    own = exchange(back, "z")
    own, rows, hidden, both = lax.optimization_barrier((own, rows, hidden, both))
    other = lax.ppermute(own, "c", SWAP)
    grad_gate, grad_up, grad_down = call(
        weight_kernel,
        [arr((2048, 128), BF), arr((2048, 128), BF), arr((128, 2048), BF)],
        (rows, hidden, both),
        "weights",
        16,
        1 << 29,
    )
    resid = call(resid_kernel, arr((NT, TOK, COL), BF), (picks, own, other, held), "resid")
    resid, grad_gate, grad_up, grad_down = lax.optimization_barrier(
        (resid, grad_gate, grad_up, grad_down)
    )
    resid = exchange(resid, "tp")
    out_grad, proj_keep, proj_send, state = call(
        proj_kernel,
        [
            arr((TOK, VD), F32), arr((NZ, 64, COL), F32), arr((18, 64, COL), BF),
            arr((2, KD, VD), F32),
        ],
        (resid, proj_weight, mixer_out, queries, mine),
        "proj",
        8,
    )
    got = lax.ppermute(proj_send, "c", SWAP)
    grad_queries, part, weight = call(
        intra_kernel,
        [arr((KD, TOK), F32), arr((392, TOK), F32), arr((32, TOK), F32)],
        (out_grad, queries, held, mine, own, other),
        "intra",
    )
    chip, near = call(
        chip_kernel,
        [arr((NZ, 96, COL), BF), arr((KD, VD), F32)],
        (proj_keep, got, state, mine),
        "chip",
    )
    chip, grad_queries, part, weight = lax.optimization_barrier((chip, grad_queries, part, weight))
    chip = exchange(chip, "z")
    far = call(gather_kernel, arr((2, 32, COL), F32), (chip, weight), "gather")
    far = lax.all_gather(far, "c")
    grad_proj, grad_keys, grad_values = call(
        final_kernel,
        [arr((64, COL), F32), arr((KD, TOK), F32), arr((VD, TOK), F32)],
        (far, near, part, chip),
        "final",
    )
    return (
        grad_gate[None], grad_up[None], grad_down[None],
        grad_proj, grad_queries, grad_keys, grad_values,
    )


def solution(mesh):
    finer = Mesh(mesh.devices.reshape(NZ, 2, NT), ("z", "c", "tp"))
    in_specs = (
        P(SP, None), P(SP, None), P(SP, None), P(SP), P(SP, None), P(SP, "tp"),
        P("tp", SP), P("tp", SP), P("tp", SP), P("tp", SP), P(None, "tp"),
        P(SP, None, "tp"), P(SP, None, "tp"), P(SP, "tp", None),
    )
    out_specs = (
        P(SP, None, "tp"), P(SP, None, "tp"), P(SP, "tp", None), P(SP, "tp"),
        P("tp", SP), P("tp", SP), P("tp", SP),
    )
    return jax.shard_map(
        on_device, mesh=finer, in_specs=in_specs, out_specs=out_specs, check_vma=False
    )
```

```python
import jax
import jax.numpy as jnp
from jax import lax
from jax.experimental import pallas as pl
from jax.experimental.pallas import tpu as pltpu
from jax.sharding import Mesh
from jax.sharding import PartitionSpec as P

BF = jnp.bfloat16
F32 = jnp.float32
NZ = 16
NT = 16
CAP = 12
TOK = 128
COL = 128
KD = 64
VD = 128
SP = ("z", "c")
SWAP = [(0, 1), (1, 0)]

NN = (((1,), (0,)), ((), ()))
NTR = (((1,), (1,)), ((), ()))
TN = (((0,), (0,)), ((), ()))


def mm(a, b, dims=NN):
    return lax.dot_general(a, b, dims, preferred_element_type=F32)


def halves(a):
    high = a.astype(BF)
    return high, (a - high.astype(F32)).astype(BF)


def exact(a, b, dims=NN):
    if a.dtype == BF:
        high, low = halves(b)
        return mm(a, high, dims) + mm(a, low, dims)
    high, low = halves(a)
    if b.dtype == BF:
        return mm(high, b, dims) + mm(low, b, dims)
    other, rest = halves(b)
    return mm(high, other, dims) + (mm(high, rest, dims) + mm(low, other, dims))


def vmem():
    return pl.BlockSpec(memory_space=pltpu.VMEM)


def hbm():
    return pl.BlockSpec(memory_space=pltpu.HBM)


def call(kernel, outs, args, name, mib=4, flops=1 << 27, stay=0, scratch=(), out=None):
    return pl.pallas_call(
        kernel,
        out_shape=outs,
        in_specs=[hbm()] * stay + [vmem()] * (len(args) - stay),
        out_specs=jax.tree.map(lambda _: (out or vmem)(), outs),
        scratch_shapes=scratch,
        name=name,
        compiler_params=pltpu.CompilerParams(vmem_limit_bytes=mib << 20),
        cost_estimate=pl.CostEstimate(flops=flops, bytes_accessed=1 << 20, transcendentals=0),
    )(*args)


def spot(axis):
    return lax.axis_index(axis).astype(jnp.int32)


def fetch(sources, targets, sems):
    copies = [
        pltpu.make_async_copy(src, dst, sems.at[n])
        for n, (src, dst) in enumerate(zip(sources, targets))
    ]
    for copy in copies:
        copy.start()
    for copy in copies:
        copy.wait()


def arr(shape, dtype):
    return jax.ShapeDtypeStruct(shape, dtype)


def placement(ids, wanted, rank):
    first = ids[0:1, :] == wanted
    match = first | (ids[1:2, :] == wanted)
    tok = TOK
    before = lax.broadcasted_iota(jnp.int32, (tok, tok), 0) < lax.broadcasted_iota(
        jnp.int32, (tok, tok), 1
    )
    ranks = mm(jnp.where(match, 1.0, 0.0).astype(BF), jnp.where(before, 1.0, 0.0).astype(BF))
    return match & (ranks == rank.astype(F32)), first


def decay_parts(rates):
    upto = lax.broadcasted_iota(jnp.int32, (TOK, TOK), 1) <= lax.broadcasted_iota(
        jnp.int32, (TOK, TOK), 0
    )
    col = jnp.broadcast_to(
        jnp.sum(jnp.where(upto, rates, 0.0), axis=1, keepdims=True), (TOK, TOK)
    )
    row = col.T
    total = jnp.sum(rates, axis=1, keepdims=True)
    prefix = row[0:1, :]
    start = jnp.exp(-prefix)
    end = jnp.exp(jnp.minimum(prefix - total, 0.0))
    return col, row, start, end, jnp.broadcast_to(total, (1, TOK))


def in_pieces(row):
    hi = row.astype(BF).astype(F32)
    mid = (row - hi).astype(BF).astype(F32)
    return jnp.concatenate([hi, mid, row - hi - mid], axis=0)


def in_one(pieces):
    pieces = pieces.astype(F32)
    return pieces[0:1, :] + pieces[1:2, :] + pieces[2:3, :]


def ids_of(rows):
    return rows[IDS - ROUTE : IDS - ROUTE + 2, :].astype(jnp.int32)


def rates_of(g_ref, block):
    return in_one(g_ref[block, ROUTE:HELD, :].astype(F32)[RATE - ROUTE : IDS - ROUTE])


COT, INP, KEY, VALUE, ROUTE, RATE, IDS, HELD = 0, 128, 256, 320, 448, 456, 459, 464


def load_kernel(
    ids_in, gw_in, ew_in, cot_in, inp_in, rate_in, k_in, v_in,
    out_ref, ids_ref, gw_ref, ew_ref, rate_ref, sems,
):
    here = pl.ds(pl.multiple_of(spot("tp") * COL, COL), COL)
    fetch(
        (ids_in, gw_in, ew_in, cot_in.at[:, here], inp_in.at[:, here], rate_in, k_in, v_in),
        (
            ids_ref, gw_ref, ew_ref, out_ref.at[pl.ds(COT, TOK)], out_ref.at[pl.ds(INP, TOK)],
            rate_ref, out_ref.at[pl.ds(KEY, KD)], out_ref.at[pl.ds(VALUE, VD)],
        ),
        sems,
    )
    weights = gw_ref[...] * ew_ref[...]
    none = jnp.zeros((2, TOK), F32)
    out_ref[ROUTE:HELD, :] = jnp.concatenate(
        [in_pieces(weights[0:1, :]), in_pieces(weights[1:2, :]), none]
        + [in_pieces(rate_ref[...]), ids_ref[...].astype(F32), none, none[0:1, :]],
        axis=0,
    ).astype(BF)


def pack_kernel(g_ref, rows_ref, picks_ref, small_ref, mine_ref):
    core = spot("c")
    number = lax.broadcasted_iota(jnp.int32, (NZ * 2 * CAP, TOK), 0)
    z = lax.shift_right_logical(number * 2731, 16)
    q = number - 2 * CAP * z
    first_half = q < CAP
    inp_rows = cot_rows = 0.0
    for block, wanted, rank in (
        (core, jnp.where(first_half, 2 * z + core, -1), q),
        (1 - core, jnp.where(first_half, -1, 2 * z + core), q - CAP),
    ):
        rows = g_ref[block, ROUTE:HELD, :].astype(F32)
        hit, first = placement(ids_of(rows), wanted, rank)
        scale = jnp.sum(
            jnp.where(hit, jnp.where(first, in_one(rows[0:3]), in_one(rows[3:6])), 0.0),
            axis=1,
            keepdims=True,
        )
        take = jnp.where(hit, 1.0, 0.0).astype(BF)
        if block is core:
            picks_ref[0:384, :] = take
        inp_rows = inp_rows + mm(take, g_ref[block, INP : INP + TOK, :])
        cot_rows = cot_rows + mm(take, g_ref[block, COT : COT + TOK, :]) * scale
    for z in range(NZ):
        part = slice(2 * CAP * z, 2 * CAP * (z + 1))
        rows_ref[z, 0 : 2 * CAP, :] = inp_rows[part].astype(BF)
        rows_ref[z, 2 * CAP : 4 * CAP, :] = cot_rows[part].astype(BF)
    z = lax.shift_right_logical(number * 2731, 16)
    hit, _ = placement(
        ids_of(g_ref[core, ROUTE:HELD, :].astype(F32)),
        jnp.where(first_half, -1, 2 * z + 1 - core),
        q - CAP,
    )
    picks_ref[384:768, :] = jnp.where(hit, 1.0, 0.0).astype(BF)

    _, _, start_a, end_a, total_a = decay_parts(rates_of(g_ref, 0))
    _, _, start_b, end_b, total_b = decay_parts(rates_of(g_ref, 1))
    half = pl.ds(pl.multiple_of(KEY + 32 * core, 32), 32)
    keys = jnp.concatenate([g_ref[0, half, :], g_ref[1, half, :]], axis=1).astype(F32)
    values = jnp.concatenate([g_ref[k, VALUE : VALUE + VD, :] for k in (0, 1)], axis=1)
    early = jnp.concatenate([end_a * jnp.exp(-total_b), end_b], axis=1)
    late = jnp.concatenate([start_a, start_b * jnp.exp(-total_a)], axis=1)
    small_ref[0:32, :] = exact(keys * early, values, NTR).astype(BF)
    small_ref[32:64, :] = exact(keys * late, values, NTR).astype(BF)
    small_ref[64:72, :] = jnp.concatenate(
        [in_pieces(total_a + total_b), jnp.zeros((5, TOK), F32)], axis=0
    ).astype(BF)
    is_first = core == 0
    mine_ref[...] = jnp.concatenate(
        [
            jnp.where(is_first, start_a, start_b), jnp.where(is_first, end_a, end_b),
            jnp.where(is_first, total_a, total_b), jnp.where(is_first, total_b, total_a),
            jnp.zeros((4, TOK), F32),
        ],
        axis=0,
    )


def copies_kernel(got_ref, out_ref):
    for j in range(4):
        for kind in range(2):
            part = got_ref[j, kind]
            for k in range(4):
                out_ref[k, j, kind] = part


def spread_kernel(got_ref, rows_ref):
    for z in range(NZ):
        for kind in range(2):
            part = got_ref[z, 24 * kind : 24 * (kind + 1), :]
            for k in range(4):
                rows_ref[k, kind, 24 * z : 24 * (z + 1), :] = part


def expert_kernel(x_ref, gw_ref, uw_ref, dw_ref, part_ref, hid_ref, both_ref):
    inp = jnp.concatenate([x_ref[held_at(t), 0] for t in range(NT)], axis=1)
    cot = jnp.concatenate([x_ref[held_at(t), 1] for t in range(NT)], axis=1)
    both_w = jnp.concatenate([gw_ref[...], uw_ref[...]], axis=1)
    pre = mm(inp, both_w)
    gate, up = pre[:, :128], pre[:, 128:]
    hidden_grad = mm(cot, dw_ref[...], NTR)
    sig = jax.nn.sigmoid(gate)
    act = gate * sig
    hid_ref[...] = (act * up).astype(BF)
    gate_grad = (hidden_grad * up * sig * (1.0 + gate * (1.0 - sig))).astype(BF)
    up_grad = (hidden_grad * act).astype(BF)
    both = jnp.concatenate([gate_grad, up_grad], axis=1)
    both_ref[...] = both
    for t in range(0, NT, 2):
        out = mm(both, both_w[t * COL : (t + 2) * COL], NTR).astype(BF)
        part_ref[t] = out[:, :COL]
        part_ref[t + 1] = out[:, COL:]


def weight_kernel(
    x_ref, hid_ref, both_ref, gg_out, gu_out, gd_out, gg_ref, gu_ref, gd_ref, sems
):
    both = both_ref[...].T
    hidden = hid_ref[...].T
    copies = []
    for t in range(0, NT, 2):
        rows = slice(t * COL, (t + 2) * COL)
        inp = jnp.concatenate([x_ref[held_at(t), 0], x_ref[held_at(t + 1), 0]], axis=1)
        cot = jnp.concatenate([x_ref[held_at(t), 1], x_ref[held_at(t + 1), 1]], axis=1)
        out = mm(both, inp).astype(BF).T
        gg_ref[rows, :] = out[:, :128]
        gu_ref[rows, :] = out[:, 128:]
        gd_ref[:, rows] = mm(hidden, cot).astype(BF)
        if t % 4 == 2:
            done = pl.ds((t - 2) * COL, 4 * COL)
            for n, (src, dst) in enumerate(
                (
                    (gg_ref.at[done], gg_out.at[done]), (gu_ref.at[done], gu_out.at[done]),
                    (gd_ref.at[:, done], gd_out.at[:, done]),
                )
            ):
                copies.append(pltpu.make_async_copy(src, dst, sems.at[t // 4, n]))
                copies[-1].start()
    for copy in copies:
        copy.wait()


def chip_states(early, late, early_other, late_other, mine, theirs):
    is_first = spot("c") == 0
    both_early = early * jnp.where(is_first, theirs, 1.0) + early_other * jnp.where(
        is_first, 1.0, mine
    )
    both_late = late * jnp.where(is_first, 1.0, theirs) + late_other * jnp.where(
        is_first, mine, 1.0
    )
    return [jnp.where(is_first, a[:32], a[32:]).astype(BF) for a in (both_early, both_late)]


def sum_kernel(part_ref, small_ref, out_ref):
    total = part_ref[0].astype(F32)
    for t in range(1, NT):
        total = total + part_ref[t].astype(F32)
    out_ref[:, 0 : 2 * CAP, :] = total.reshape(NZ, 2 * CAP, COL).astype(BF)
    early, late, pieces = small_ref[0:32, :], small_ref[32:64, :], small_ref[64:72, :]
    place = spot("z")
    for z in range(NZ):
        out_ref[z, 24:56, :] = jnp.where(z > place, early, late)
        out_ref[z, 56:64, :] = pieces


def resid_kernel(picks_ref, own_ref, other_ref, g_ref, out_ref):
    own, other = [
        r[:, 0 : 2 * CAP, :].astype(F32).reshape(384, COL).astype(BF) for r in (own_ref, other_ref)
    ]
    moe = mm(picks_ref[0:384, :], own, TN) + mm(picks_ref[384:768, :], other, TN)
    cot = g_ref[spot("c"), COT : COT + TOK, :]
    resid = (cot.astype(F32) + moe).astype(BF)
    for t in range(NT):
        out_ref[t] = resid


def proj_kernel(r_ref, p_ref, mixer_ref, q_ref, mine_ref, og_ref, keep_ref, send_ref, state_ref):
    core = spot("c")
    resid = jnp.concatenate([r_ref[t] for t in range(NT)], axis=1)
    out_grad = mm(resid, p_ref[...])
    og_ref[...] = out_grad
    query = q_ref[...].astype(F32)
    early = exact(query * mine_ref[1:2, :], out_grad)
    late = exact(query * mine_ref[0:1, :], out_grad)
    state_ref[0] = early
    state_ref[1] = late
    send_ref[16] = early.astype(BF)
    send_ref[17] = late.astype(BF)
    mixer = mixer_ref[...]
    for t in range(NT):
        share = mm(r_ref[t], mixer, TN)
        low, high = share[:64], share[64:]
        keep_ref[t] = jnp.where(core == 0, low, high)
        send_ref[t] = jnp.where(core == 0, high, low).astype(BF)


def at_block(far_early, far_late, near, theirs):
    is_first = spot("c") == 0
    early = far_early * jnp.where(is_first, 1.0, theirs) + jnp.where(is_first, 0.0, near)
    late = far_late * jnp.where(is_first, theirs, 1.0) + jnp.where(is_first, near, 0.0)
    return early, late


def intra_kernel(
    og_ref, q_ref, g_ref, mine_ref, own_ref, other_ref, gq_ref, part_ref, weight_ref
):
    place, core = spot("z"), spot("c")
    rows = own_ref[:, 56:64, :].astype(F32)
    chip = rows[:, 0, :] + rows[:, 1, :] + rows[:, 2, :]
    number = lax.broadcasted_iota(jnp.int32, (NZ, COL), 0)
    between = jnp.zeros((NZ, COL), F32)
    for u in range(NZ):
        inside = ((number < u) & (u < place)) | ((number > u) & (u > place))
        between = between + jnp.where(inside, chip[u : u + 1, :], 0.0)
    weight = jnp.exp(-between)
    early_w = jnp.where(number < place, weight, 0.0)
    late_w = jnp.where(number > place, weight, 0.0)
    weight_ref[0:16, :] = early_w
    weight_ref[16:32, :] = late_w

    def far(ref):
        early = late = jnp.zeros((32, COL), F32)
        for z in range(NZ):
            state = ref[z, 24:56, :].astype(F32)
            early = early + state * early_w[z : z + 1, :]
            late = late + state * late_w[z : z + 1, :]
        return early, late

    is_first = core == 0
    here, there = far(own_ref), far(other_ref)
    far_early, far_late = [
        jnp.concatenate([jnp.where(is_first, a, b), jnp.where(is_first, b, a)], axis=0)
        for a, b in zip(here, there)
    ]
    _, _, start, end, _ = decay_parts(rates_of(g_ref, 1 - core))
    there = g_ref[1 - core, KEY : KEY + KD, :].astype(F32) * jnp.where(is_first, start, end)
    near = exact(there, g_ref[1 - core, VALUE : VALUE + VD, :], NTR)
    theirs = jnp.exp(-mine_ref[3:4, :])
    kv_early, kv_late = at_block(far_early, far_late, near, theirs)
    scale = KD ** (-0.5)
    col, row, start, end, _ = decay_parts(rates_of(g_ref, core))
    low, high = scale * start, scale * end
    mixed = scale * jnp.exp(-jnp.abs(col - row))
    out_grad = og_ref[...]
    query, key = q_ref[...], g_ref[core, KEY : KEY + KD, :]
    value = g_ref[core, VALUE : VALUE + VD, :]
    score_grad = exact(out_grad, value) * mixed
    gq_ref[...] = (
        exact(key, score_grad, NTR)
        + low * exact(kv_early, out_grad, NTR)
        + high * exact(kv_late, out_grad, NTR)
    )
    part_ref[0:64, :] = exact(query, score_grad)
    part_ref[64:192, :] = exact(out_grad, mm(query, key, TN) * mixed, TN)
    part_ref[192:256, :] = key.astype(F32)
    part_ref[256:384, :] = value.astype(F32)
    part_ref[384:392, :] = jnp.concatenate([low, high, theirs, jnp.zeros((5, TOK), F32)], axis=0)


def chip_kernel(keep_ref, got_ref, state_ref, mine_ref, out_ref, near_ref):
    place, core = spot("z"), spot("c")
    mine, theirs = jnp.exp(-mine_ref[2:3, :]), jnp.exp(-mine_ref[3:4, :])
    early_other, late_other = got_ref[16].astype(F32), got_ref[17].astype(F32)
    early, late = chip_states(state_ref[0], state_ref[1], early_other, late_other, mine, theirs)
    near_ref[...] = jnp.where(core == 0, late_other, early_other)
    for z in range(NZ):
        out_ref[z, 0:64, :] = (keep_ref[z] + got_ref[z].astype(F32)).astype(BF)
        out_ref[z, 64:96, :] = jnp.where(z > place, early, late)


def gather_kernel(got_ref, weight_ref, state_ref):
    early = late = jnp.zeros((32, COL), F32)
    for z in range(NZ):
        state = got_ref[z, 64:96, :].astype(F32)
        early = early + state * weight_ref[z : z + 1, :]
        late = late + state * weight_ref[16 + z : 17 + z, :]
    state_ref[0] = early
    state_ref[1] = late


def final_kernel(far_ref, near_ref, part_ref, got_ref, proj_ref, gk_ref, gv_ref):
    share = jnp.zeros((64, COL), F32)
    for z in range(NZ):
        share = share + got_ref[z, 0:64, :].astype(F32)
    proj_ref[...] = share
    early, late = at_block(
        jnp.concatenate([far_ref[0, 0], far_ref[1, 0]], axis=0),
        jnp.concatenate([far_ref[0, 1], far_ref[1, 1]], axis=0),
        near_ref[...],
        part_ref[386:387, :],
    )
    low, high = part_ref[384:385, :], part_ref[385:386, :]
    key, value = part_ref[192:256, :].astype(BF), part_ref[256:384, :].astype(BF)
    gk_ref[...] = part_ref[0:64, :] + low * exact(early, value) + high * exact(late, value)
    gv_ref[...] = part_ref[64:192, :] + low * exact(early, key, TN) + high * exact(late, key, TN)


def groups(step, stride, step_other, stride_other):
    first = [[stride * g + step * k for k in range(4)] for g in range(4)]
    second = [[16 + stride_other * g + step_other * k for k in range(4)] for g in range(4)]
    return first + second


def within(blocks, axis, sets):
    return lax.all_to_all(
        blocks, axis, split_axis=0, concat_axis=0, axis_index_groups=sets, tiled=True
    )


def exchange(blocks, axis):
    return lax.all_to_all(blocks, axis, split_axis=0, concat_axis=0, tiled=True)


def held_at(t):
    return jnp.where(spot("c") == 0, (t % 4) * 4 + t // 4, t)


def on_device(
    cotangent, moe_input, expert_ids, group_weight, expert_weight, mixer_out,
    queries, key_vectors, value_vectors, decay_rates, proj_weight,
    gate_weight, up_weight, down_weight,
):
    ids = expert_ids.T
    held = call(
        load_kernel,
        arr((HELD, COL), BF),
        (
            ids, group_weight.reshape(1, TOK), expert_weight.T, cotangent, moe_input,
            decay_rates, key_vectors, value_vectors,
        ),
        "load",
        60,
        stay=8,
        scratch=[
            pltpu.VMEM((2, TOK), jnp.int32), pltpu.VMEM((1, TOK), F32), pltpu.VMEM((2, TOK), F32),
            pltpu.VMEM((1, TOK), F32), pltpu.SemaphoreType.DMA((8,)),
        ],
    )
    held = lax.all_gather(held, "c")
    rows, picks, small, mine = call(
        pack_kernel,
        [
            arr((NZ, 4 * CAP, COL), BF), arr((768, TOK), BF), arr((72, COL), BF),
            arr((8, TOK), F32),
        ],
        (held,),
        "pack",
    )
    rows = exchange(rows, "z")
    copies = call(spread_kernel, arr((4, 2, NZ * 2 * CAP, COL), BF), (rows,), "spread")
    rows = within(copies, ("c", "tp"), groups(4, 1, 1, 4))
    rows = rows.reshape(4, 2, NZ * 2 * CAP, COL)
    copies = call(copies_kernel, arr((4, *rows.shape), BF), (rows,), "copies", 12)
    rows = within(copies, ("c", "tp"), groups(1, 4, 4, 1))
    rows = rows.reshape(NT, 2, NZ * 2 * CAP, COL)
    shares, hidden, both = call(
        expert_kernel,
        [arr((NT, 384, COL), BF), arr((384, 128), BF), arr((384, 256), BF)],
        (rows, gate_weight[0], up_weight[0], down_weight[0]),
        "expert",
        20,
    )
    shares = exchange(shares, "tp")
    back = call(sum_kernel, arr((NZ, 64, COL), BF), (shares, small), "sums", 6)
    own = exchange(back, "z")
    own, rows, hidden, both = lax.optimization_barrier((own, rows, hidden, both))
    other = lax.ppermute(own, "c", SWAP)
    shapes = [arr((2048, 128), BF), arr((2048, 128), BF), arr((128, 2048), BF)]
    grad_gate, grad_up, grad_down = call(
        weight_kernel,
        shapes,
        (rows, hidden, both),
        "weights",
        16,
        1 << 29,
        scratch=[pltpu.VMEM(a.shape, BF) for a in shapes] + [pltpu.SemaphoreType.DMA((4, 3))],
        out=hbm,
    )
    resid = call(resid_kernel, arr((NT, TOK, COL), BF), (picks, own, other, held), "resid")
    resid, grad_gate, grad_up, grad_down = lax.optimization_barrier(
        (resid, grad_gate, grad_up, grad_down)
    )
    resid = exchange(resid, "tp")
    out_grad, proj_keep, proj_send, state = call(
        proj_kernel,
        [
            arr((TOK, VD), F32), arr((NZ, 64, COL), F32), arr((18, 64, COL), BF),
            arr((2, KD, VD), F32),
        ],
        (resid, proj_weight, mixer_out, queries, mine),
        "proj",
        8,
    )
    got = lax.ppermute(proj_send, "c", SWAP)
    grad_queries, part, weight = call(
        intra_kernel,
        [arr((KD, TOK), F32), arr((392, TOK), F32), arr((32, TOK), F32)],
        (out_grad, queries, held, mine, own, other),
        "intra",
    )
    chip, near = call(
        chip_kernel,
        [arr((NZ, 96, COL), BF), arr((KD, VD), F32)],
        (proj_keep, got, state, mine),
        "chip",
    )
    chip, grad_queries, part, weight = lax.optimization_barrier((chip, grad_queries, part, weight))
    chip = exchange(chip, "z")
    far = call(gather_kernel, arr((2, 32, COL), F32), (chip, weight), "gather")
    far = lax.all_gather(far, "c")
    grad_proj, grad_keys, grad_values = call(
        final_kernel,
        [arr((64, COL), F32), arr((KD, TOK), F32), arr((VD, TOK), F32)],
        (far, near, part, chip),
        "final",
    )
    return (
        grad_gate[None], grad_up[None], grad_down[None],
        grad_proj, grad_queries, grad_keys, grad_values,
    )


def solution(mesh):
    finer = Mesh(mesh.devices.reshape(NZ, 2, NT), ("z", "c", "tp"))
    in_specs = (
        P(SP, None), P(SP, None), P(SP, None), P(SP), P(SP, None), P(SP, "tp"),
        P("tp", SP), P("tp", SP), P("tp", SP), P("tp", SP), P(None, "tp"),
        P(SP, None, "tp"), P(SP, None, "tp"), P(SP, "tp", None),
    )
    out_specs = (
        P(SP, None, "tp"), P(SP, None, "tp"), P(SP, "tp", None), P(SP, "tp"),
        P("tp", SP), P("tp", SP), P("tp", SP),
    )
    return jax.shard_map(
        on_device, mesh=finer, in_specs=in_specs, out_specs=out_specs, check_vma=False
    )
```

```python
import jax
import jax.numpy as jnp
from jax import lax
from jax.experimental import pallas as pl
from jax.experimental.pallas import tpu as pltpu
from jax.sharding import Mesh
from jax.sharding import PartitionSpec as P

BF = jnp.bfloat16
F32 = jnp.float32
NZ = 16
NT = 16
CAP = 12
TOK = 128
COL = 128
KD = 64
VD = 128
SP = ("z", "c")
SWAP = [(0, 1), (1, 0)]

NN = (((1,), (0,)), ((), ()))
NTR = (((1,), (1,)), ((), ()))
TN = (((0,), (0,)), ((), ()))


def mm(a, b, dims=NN):
    return lax.dot_general(a, b, dims, preferred_element_type=F32)


def halves(a):
    high = a.astype(BF)
    return high, (a - high.astype(F32)).astype(BF)


def exact(a, b, dims=NN):
    if a.dtype == BF:
        high, low = halves(b)
        return mm(a, high, dims) + mm(a, low, dims)
    high, low = halves(a)
    if b.dtype == BF:
        return mm(high, b, dims) + mm(low, b, dims)
    other, rest = halves(b)
    return mm(high, other, dims) + (mm(high, rest, dims) + mm(low, other, dims))


def vmem():
    return pl.BlockSpec(memory_space=pltpu.VMEM)


def hbm():
    return pl.BlockSpec(memory_space=pltpu.HBM)


def call(kernel, outs, args, name, mib=4, flops=1 << 27, stay=0, scratch=(), out=None):
    return pl.pallas_call(
        kernel,
        out_shape=outs,
        in_specs=[hbm()] * stay + [vmem()] * (len(args) - stay),
        out_specs=jax.tree.map(lambda _: (out or vmem)(), outs),
        scratch_shapes=scratch,
        name=name,
        compiler_params=pltpu.CompilerParams(vmem_limit_bytes=mib << 20),
        cost_estimate=pl.CostEstimate(flops=flops, bytes_accessed=1 << 20, transcendentals=0),
    )(*args)


def spot(axis):
    return lax.axis_index(axis).astype(jnp.int32)


def fetch(sources, targets, sems):
    copies = [
        pltpu.make_async_copy(src, dst, sems.at[n])
        for n, (src, dst) in enumerate(zip(sources, targets))
    ]
    for copy in copies:
        copy.start()
    for copy in copies:
        copy.wait()


def arr(shape, dtype):
    return jax.ShapeDtypeStruct(shape, dtype)


def placement(ids, wanted, rank):
    first = ids[0:1, :] == wanted
    match = first | (ids[1:2, :] == wanted)
    tok = TOK
    before = lax.broadcasted_iota(jnp.int32, (tok, tok), 0) < lax.broadcasted_iota(
        jnp.int32, (tok, tok), 1
    )
    ranks = mm(jnp.where(match, 1.0, 0.0).astype(BF), jnp.where(before, 1.0, 0.0).astype(BF))
    return match & (ranks == rank.astype(F32)), first


def decay_parts(rates):
    upto = lax.broadcasted_iota(jnp.int32, (TOK, TOK), 1) <= lax.broadcasted_iota(
        jnp.int32, (TOK, TOK), 0
    )
    col = jnp.broadcast_to(
        jnp.sum(jnp.where(upto, rates, 0.0), axis=1, keepdims=True), (TOK, TOK)
    )
    row = col.T
    total = jnp.sum(rates, axis=1, keepdims=True)
    prefix = row[0:1, :]
    start = jnp.exp(-prefix)
    end = jnp.exp(jnp.minimum(prefix - total, 0.0))
    return col, row, start, end, jnp.broadcast_to(total, (1, TOK))


def in_pieces(row):
    hi = row.astype(BF).astype(F32)
    mid = (row - hi).astype(BF).astype(F32)
    return jnp.concatenate([hi, mid, row - hi - mid], axis=0)


def in_one(pieces):
    pieces = pieces.astype(F32)
    return pieces[0:1, :] + pieces[1:2, :] + pieces[2:3, :]


def ids_of(rows):
    return rows[IDS - ROUTE : IDS - ROUTE + 2, :].astype(jnp.int32)


def rates_of(g_ref, block):
    return in_one(g_ref[block, ROUTE:HELD, :].astype(F32)[RATE - ROUTE : IDS - ROUTE])


COT, INP, KEY, VALUE, ROUTE, RATE, IDS, HELD = 0, 128, 256, 320, 448, 456, 459, 464


def load_kernel(
    ids_in, gw_in, ew_in, cot_in, inp_in, rate_in, k_in, v_in,
    out, held_ref, ids_ref, gw_ref, ew_ref, rate_ref, sems, out_sems,
):
    here = pl.ds(pl.multiple_of(spot("tp") * COL, COL), COL)
    bulk = [pl.ds(COT, TOK), pl.ds(INP, TOK), pl.ds(KEY, KD), pl.ds(VALUE, VD)]
    sources = (cot_in.at[:, here], inp_in.at[:, here], k_in, v_in, ids_in, gw_in, ew_in, rate_in)
    targets = [held_ref.at[part] for part in bulk] + [ids_ref, gw_ref, ew_ref, rate_ref]
    copies = [
        pltpu.make_async_copy(src, dst, sems.at[n])
        for n, (src, dst) in enumerate(zip(sources, targets))
    ]
    small = pl.ds(ROUTE, HELD - ROUTE)
    leaving = [
        pltpu.make_async_copy(held_ref.at[part], out.at[part], out_sems.at[n])
        for n, part in enumerate(bulk + [small])
    ]
    for copy in copies:
        copy.start()
    for copy, leave in zip(copies[:4], leaving):
        copy.wait()
        leave.start()
    for copy in copies[4:]:
        copy.wait()
    weights = gw_ref[...] * ew_ref[...]
    none = jnp.zeros((2, TOK), F32)
    held_ref[ROUTE:HELD, :] = jnp.concatenate(
        [in_pieces(weights[0:1, :]), in_pieces(weights[1:2, :]), none]
        + [in_pieces(rate_ref[...]), ids_ref[...].astype(F32), none, none[0:1, :]],
        axis=0,
    ).astype(BF)
    leaving[4].start()
    for leave in leaving:
        leave.wait()


def pack_kernel(g_ref, rows_ref, picks_ref, small_ref, mine_ref):
    core = spot("c")
    number = lax.broadcasted_iota(jnp.int32, (NZ * 2 * CAP, TOK), 0)
    z = lax.shift_right_logical(number * 2731, 16)
    q = number - 2 * CAP * z
    first_half = q < CAP
    inp_rows = cot_rows = 0.0
    for block, wanted, rank in (
        (core, jnp.where(first_half, 2 * z + core, -1), q),
        (1 - core, jnp.where(first_half, -1, 2 * z + core), q - CAP),
    ):
        rows = g_ref[block, ROUTE:HELD, :].astype(F32)
        hit, first = placement(ids_of(rows), wanted, rank)
        scale = jnp.sum(
            jnp.where(hit, jnp.where(first, in_one(rows[0:3]), in_one(rows[3:6])), 0.0),
            axis=1,
            keepdims=True,
        )
        take = jnp.where(hit, 1.0, 0.0).astype(BF)
        if block is core:
            picks_ref[0:384, :] = take
        inp_rows = inp_rows + mm(take, g_ref[block, INP : INP + TOK, :])
        cot_rows = cot_rows + mm(take, g_ref[block, COT : COT + TOK, :]) * scale
    for z in range(NZ):
        part = slice(2 * CAP * z, 2 * CAP * (z + 1))
        rows_ref[z, 0 : 2 * CAP, :] = inp_rows[part].astype(BF)
        rows_ref[z, 2 * CAP : 4 * CAP, :] = cot_rows[part].astype(BF)
    z = lax.shift_right_logical(number * 2731, 16)
    hit, _ = placement(
        ids_of(g_ref[core, ROUTE:HELD, :].astype(F32)),
        jnp.where(first_half, -1, 2 * z + 1 - core),
        q - CAP,
    )
    picks_ref[384:768, :] = jnp.where(hit, 1.0, 0.0).astype(BF)

    _, _, start_a, end_a, total_a = decay_parts(rates_of(g_ref, 0))
    _, _, start_b, end_b, total_b = decay_parts(rates_of(g_ref, 1))
    half = pl.ds(pl.multiple_of(KEY + 32 * core, 32), 32)
    keys = jnp.concatenate([g_ref[0, half, :], g_ref[1, half, :]], axis=1).astype(F32)
    values = jnp.concatenate([g_ref[k, VALUE : VALUE + VD, :] for k in (0, 1)], axis=1)
    early = jnp.concatenate([end_a * jnp.exp(-total_b), end_b], axis=1)
    late = jnp.concatenate([start_a, start_b * jnp.exp(-total_a)], axis=1)
    small_ref[0:32, :] = exact(keys * early, values, NTR).astype(BF)
    small_ref[32:64, :] = exact(keys * late, values, NTR).astype(BF)
    small_ref[64:72, :] = jnp.concatenate(
        [in_pieces(total_a + total_b), jnp.zeros((5, TOK), F32)], axis=0
    ).astype(BF)
    is_first = core == 0
    mine_ref[...] = jnp.concatenate(
        [
            jnp.where(is_first, start_a, start_b), jnp.where(is_first, end_a, end_b),
            jnp.where(is_first, total_a, total_b), jnp.where(is_first, total_b, total_a),
            jnp.zeros((4, TOK), F32),
        ],
        axis=0,
    )


def copies_kernel(got_ref, out_ref):
    for j in range(4):
        for kind in range(2):
            part = got_ref[j, kind]
            for k in range(4):
                out_ref[k, j, kind] = part


def spread_kernel(got_ref, rows_ref):
    for z in range(NZ):
        for kind in range(2):
            part = got_ref[z, 24 * kind : 24 * (kind + 1), :]
            for k in range(4):
                rows_ref[k, kind, 24 * z : 24 * (z + 1), :] = part


def expert_kernel(x_ref, gw_ref, uw_ref, dw_ref, part_ref, hid_ref, both_ref):
    inp = jnp.concatenate([x_ref[held_at(t), 0] for t in range(NT)], axis=1)
    cot = jnp.concatenate([x_ref[held_at(t), 1] for t in range(NT)], axis=1)
    both_w = jnp.concatenate([gw_ref[...], uw_ref[...]], axis=1)
    pre = mm(inp, both_w)
    gate, up = pre[:, :128], pre[:, 128:]
    hidden_grad = mm(cot, dw_ref[...], NTR)
    sig = jax.nn.sigmoid(gate)
    act = gate * sig
    hid_ref[...] = (act * up).astype(BF)
    gate_grad = (hidden_grad * up * sig * (1.0 + gate * (1.0 - sig))).astype(BF)
    up_grad = (hidden_grad * act).astype(BF)
    both = jnp.concatenate([gate_grad, up_grad], axis=1)
    both_ref[...] = both
    for t in range(0, NT, 2):
        out = mm(both, both_w[t * COL : (t + 2) * COL], NTR).astype(BF)
        part_ref[t] = out[:, :COL]
        part_ref[t + 1] = out[:, COL:]


def weight_kernel(
    x_ref, hid_ref, both_ref, gg_out, gu_out, gd_out, gg_ref, gu_ref, gd_ref, sems
):
    both = both_ref[...].T
    hidden = hid_ref[...].T
    copies = []
    for t in range(0, NT, 2):
        rows = slice(t * COL, (t + 2) * COL)
        inp = jnp.concatenate([x_ref[held_at(t), 0], x_ref[held_at(t + 1), 0]], axis=1)
        cot = jnp.concatenate([x_ref[held_at(t), 1], x_ref[held_at(t + 1), 1]], axis=1)
        out = mm(both, inp).astype(BF).T
        gg_ref[rows, :] = out[:, :128]
        gu_ref[rows, :] = out[:, 128:]
        gd_ref[:, rows] = mm(hidden, cot).astype(BF)
        if t % 4 == 2:
            done = pl.ds((t - 2) * COL, 4 * COL)
            for n, (src, dst) in enumerate(
                (
                    (gg_ref.at[done], gg_out.at[done]), (gu_ref.at[done], gu_out.at[done]),
                    (gd_ref.at[:, done], gd_out.at[:, done]),
                )
            ):
                copies.append(pltpu.make_async_copy(src, dst, sems.at[t // 4, n]))
                copies[-1].start()
    for copy in copies:
        copy.wait()


def chip_states(early, late, early_other, late_other, mine, theirs):
    is_first = spot("c") == 0
    both_early = early * jnp.where(is_first, theirs, 1.0) + early_other * jnp.where(
        is_first, 1.0, mine
    )
    both_late = late * jnp.where(is_first, 1.0, theirs) + late_other * jnp.where(
        is_first, mine, 1.0
    )
    return [jnp.where(is_first, a[:32], a[32:]).astype(BF) for a in (both_early, both_late)]


def sum_kernel(part_ref, small_ref, out_ref):
    total = part_ref[0].astype(F32)
    for t in range(1, NT):
        total = total + part_ref[t].astype(F32)
    out_ref[:, 0 : 2 * CAP, :] = total.reshape(NZ, 2 * CAP, COL).astype(BF)
    early, late, pieces = small_ref[0:32, :], small_ref[32:64, :], small_ref[64:72, :]
    place = spot("z")
    for z in range(NZ):
        out_ref[z, 24:56, :] = jnp.where(z > place, early, late)
        out_ref[z, 56:64, :] = pieces


def resid_kernel(picks_ref, own_ref, other_ref, g_ref, out_ref):
    own, other = [
        r[:, 0 : 2 * CAP, :].astype(F32).reshape(384, COL).astype(BF) for r in (own_ref, other_ref)
    ]
    moe = mm(picks_ref[0:384, :], own, TN) + mm(picks_ref[384:768, :], other, TN)
    cot = g_ref[spot("c"), COT : COT + TOK, :]
    resid = (cot.astype(F32) + moe).astype(BF)
    for t in range(NT):
        out_ref[t] = resid


def proj_kernel(r_ref, p_ref, mixer_ref, q_ref, mine_ref, og_ref, keep_ref, send_ref, state_ref):
    core = spot("c")
    resid = jnp.concatenate([r_ref[t] for t in range(NT)], axis=1)
    out_grad = mm(resid, p_ref[...])
    og_ref[...] = out_grad
    query = q_ref[...].astype(F32)
    early = exact(query * mine_ref[1:2, :], out_grad)
    late = exact(query * mine_ref[0:1, :], out_grad)
    state_ref[0] = early
    state_ref[1] = late
    send_ref[16] = early.astype(BF)
    send_ref[17] = late.astype(BF)
    mixer = mixer_ref[...]
    for t in range(NT):
        share = mm(r_ref[t], mixer, TN)
        low, high = share[:64], share[64:]
        keep_ref[t] = jnp.where(core == 0, low, high)
        send_ref[t] = jnp.where(core == 0, high, low).astype(BF)


def at_block(far_early, far_late, near, theirs):
    is_first = spot("c") == 0
    early = far_early * jnp.where(is_first, 1.0, theirs) + jnp.where(is_first, 0.0, near)
    late = far_late * jnp.where(is_first, theirs, 1.0) + jnp.where(is_first, near, 0.0)
    return early, late


def intra_kernel(
    og_ref, q_ref, g_ref, mine_ref, own_ref, other_ref, gq_ref, part_ref, weight_ref
):
    place, core = spot("z"), spot("c")
    rows = own_ref[:, 56:64, :].astype(F32)
    chip = rows[:, 0, :] + rows[:, 1, :] + rows[:, 2, :]
    number = lax.broadcasted_iota(jnp.int32, (NZ, COL), 0)
    between = jnp.zeros((NZ, COL), F32)
    for u in range(NZ):
        inside = ((number < u) & (u < place)) | ((number > u) & (u > place))
        between = between + jnp.where(inside, chip[u : u + 1, :], 0.0)
    weight = jnp.exp(-between)
    early_w = jnp.where(number < place, weight, 0.0)
    late_w = jnp.where(number > place, weight, 0.0)
    weight_ref[0:16, :] = early_w
    weight_ref[16:32, :] = late_w

    def far(ref):
        early = late = jnp.zeros((32, COL), F32)
        for z in range(NZ):
            state = ref[z, 24:56, :].astype(F32)
            early = early + state * early_w[z : z + 1, :]
            late = late + state * late_w[z : z + 1, :]
        return early, late

    is_first = core == 0
    here, there = far(own_ref), far(other_ref)
    far_early, far_late = [
        jnp.concatenate([jnp.where(is_first, a, b), jnp.where(is_first, b, a)], axis=0)
        for a, b in zip(here, there)
    ]
    _, _, start, end, _ = decay_parts(rates_of(g_ref, 1 - core))
    there = g_ref[1 - core, KEY : KEY + KD, :].astype(F32) * jnp.where(is_first, start, end)
    near = exact(there, g_ref[1 - core, VALUE : VALUE + VD, :], NTR)
    theirs = jnp.exp(-mine_ref[3:4, :])
    kv_early, kv_late = at_block(far_early, far_late, near, theirs)
    scale = KD ** (-0.5)
    col, row, start, end, _ = decay_parts(rates_of(g_ref, core))
    low, high = scale * start, scale * end
    mixed = scale * jnp.exp(-jnp.abs(col - row))
    out_grad = og_ref[...]
    query, key = q_ref[...], g_ref[core, KEY : KEY + KD, :]
    value = g_ref[core, VALUE : VALUE + VD, :]
    score_grad = exact(out_grad, value) * mixed
    gq_ref[...] = (
        exact(key, score_grad, NTR)
        + low * exact(kv_early, out_grad, NTR)
        + high * exact(kv_late, out_grad, NTR)
    )
    part_ref[0:64, :] = exact(query, score_grad)
    part_ref[64:192, :] = exact(out_grad, mm(query, key, TN) * mixed, TN)
    part_ref[192:256, :] = key.astype(F32)
    part_ref[256:384, :] = value.astype(F32)
    part_ref[384:392, :] = jnp.concatenate([low, high, theirs, jnp.zeros((5, TOK), F32)], axis=0)


def chip_kernel(keep_ref, got_ref, state_ref, mine_ref, out_ref, near_ref):
    place, core = spot("z"), spot("c")
    mine, theirs = jnp.exp(-mine_ref[2:3, :]), jnp.exp(-mine_ref[3:4, :])
    early_other, late_other = got_ref[16].astype(F32), got_ref[17].astype(F32)
    early, late = chip_states(state_ref[0], state_ref[1], early_other, late_other, mine, theirs)
    near_ref[...] = jnp.where(core == 0, late_other, early_other)
    for z in range(NZ):
        out_ref[z, 0:64, :] = (keep_ref[z] + got_ref[z].astype(F32)).astype(BF)
        out_ref[z, 64:96, :] = jnp.where(z > place, early, late)


def gather_kernel(got_ref, weight_ref, state_ref):
    early = late = jnp.zeros((32, COL), F32)
    for z in range(NZ):
        state = got_ref[z, 64:96, :].astype(F32)
        early = early + state * weight_ref[z : z + 1, :]
        late = late + state * weight_ref[16 + z : 17 + z, :]
    state_ref[0] = early
    state_ref[1] = late


def final_kernel(
    far_ref, near_ref, part_ref, got_ref, proj_out, gk_out, gv_out, proj_ref, gk_ref, gv_ref, sems
):
    copies = [
        pltpu.make_async_copy(src, dst, sems.at[n])
        for n, (src, dst) in enumerate(
            ((proj_ref, proj_out), (gk_ref, gk_out), (gv_ref, gv_out))
        )
    ]
    share = jnp.zeros((64, COL), F32)
    for z in range(NZ):
        share = share + got_ref[z, 0:64, :].astype(F32)
    proj_ref[...] = share
    copies[0].start()
    early, late = at_block(
        jnp.concatenate([far_ref[0, 0], far_ref[1, 0]], axis=0),
        jnp.concatenate([far_ref[0, 1], far_ref[1, 1]], axis=0),
        near_ref[...],
        part_ref[386:387, :],
    )
    low, high = part_ref[384:385, :], part_ref[385:386, :]
    key, value = part_ref[192:256, :].astype(BF), part_ref[256:384, :].astype(BF)
    gv_ref[...] = part_ref[64:192, :] + low * exact(early, key, TN) + high * exact(late, key, TN)
    copies[2].start()
    gk_ref[...] = part_ref[0:64, :] + low * exact(early, value) + high * exact(late, value)
    copies[1].start()
    for copy in copies:
        copy.wait()


def groups(step, stride, step_other, stride_other):
    first = [[stride * g + step * k for k in range(4)] for g in range(4)]
    second = [[16 + stride_other * g + step_other * k for k in range(4)] for g in range(4)]
    return first + second


def within(blocks, axis, sets):
    return lax.all_to_all(
        blocks, axis, split_axis=0, concat_axis=0, axis_index_groups=sets, tiled=True
    )


def exchange(blocks, axis):
    return lax.all_to_all(blocks, axis, split_axis=0, concat_axis=0, tiled=True)


def held_at(t):
    return jnp.where(spot("c") == 0, (t % 4) * 4 + t // 4, t)


def on_device(
    cotangent, moe_input, expert_ids, group_weight, expert_weight, mixer_out,
    queries, key_vectors, value_vectors, decay_rates, proj_weight,
    gate_weight, up_weight, down_weight,
):
    ids = expert_ids.T
    held = call(
        load_kernel,
        arr((HELD, COL), BF),
        (
            ids, group_weight.reshape(1, TOK), expert_weight.T, cotangent, moe_input,
            decay_rates, key_vectors, value_vectors,
        ),
        "load",
        60,
        stay=8,
        scratch=[
            pltpu.VMEM((HELD, COL), BF), pltpu.VMEM((2, TOK), jnp.int32), pltpu.VMEM((1, TOK), F32),
            pltpu.VMEM((2, TOK), F32), pltpu.VMEM((1, TOK), F32),
            pltpu.SemaphoreType.DMA((8,)), pltpu.SemaphoreType.DMA((5,)),
        ],
        out=hbm,
    )
    held = lax.all_gather(held, "c")
    rows, picks, small, mine = call(
        pack_kernel,
        [
            arr((NZ, 4 * CAP, COL), BF), arr((768, TOK), BF), arr((72, COL), BF),
            arr((8, TOK), F32),
        ],
        (held,),
        "pack",
    )
    rows = exchange(rows, "z")
    copies = call(spread_kernel, arr((4, 2, NZ * 2 * CAP, COL), BF), (rows,), "spread")
    rows = within(copies, ("c", "tp"), groups(4, 1, 1, 4))
    rows = rows.reshape(4, 2, NZ * 2 * CAP, COL)
    copies = call(copies_kernel, arr((4, *rows.shape), BF), (rows,), "copies", 12)
    rows = within(copies, ("c", "tp"), groups(1, 4, 4, 1))
    rows = rows.reshape(NT, 2, NZ * 2 * CAP, COL)
    shares, hidden, both = call(
        expert_kernel,
        [arr((NT, 384, COL), BF), arr((384, 128), BF), arr((384, 256), BF)],
        (rows, gate_weight[0], up_weight[0], down_weight[0]),
        "expert",
        20,
    )
    shares = exchange(shares, "tp")
    back = call(sum_kernel, arr((NZ, 64, COL), BF), (shares, small), "sums", 6)
    own = exchange(back, "z")
    own, rows, hidden, both = lax.optimization_barrier((own, rows, hidden, both))
    other = lax.ppermute(own, "c", SWAP)
    shapes = [arr((2048, 128), BF), arr((2048, 128), BF), arr((128, 2048), BF)]
    grad_gate, grad_up, grad_down = call(
        weight_kernel,
        shapes,
        (rows, hidden, both),
        "weights",
        16,
        1 << 29,
        scratch=[pltpu.VMEM(a.shape, BF) for a in shapes] + [pltpu.SemaphoreType.DMA((4, 3))],
        out=hbm,
    )
    resid = call(resid_kernel, arr((NT, TOK, COL), BF), (picks, own, other, held), "resid")
    resid, grad_gate, grad_up, grad_down = lax.optimization_barrier(
        (resid, grad_gate, grad_up, grad_down)
    )
    resid = exchange(resid, "tp")
    out_grad, proj_keep, proj_send, state = call(
        proj_kernel,
        [
            arr((TOK, VD), F32), arr((NZ, 64, COL), F32), arr((18, 64, COL), BF),
            arr((2, KD, VD), F32),
        ],
        (resid, proj_weight, mixer_out, queries, mine),
        "proj",
        8,
    )
    got = lax.ppermute(proj_send, "c", SWAP)
    grad_queries, part, weight = call(
        intra_kernel,
        [arr((KD, TOK), F32), arr((392, TOK), F32), arr((32, TOK), F32)],
        (out_grad, queries, held, mine, own, other),
        "intra",
    )
    chip, near = call(
        chip_kernel,
        [arr((NZ, 96, COL), BF), arr((KD, VD), F32)],
        (proj_keep, got, state, mine),
        "chip",
    )
    chip, grad_queries, part, weight = lax.optimization_barrier((chip, grad_queries, part, weight))
    chip = exchange(chip, "z")
    far = call(gather_kernel, arr((2, 32, COL), F32), (chip, weight), "gather")
    far = lax.all_gather(far, "c")
    shapes = [arr((64, COL), F32), arr((KD, TOK), F32), arr((VD, TOK), F32)]
    grad_proj, grad_keys, grad_values = call(
        final_kernel,
        shapes,
        (far, near, part, chip),
        "final",
        scratch=[pltpu.VMEM(a.shape, F32) for a in shapes] + [pltpu.SemaphoreType.DMA((3,))],
        out=hbm,
    )
    return (
        grad_gate[None], grad_up[None], grad_down[None],
        grad_proj, grad_queries, grad_keys, grad_values,
    )


def solution(mesh):
    finer = Mesh(mesh.devices.reshape(NZ, 2, NT), ("z", "c", "tp"))
    in_specs = (
        P(SP, None), P(SP, None), P(SP, None), P(SP), P(SP, None), P(SP, "tp"),
        P("tp", SP), P("tp", SP), P("tp", SP), P("tp", SP), P(None, "tp"),
        P(SP, None, "tp"), P(SP, None, "tp"), P(SP, "tp", None),
    )
    out_specs = (
        P(SP, None, "tp"), P(SP, None, "tp"), P(SP, "tp", None), P(SP, "tp"),
        P("tp", SP), P("tp", SP), P("tp", SP),
    )
    return jax.shard_map(
        on_device, mesh=finer, in_specs=in_specs, out_specs=out_specs, check_vma=False
    )
```

```python
import jax
import jax.numpy as jnp
from jax import lax
from jax.experimental import pallas as pl
from jax.experimental.pallas import tpu as pltpu
from jax.sharding import Mesh
from jax.sharding import PartitionSpec as P

BF = jnp.bfloat16
F32 = jnp.float32
NZ = 16
NT = 16
CAP = 12
TOK = 128
COL = 128
KD = 64
VD = 128
SP = ("z", "c")
SWAP = [(0, 1), (1, 0)]

NN = (((1,), (0,)), ((), ()))
NTR = (((1,), (1,)), ((), ()))
TN = (((0,), (0,)), ((), ()))


def mm(a, b, dims=NN):
    return lax.dot_general(a, b, dims, preferred_element_type=F32)


def halves(a):
    high = a.astype(BF)
    return high, (a - high.astype(F32)).astype(BF)


def exact(a, b, dims=NN):
    if a.dtype == BF:
        high, low = halves(b)
        return mm(a, high, dims) + mm(a, low, dims)
    high, low = halves(a)
    if b.dtype == BF:
        return mm(high, b, dims) + mm(low, b, dims)
    other, rest = halves(b)
    return mm(high, other, dims) + (mm(high, rest, dims) + mm(low, other, dims))


def vmem():
    return pl.BlockSpec(memory_space=pltpu.VMEM)


def hbm():
    return pl.BlockSpec(memory_space=pltpu.HBM)


def call(kernel, outs, args, name, mib=4, flops=1 << 27, stay=0, scratch=(), out=None):
    return pl.pallas_call(
        kernel,
        out_shape=outs,
        in_specs=[hbm()] * stay + [vmem()] * (len(args) - stay),
        out_specs=jax.tree.map(lambda _: (out or vmem)(), outs),
        scratch_shapes=scratch,
        name=name,
        compiler_params=pltpu.CompilerParams(vmem_limit_bytes=mib << 20),
        cost_estimate=pl.CostEstimate(flops=flops, bytes_accessed=1 << 20, transcendentals=0),
    )(*args)


def spot(axis):
    return lax.axis_index(axis).astype(jnp.int32)


def fetch(sources, targets, sems):
    copies = [
        pltpu.make_async_copy(src, dst, sems.at[n])
        for n, (src, dst) in enumerate(zip(sources, targets))
    ]
    for copy in copies:
        copy.start()
    for copy in copies:
        copy.wait()


def arr(shape, dtype):
    return jax.ShapeDtypeStruct(shape, dtype)


def placement(ids, wanted, rank):
    first = ids[0:1, :] == wanted
    match = first | (ids[1:2, :] == wanted)
    tok = TOK
    before = lax.broadcasted_iota(jnp.int32, (tok, tok), 0) < lax.broadcasted_iota(
        jnp.int32, (tok, tok), 1
    )
    ranks = mm(jnp.where(match, 1.0, 0.0).astype(BF), jnp.where(before, 1.0, 0.0).astype(BF))
    return match & (ranks == rank.astype(F32)), first


def decay_parts(rates):
    upto = lax.broadcasted_iota(jnp.int32, (TOK, TOK), 1) <= lax.broadcasted_iota(
        jnp.int32, (TOK, TOK), 0
    )
    col = jnp.broadcast_to(
        jnp.sum(jnp.where(upto, rates, 0.0), axis=1, keepdims=True), (TOK, TOK)
    )
    row = col.T
    total = jnp.sum(rates, axis=1, keepdims=True)
    prefix = row[0:1, :]
    start = jnp.exp(-prefix)
    end = jnp.exp(jnp.minimum(prefix - total, 0.0))
    return col, row, start, end, jnp.broadcast_to(total, (1, TOK))


def in_pieces(row):
    hi = row.astype(BF).astype(F32)
    mid = (row - hi).astype(BF).astype(F32)
    return jnp.concatenate([hi, mid, row - hi - mid], axis=0)


def in_one(pieces):
    pieces = pieces.astype(F32)
    return pieces[0:1, :] + pieces[1:2, :] + pieces[2:3, :]


def ids_of(rows):
    return rows[IDS - ROUTE : IDS - ROUTE + 2, :].astype(jnp.int32)


def rates_of(g_ref, block):
    return in_one(g_ref[block, ROUTE:HELD, :].astype(F32)[RATE - ROUTE : IDS - ROUTE])


COT, INP, KEY, VALUE, ROUTE, RATE, IDS, HELD = 0, 128, 256, 320, 448, 456, 459, 464


def load_kernel(
    ids_in, gw_in, ew_in, cot_in, inp_in, rate_in, k_in, v_in,
    out, held_ref, ids_ref, gw_ref, ew_ref, rate_ref, sems, out_sems,
):
    here = pl.ds(pl.multiple_of(spot("tp") * COL, COL), COL)
    bulk = [pl.ds(COT, TOK), pl.ds(INP, TOK), pl.ds(KEY, KD), pl.ds(VALUE, VD)]
    sources = (cot_in.at[:, here], inp_in.at[:, here], k_in, v_in, ids_in, gw_in, ew_in, rate_in)
    targets = [held_ref.at[part] for part in bulk] + [ids_ref, gw_ref, ew_ref, rate_ref]
    copies = [
        pltpu.make_async_copy(src, dst, sems.at[n])
        for n, (src, dst) in enumerate(zip(sources, targets))
    ]
    small = pl.ds(ROUTE, HELD - ROUTE)
    leaving = [
        pltpu.make_async_copy(held_ref.at[part], out.at[part], out_sems.at[n])
        for n, part in enumerate(bulk + [small])
    ]
    for copy in copies:
        copy.start()
    for copy, leave in zip(copies[:4], leaving):
        copy.wait()
        leave.start()
    for copy in copies[4:]:
        copy.wait()
    weights = gw_ref[...] * ew_ref[...]
    none = jnp.zeros((2, TOK), F32)
    held_ref[ROUTE:HELD, :] = jnp.concatenate(
        [in_pieces(weights[0:1, :]), in_pieces(weights[1:2, :]), none]
        + [in_pieces(rate_ref[...]), ids_ref[...].astype(F32), none, none[0:1, :]],
        axis=0,
    ).astype(BF)
    leaving[4].start()
    for leave in leaving:
        leave.wait()


def pack_kernel(g_ref, rows_ref, picks_ref, small_ref, mine_ref):
    core = spot("c")
    number = lax.broadcasted_iota(jnp.int32, (NZ * 2 * CAP, TOK), 0)
    z = lax.shift_right_logical(number * 2731, 16)
    q = number - 2 * CAP * z
    first_half = q < CAP
    inp_rows = cot_rows = 0.0
    for block, wanted, rank in (
        (core, jnp.where(first_half, 2 * z + core, -1), q),
        (1 - core, jnp.where(first_half, -1, 2 * z + core), q - CAP),
    ):
        rows = g_ref[block, ROUTE:HELD, :].astype(F32)
        hit, first = placement(ids_of(rows), wanted, rank)
        scale = jnp.sum(
            jnp.where(hit, jnp.where(first, in_one(rows[0:3]), in_one(rows[3:6])), 0.0),
            axis=1,
            keepdims=True,
        )
        take = jnp.where(hit, 1.0, 0.0).astype(BF)
        if block is core:
            picks_ref[0:384, :] = take
        inp_rows = inp_rows + mm(take, g_ref[block, INP : INP + TOK, :])
        cot_rows = cot_rows + mm(take, g_ref[block, COT : COT + TOK, :]) * scale
    for z in range(NZ):
        part = slice(2 * CAP * z, 2 * CAP * (z + 1))
        rows_ref[z, 0 : 2 * CAP, :] = inp_rows[part].astype(BF)
        rows_ref[z, 2 * CAP : 4 * CAP, :] = cot_rows[part].astype(BF)
    z = lax.shift_right_logical(number * 2731, 16)
    hit, _ = placement(
        ids_of(g_ref[core, ROUTE:HELD, :].astype(F32)),
        jnp.where(first_half, -1, 2 * z + 1 - core),
        q - CAP,
    )
    picks_ref[384:768, :] = jnp.where(hit, 1.0, 0.0).astype(BF)

    _, _, start_a, end_a, total_a = decay_parts(rates_of(g_ref, 0))
    _, _, start_b, end_b, total_b = decay_parts(rates_of(g_ref, 1))
    half = pl.ds(pl.multiple_of(KEY + 32 * core, 32), 32)
    keys = jnp.concatenate([g_ref[0, half, :], g_ref[1, half, :]], axis=1).astype(F32)
    values = jnp.concatenate([g_ref[k, VALUE : VALUE + VD, :] for k in (0, 1)], axis=1)
    early = jnp.concatenate([end_a * jnp.exp(-total_b), end_b], axis=1)
    late = jnp.concatenate([start_a, start_b * jnp.exp(-total_a)], axis=1)
    small_ref[0:32, :] = exact(keys * early, values, NTR).astype(BF)
    small_ref[32:64, :] = exact(keys * late, values, NTR).astype(BF)
    small_ref[64:72, :] = jnp.concatenate(
        [in_pieces(total_a + total_b), jnp.zeros((5, TOK), F32)], axis=0
    ).astype(BF)
    is_first = core == 0
    mine_ref[...] = jnp.concatenate(
        [
            jnp.where(is_first, start_a, start_b), jnp.where(is_first, end_a, end_b),
            jnp.where(is_first, total_a, total_b), jnp.where(is_first, total_b, total_a),
            jnp.zeros((4, TOK), F32),
        ],
        axis=0,
    )


def copies_kernel(got_ref, out_ref):
    for j in range(4):
        for kind in range(2):
            part = got_ref[j, kind]
            for k in range(4):
                out_ref[k, j, kind] = part


def spread_kernel(got_ref, rows_ref):
    for z in range(NZ):
        for kind in range(2):
            part = got_ref[z, 24 * kind : 24 * (kind + 1), :]
            for k in range(4):
                rows_ref[k, kind, 24 * z : 24 * (z + 1), :] = part


def expert_kernel(x_ref, gw_ref, uw_ref, dw_ref, part_ref, hid_ref, both_ref):
    inp = jnp.concatenate([x_ref[held_at(t), 0] for t in range(NT)], axis=1)
    cot = jnp.concatenate([x_ref[held_at(t), 1] for t in range(NT)], axis=1)
    both_w = jnp.concatenate([gw_ref[...], uw_ref[...]], axis=1)
    pre = mm(inp, both_w)
    gate, up = pre[:, :128], pre[:, 128:]
    hidden_grad = mm(cot, dw_ref[...], NTR)
    sig = jax.nn.sigmoid(gate)
    act = gate * sig
    hid_ref[...] = (act * up).astype(BF)
    gate_grad = (hidden_grad * up * sig * (1.0 + gate * (1.0 - sig))).astype(BF)
    up_grad = (hidden_grad * act).astype(BF)
    both = jnp.concatenate([gate_grad, up_grad], axis=1)
    both_ref[...] = both
    for t in range(0, NT, 2):
        out = mm(both, both_w[t * COL : (t + 2) * COL], NTR).astype(BF)
        part_ref[t] = out[:, :COL]
        part_ref[t + 1] = out[:, COL:]


def weight_kernel(
    x_ref, hid_ref, both_ref, gg_out, gu_out, gd_out, gg_ref, gu_ref, gd_ref, sems
):
    both = both_ref[...].T
    hidden = hid_ref[...].T
    copies = []
    for t in range(0, NT, 2):
        rows = slice(t * COL, (t + 2) * COL)
        inp = jnp.concatenate([x_ref[held_at(t), 0], x_ref[held_at(t + 1), 0]], axis=1)
        cot = jnp.concatenate([x_ref[held_at(t), 1], x_ref[held_at(t + 1), 1]], axis=1)
        out = mm(both, inp).astype(BF).T
        gg_ref[rows, :] = out[:, :128]
        gu_ref[rows, :] = out[:, 128:]
        gd_ref[:, rows] = mm(hidden, cot).astype(BF)
        if t % 4 == 2:
            done = pl.ds((t - 2) * COL, 4 * COL)
            for n, (src, dst) in enumerate(
                (
                    (gg_ref.at[done], gg_out.at[done]), (gu_ref.at[done], gu_out.at[done]),
                    (gd_ref.at[:, done], gd_out.at[:, done]),
                )
            ):
                copies.append(pltpu.make_async_copy(src, dst, sems.at[t // 4, n]))
                copies[-1].start()
    for copy in copies:
        copy.wait()


def chip_states(early, late, early_other, late_other, mine, theirs):
    is_first = spot("c") == 0
    both_early = early * jnp.where(is_first, theirs, 1.0) + early_other * jnp.where(
        is_first, 1.0, mine
    )
    both_late = late * jnp.where(is_first, 1.0, theirs) + late_other * jnp.where(
        is_first, mine, 1.0
    )
    return [jnp.where(is_first, a[:32], a[32:]).astype(BF) for a in (both_early, both_late)]


def sum_kernel(part_ref, small_ref, out_ref):
    total = part_ref[0].astype(F32)
    for t in range(1, NT):
        total = total + part_ref[t].astype(F32)
    out_ref[:, 0 : 2 * CAP, :] = total.reshape(NZ, 2 * CAP, COL).astype(BF)
    early, late, pieces = small_ref[0:32, :], small_ref[32:64, :], small_ref[64:72, :]
    place = spot("z")
    for z in range(NZ):
        out_ref[z, 24:56, :] = jnp.where(z > place, early, late)
        out_ref[z, 56:64, :] = pieces


def resid_kernel(picks_ref, own_ref, other_ref, g_ref, out_ref):
    own, other = [
        r[:, 0 : 2 * CAP, :].astype(F32).reshape(384, COL).astype(BF) for r in (own_ref, other_ref)
    ]
    moe = mm(picks_ref[0:384, :], own, TN) + mm(picks_ref[384:768, :], other, TN)
    cot = g_ref[spot("c"), COT : COT + TOK, :]
    resid = (cot.astype(F32) + moe).astype(BF)
    for t in range(NT):
        out_ref[t] = resid


def proj_kernel(r_ref, p_ref, mixer_ref, q_ref, mine_ref, og_ref, keep_ref, send_ref, state_ref):
    core = spot("c")
    resid = jnp.concatenate([r_ref[t] for t in range(NT)], axis=1)
    out_grad = mm(resid, p_ref[...])
    og_ref[...] = out_grad
    query = q_ref[...].astype(F32)
    early = exact(query * mine_ref[1:2, :], out_grad)
    late = exact(query * mine_ref[0:1, :], out_grad)
    state_ref[0] = early
    state_ref[1] = late
    send_ref[16] = early.astype(BF)
    send_ref[17] = late.astype(BF)
    mixer = mixer_ref[...]
    for t in range(NT):
        share = mm(r_ref[t], mixer, TN)
        low, high = share[:64], share[64:]
        keep_ref[t] = jnp.where(core == 0, low, high)
        send_ref[t] = jnp.where(core == 0, high, low).astype(BF)


def at_block(far_early, far_late, near, theirs):
    is_first = spot("c") == 0
    early = far_early * jnp.where(is_first, 1.0, theirs) + jnp.where(is_first, 0.0, near)
    late = far_late * jnp.where(is_first, theirs, 1.0) + jnp.where(is_first, near, 0.0)
    return early, late


def intra_kernel(
    og_ref, q_ref, g_ref, mine_ref, own_ref, other_ref, gq_ref, part_ref, weight_ref
):
    place, core = spot("z"), spot("c")
    rows = own_ref[:, 56:64, :].astype(F32)
    chip = rows[:, 0, :] + rows[:, 1, :] + rows[:, 2, :]
    number = lax.broadcasted_iota(jnp.int32, (NZ, COL), 0)
    between = jnp.zeros((NZ, COL), F32)
    for u in range(NZ):
        inside = ((number < u) & (u < place)) | ((number > u) & (u > place))
        between = between + jnp.where(inside, chip[u : u + 1, :], 0.0)
    weight = jnp.exp(-between)
    early_w = jnp.where(number < place, weight, 0.0)
    late_w = jnp.where(number > place, weight, 0.0)
    weight_ref[0:16, :] = early_w
    weight_ref[16:32, :] = late_w

    def far(ref):
        early = late = jnp.zeros((32, COL), F32)
        for z in range(NZ):
            state = ref[z, 24:56, :].astype(F32)
            early = early + state * early_w[z : z + 1, :]
            late = late + state * late_w[z : z + 1, :]
        return early, late

    is_first = core == 0
    here, there = far(own_ref), far(other_ref)
    far_early, far_late = [
        jnp.concatenate([jnp.where(is_first, a, b), jnp.where(is_first, b, a)], axis=0)
        for a, b in zip(here, there)
    ]
    _, _, start, end, _ = decay_parts(rates_of(g_ref, 1 - core))
    there = g_ref[1 - core, KEY : KEY + KD, :].astype(F32) * jnp.where(is_first, start, end)
    near = exact(there, g_ref[1 - core, VALUE : VALUE + VD, :], NTR)
    theirs = jnp.exp(-mine_ref[3:4, :])
    kv_early, kv_late = at_block(far_early, far_late, near, theirs)
    scale = KD ** (-0.5)
    col, row, start, end, _ = decay_parts(rates_of(g_ref, core))
    low, high = scale * start, scale * end
    mixed = scale * jnp.exp(-jnp.abs(col - row))
    out_grad = og_ref[...]
    query, key = q_ref[...], g_ref[core, KEY : KEY + KD, :]
    value = g_ref[core, VALUE : VALUE + VD, :]
    score_grad = exact(out_grad, value) * mixed
    gq_ref[...] = (
        exact(key, score_grad, NTR)
        + low * exact(kv_early, out_grad, NTR)
        + high * exact(kv_late, out_grad, NTR)
    )
    part_ref[0:64, :] = exact(query, score_grad)
    part_ref[64:192, :] = exact(out_grad, mm(query, key, TN) * mixed, TN)
    part_ref[192:256, :] = key.astype(F32)
    part_ref[256:384, :] = value.astype(F32)
    part_ref[384:392, :] = jnp.concatenate([low, high, theirs, jnp.zeros((5, TOK), F32)], axis=0)


def chip_kernel(keep_ref, got_ref, state_ref, mine_ref, out_ref, near_ref):
    place, core = spot("z"), spot("c")
    mine, theirs = jnp.exp(-mine_ref[2:3, :]), jnp.exp(-mine_ref[3:4, :])
    early_other, late_other = got_ref[16].astype(F32), got_ref[17].astype(F32)
    early, late = chip_states(state_ref[0], state_ref[1], early_other, late_other, mine, theirs)
    near_ref[...] = jnp.where(core == 0, late_other, early_other)
    for z in range(NZ):
        out_ref[z, 0:64, :] = (keep_ref[z] + got_ref[z].astype(F32)).astype(BF)
        out_ref[z, 64:96, :] = jnp.where(z > place, early, late)


def gather_kernel(got_ref, weight_ref, state_ref):
    early = late = jnp.zeros((32, COL), F32)
    for z in range(NZ):
        state = got_ref[z, 64:96, :].astype(F32)
        early = early + state * weight_ref[z : z + 1, :]
        late = late + state * weight_ref[16 + z : 17 + z, :]
    state_ref[0] = early
    state_ref[1] = late


def final_kernel(far_ref, near_ref, part_ref, got_ref, proj_ref, gk_ref, gv_ref):
    share = jnp.zeros((64, COL), F32)
    for z in range(NZ):
        share = share + got_ref[z, 0:64, :].astype(F32)
    proj_ref[...] = share
    early, late = at_block(
        jnp.concatenate([far_ref[0, 0], far_ref[1, 0]], axis=0),
        jnp.concatenate([far_ref[0, 1], far_ref[1, 1]], axis=0),
        near_ref[...],
        part_ref[386:387, :],
    )
    low, high = part_ref[384:385, :], part_ref[385:386, :]
    key, value = part_ref[192:256, :].astype(BF), part_ref[256:384, :].astype(BF)
    gk_ref[...] = part_ref[0:64, :] + low * exact(early, value) + high * exact(late, value)
    gv_ref[...] = part_ref[64:192, :] + low * exact(early, key, TN) + high * exact(late, key, TN)


def groups(step, stride, step_other, stride_other):
    first = [[stride * g + step * k for k in range(4)] for g in range(4)]
    second = [[16 + stride_other * g + step_other * k for k in range(4)] for g in range(4)]
    return first + second


def within(blocks, axis, sets):
    return lax.all_to_all(
        blocks, axis, split_axis=0, concat_axis=0, axis_index_groups=sets, tiled=True
    )


def exchange(blocks, axis):
    return lax.all_to_all(blocks, axis, split_axis=0, concat_axis=0, tiled=True)


def held_at(t):
    return jnp.where(spot("c") == 0, (t % 4) * 4 + t // 4, t)


def on_device(
    cotangent, moe_input, expert_ids, group_weight, expert_weight, mixer_out,
    queries, key_vectors, value_vectors, decay_rates, proj_weight,
    gate_weight, up_weight, down_weight,
):
    ids = expert_ids.T
    held = call(
        load_kernel,
        arr((HELD, COL), BF),
        (
            ids, group_weight.reshape(1, TOK), expert_weight.T, cotangent, moe_input,
            decay_rates, key_vectors, value_vectors,
        ),
        "load",
        60,
        stay=8,
        scratch=[
            pltpu.VMEM((HELD, COL), BF), pltpu.VMEM((2, TOK), jnp.int32), pltpu.VMEM((1, TOK), F32),
            pltpu.VMEM((2, TOK), F32), pltpu.VMEM((1, TOK), F32),
            pltpu.SemaphoreType.DMA((8,)), pltpu.SemaphoreType.DMA((5,)),
        ],
        out=hbm,
    )
    held = lax.all_gather(held, "c")
    rows, picks, small, mine = call(
        pack_kernel,
        [
            arr((NZ, 4 * CAP, COL), BF), arr((768, TOK), BF), arr((72, COL), BF),
            arr((8, TOK), F32),
        ],
        (held,),
        "pack",
    )
    rows = exchange(rows, "z")
    copies = call(spread_kernel, arr((4, 2, NZ * 2 * CAP, COL), BF), (rows,), "spread")
    rows = within(copies, ("c", "tp"), groups(4, 1, 1, 4))
    rows = rows.reshape(4, 2, NZ * 2 * CAP, COL)
    copies = call(copies_kernel, arr((4, *rows.shape), BF), (rows,), "copies", 12)
    rows = within(copies, ("c", "tp"), groups(1, 4, 4, 1))
    rows = rows.reshape(NT, 2, NZ * 2 * CAP, COL)
    shares, hidden, both = call(
        expert_kernel,
        [arr((NT, 384, COL), BF), arr((384, 128), BF), arr((384, 256), BF)],
        (rows, gate_weight[0], up_weight[0], down_weight[0]),
        "expert",
        20,
    )
    shares = exchange(shares, "tp")
    back = call(sum_kernel, arr((NZ, 64, COL), BF), (shares, small), "sums", 6)
    own = exchange(back, "z")
    own, rows, hidden, both = lax.optimization_barrier((own, rows, hidden, both))
    other = lax.ppermute(own, "c", SWAP)
    shapes = [arr((2048, 128), BF), arr((2048, 128), BF), arr((128, 2048), BF)]
    grad_gate, grad_up, grad_down = call(
        weight_kernel,
        shapes,
        (rows, hidden, both),
        "weights",
        16,
        1 << 29,
        scratch=[pltpu.VMEM(a.shape, BF) for a in shapes] + [pltpu.SemaphoreType.DMA((4, 3))],
        out=hbm,
    )
    resid = call(resid_kernel, arr((NT, TOK, COL), BF), (picks, own, other, held), "resid")
    resid, grad_gate, grad_up, grad_down = lax.optimization_barrier(
        (resid, grad_gate, grad_up, grad_down)
    )
    resid = exchange(resid, "tp")
    out_grad, proj_keep, proj_send, state = call(
        proj_kernel,
        [
            arr((TOK, VD), F32), arr((NZ, 64, COL), F32), arr((18, 64, COL), BF),
            arr((2, KD, VD), F32),
        ],
        (resid, proj_weight, mixer_out, queries, mine),
        "proj",
        8,
    )
    got = lax.ppermute(proj_send, "c", SWAP)
    grad_queries, part, weight = call(
        intra_kernel,
        [arr((KD, TOK), F32), arr((392, TOK), F32), arr((32, TOK), F32)],
        (out_grad, queries, held, mine, own, other),
        "intra",
    )
    chip, near = call(
        chip_kernel,
        [arr((NZ, 96, COL), BF), arr((KD, VD), F32)],
        (proj_keep, got, state, mine),
        "chip",
    )
    chip, grad_queries, part, weight = lax.optimization_barrier((chip, grad_queries, part, weight))
    chip = exchange(chip, "z")
    far = call(gather_kernel, arr((2, 32, COL), F32), (chip, weight), "gather")
    far = lax.all_gather(far, "c")
    grad_proj, grad_keys, grad_values = call(
        final_kernel,
        [arr((64, COL), F32), arr((KD, TOK), F32), arr((VD, TOK), F32)],
        (far, near, part, chip),
        "final",
    )
    return (
        grad_gate[None], grad_up[None], grad_down[None],
        grad_proj, grad_queries, grad_keys, grad_values,
    )


def solution(mesh):
    finer = Mesh(mesh.devices.reshape(NZ, 2, NT), ("z", "c", "tp"))
    in_specs = (
        P(SP, None), P(SP, None), P(SP, None), P(SP), P(SP, None), P(SP, "tp"),
        P("tp", SP), P("tp", SP), P("tp", SP), P("tp", SP), P(None, "tp"),
        P(SP, None, "tp"), P(SP, None, "tp"), P(SP, "tp", None),
    )
    out_specs = (
        P(SP, None, "tp"), P(SP, None, "tp"), P(SP, "tp", None), P(SP, "tp"),
        P("tp", SP), P("tp", SP), P("tp", SP),
    )
    return jax.shard_map(
        on_device, mesh=finer, in_specs=in_specs, out_specs=out_specs, check_vma=False
    )
```
